256 devices in a mesh: sp: 64 (over z, x, core), tp: 4 (over y).
Axes of the slice: x: 4, y: 4, z: 8, core: 2. Of those that a mesh axis runs over, the one named last changes fastest.
Arguments:
- mid: bfloat16 [12288, 2048], P('sp'), may hold values from -6 to 6
- out_grad: bfloat16 [12288, 2048], P('sp'), may hold values from -16 to 16
- expert_ids: int32 [12288, 2], P('sp'), may hold values from 0 to 63, all different within a row; in each aligned block of 192 rows (0 to 191, 192 to 383, ...) at most 9 rows name the same one
- route_weights: float32 [12288, 2], P('sp'), may hold values from 0.1 to 0.9
- gate_proj: bfloat16 [64, 2048, 1024], P('sp', None, 'tp'), may hold values from -0.375 to 0.375
- up_proj: bfloat16 [64, 2048, 1024], P('sp', None, 'tp'), may hold values from -0.375 to 0.375
- down_proj: bfloat16 [64, 1024, 2048], P('sp', 'tp'), may hold values from -0.1875 to 0.1875
- out_proj: bfloat16 [512, 2048], P('tp'), may hold values from -0.25 to 0.25
- branch_gate: bfloat16 [12288, 512], P('sp', 'tp'), may hold values from -6 to 6
- conv_out: bfloat16 [2, 12288, 512], P(None, 'sp', 'tp'), may hold values from -6 to 6
- prior_state: float32 [2, 12288, 512], P(None, 'sp', 'tp'), may hold values from -6 to 6
- rate_gate_w: bfloat16 [2, 8, 64, 64], P(None, 'tp'), may hold values from -0.75 to 0.75
- input_gate_w: bfloat16 [2, 8, 64, 64], P(None, 'tp'), may hold values from -0.75 to 0.75
- decay_param: float32 [2, 512], P(None, 'tp'), may hold values from 4 to 16
- decay_jump: float32 [2, 12288, 512], P(None, 'sp', 'tp'), may hold values from -2 to 0
- conv_taps: bfloat16 [2, 4, 512], P(None, None, 'tp'), may hold values from -3 to 3
Outputs:
- gate_grad: bfloat16 [64, 2048, 1024], P('sp', None, 'tp')
- up_grad: bfloat16 [64, 2048, 1024], P('sp', None, 'tp')
- down_grad: bfloat16 [64, 1024, 2048], P('sp', 'tp')
- proj_grad_t: float32 [2048, 512], P('sp', 'tp')
- input_grad: bfloat16 [12288, 512], P('sp', 'tp')
- branch_gate_grad: bfloat16 [12288, 512], P('sp', 'tp')
The draws below stay inside these ranges and needn't reach their ends.
Inputs may be any that keep to these rules, and one draw needn't show every extreme that they name: `expert_ids`: each row names 2 different experts. Among the rows of one device no expert is named by more than 9 rows, a bound that some block reaches of some device.
All inputs are finite; a program needn't handle non-finite values.
Results may differ from the reference program's by a relative error of at most 0.023.
The reference program's roundings to bfloat16 on the way count: a program that leaves them out, or rounds other values in their place, can miss the bound.
Values may be sent and summed in bfloat16 or wider, within the bound.
A program may use at most 64 MiB of HBM per device.

```python
import math
import jax
import jax.numpy as jnp
import numpy as np
from jax import lax

D = 2048
FF = 1024
HEADS = 8
HEAD = 64
W = 512
TAPS = 4
TOP = 2
EXPERTS = 64
TOK_DEV = 192
CAP = 9
STREAM_ITEMS = 12288
N_SP = 64
N_TP = 4


def draw_decay_param(key, part):
    selection_seed, slow_key, fast_key = jax.random.split(jax.random.fold_in(key, 11), 3)
    slow_share = 0.5
    slow_mask = jax.random.uniform(selection_seed, (2, W), jnp.float32) < slow_share
    slow_rate = jnp.exp(jax.random.uniform(slow_key, (2, W), jnp.float32, jnp.log(0.02), jnp.log(0.12))) / STREAM_ITEMS
    fast_rate = jnp.exp(jax.random.uniform(fast_key, (2, W), jnp.float32, jnp.log(0.0025), jnp.log(0.008)))
    rates = jnp.where(slow_mask, slow_rate, fast_rate)
    return -jnp.log(jnp.expm1(rates))


def draw_decay_jump(key, part):
    block_key, place_key, loss_key = jax.random.split(jax.random.fold_in(key, 23), 3)
    block_count = STREAM_ITEMS // TOK_DEV
    factors = jnp.exp(jax.random.uniform(block_key, (2, block_count, 1), jnp.float32, jnp.log(0.1), jnp.log(0.8)))
    equilibrium_level = -jnp.repeat(factors, TOK_DEV, axis=1) / STREAM_ITEMS
    assigned_positions = jax.random.randint(place_key, (2, 2), 0, STREAM_ITEMS)
    objective_scores = jax.random.uniform(loss_key, (2, 2, W), jnp.float32, 0.2, 0.5)
    arrival_tallies = (jnp.arange(STREAM_ITEMS, dtype=jnp.int32)[None, :, None] == assigned_positions[:, None, :]).astype(jnp.float32)
    return equilibrium_level + jnp.einsum('dwp,dpu->dwu', arrival_tallies, jnp.log1p(-objective_scores))


def spiked(drawn, key, source, target, parts, factor):
    owner, partner = [(jnp.arange(drawn.shape[axis_at]) // (drawn.shape[axis_at] // parts)).reshape([-1 if axis == axis_at else 1 for axis in range(drawn.ndim)]) for axis_at in (source, target)]
    chosen = jax.random.permutation(key, parts)[partner]
    strong = (owner == chosen) | (owner == (partner + parts // 2) % parts)
    return jnp.where(strong, factor * drawn, drawn)


def steps_of(key, extent, cuts, least, top_value):
    def one(axis_at, blocks):
        draws = jax.random.uniform(jax.random.fold_in(jax.random.fold_in(key, 6), axis_at), (blocks,), jnp.float32, least / len(cuts), top_value / len(cuts))
        return jnp.repeat(jnp.exp(draws), extent[axis_at] // blocks).reshape((-1,) + (1,) * (len(extent) - axis_at - 1))

    loudness = one(*cuts[0])
    for cut in cuts[1:]:
        loudness = loudness * one(*cut)
    return loudness


def routed_block(stream_key, own, number, rows, count, top, limit, slope):
    ranking = jax.random.permutation(stream_key, count)
    packed, usual = shares(count, rows * top, limit, slope, True), shares(count, rows * top, limit, slope, False)
    places = jnp.arange(count)

    def named(tallies, turn):
        used = int((tallies > 0).sum())
        fixed = max(1, used // 4)
        shifted = fixed + (places - fixed + turn * (used - fixed)) % max(1, count - fixed)
        return jnp.zeros((count,), jnp.int32).at[ranking[jnp.where(places < fixed, places, shifted)]].set(jnp.asarray(tallies, jnp.int32))

    tallies = jnp.where(number % 4 == 0, named(packed, number // 4), named(usual, number - number // 4 - 1))
    mixed = jax.random.permutation(jax.random.fold_in(own, 3), count)
    giver, sink = mixed[0:count // 2 * 2:2], mixed[1:count // 2 * 2:2]
    slack = jnp.minimum(tallies[giver] - 1, limit - tallies[sink]) // 2
    slack = jnp.where((giver == ranking[0]) | (sink == ranking[0]) | (tallies[sink] == 0), 0, jnp.maximum(slack, 0))
    shifted = jax.random.randint(jax.random.fold_in(own, 4), (count // 2,), 0, 1 << 20) % (slack + 1)
    tallies = tallies.at[giver].add(-shifted).at[sink].add(shifted)
    labels = jnp.searchsorted(jnp.cumsum(tallies), jnp.arange(rows * top), side="right").astype(jnp.int32)
    listing = labels.reshape(top, rows).T
    listing = listing[jax.random.permutation(jax.random.fold_in(own, 1), rows)]
    turn = jax.random.randint(jax.random.fold_in(own, 2), (rows, 1), 0, top)
    return jnp.take_along_axis(listing, (jnp.arange(top)[None, :] + turn) % top, axis=1)


def shares(number_of, total, bound, skew, full):
    weights = [(1 << 20) // math.isqrt(rank ** skew) + 1 for rank in range(1, number_of + 1)]
    largest = bound if full else min(bound, max(-(-total // number_of), total * weights[0] // sum(weights)))
    least = 1 if total - largest >= number_of - 1 else 0
    given, surplus = [largest] + [least] * (number_of - 1), total - largest - least * (number_of - 1)
    while surplus > 0:
        candidates = [i for i in range(1, number_of) if given[i] < largest] or [i for i in range(1, number_of) if given[i] < bound]
        pool, left = sum([weights[i] for i in candidates]), surplus
        for i in candidates:
            more = min(bound - given[i], max(1, left * weights[i] // pool), surplus)
            given[i] = given[i] + more
            surplus = surplus - more
    return np.array(given)


def normal_values(rng, extent, width, most, shards=(), held_as=jnp.bfloat16):
    loudness = steps_of(rng, extent, shards, -0.22, 0.18) if shards else 1.0
    entries = jax.random.normal(rng, extent, jnp.float32) * width * loudness
    return jnp.minimum(jnp.maximum(entries, -most), most).astype(held_as)


def heavy_noise(rng, dims, width, most, cuts, heavy, kind=jnp.bfloat16):
    values = width * jax.random.normal(rng, dims, jnp.float32)
    if cuts:
        values = values * steps_of(rng, dims, cuts, -0.22, 0.18)
    return jnp.clip(spiked(values, jax.random.fold_in(rng, 3), *heavy), -most, most).astype(kind)


def setup_inputs(seed: int = 0) -> dict:
    keys = jax.random.split(jax.random.key(seed), 17)
    mid = normal_values(keys[0], (STREAM_ITEMS, D), 1.0, 6.0, ((0, 64),))
    out_grad = heavy_noise(keys[1], (STREAM_ITEMS, D), 1.0, 16.0, ((0, 64),), (0, 1, 64, 4.0))
    expert_ids_keys = jax.random.split(jax.random.fold_in(keys[2], 1), STREAM_ITEMS // TOK_DEV)
    expert_ids_turns = jax.random.permutation(jax.random.fold_in(keys[2], 3), STREAM_ITEMS // TOK_DEV)
    expert_ids = jax.vmap(lambda own, number: routed_block(jax.random.fold_in(keys[2], 2), own, number, TOK_DEV, EXPERTS, TOP, CAP, 1))(expert_ids_keys, expert_ids_turns).reshape((STREAM_ITEMS, TOP))
    route_weights = jnp.clip(0.1 + 0.79999997 * jax.random.uniform(keys[3], (STREAM_ITEMS, TOP), jnp.float32) ** steps_of(keys[3], (STREAM_ITEMS, TOP), ((0, 64),), -0.2, 0.2), 0.1, 0.9)
    gate_proj = normal_values(keys[4], (EXPERTS, D, FF), (D // 9) ** -0.5, 0.375, ((0, 64), (2, 4)))
    up_proj = normal_values(keys[5], (EXPERTS, D, FF), (D // 9) ** -0.5, 0.375, ((0, 64), (2, 4)))
    down_proj = normal_values(keys[6], (EXPERTS, FF, D), FF ** -0.5, 0.1875, ((0, 64), (1, 4)))
    out_proj = normal_values(keys[7], (W, D), W ** -0.5, 0.25, ((0, 4),))
    branch_gate = normal_values(keys[8], (STREAM_ITEMS, W), 1.0, 6.0, ((0, 64), (1, 4)))
    conv_out = normal_values(keys[9], (2, STREAM_ITEMS, W), 1.0, 6.0, ((1, 64), (2, 4)))
    prior_state = normal_values(keys[10], (2, STREAM_ITEMS, W), 1.0, 6.0, ((1, 64), (2, 4)), jnp.float32)
    rate_gate_w = normal_values(keys[11], (2, HEADS, HEAD, HEAD), HEAD ** -0.5, 0.75, ((1, 4),))
    input_gate_w = normal_values(keys[12], (2, HEADS, HEAD, HEAD), HEAD ** -0.5, 0.75, ((1, 4),))
    decay_param = draw_decay_param(jax.random.fold_in(keys[16], 71), 0)
    decay_jump = draw_decay_jump(jax.random.fold_in(keys[16], 71), 0)
    conv_taps = normal_values(keys[15], (2, TAPS, W), 0.5, 3.0, ((2, 4),))
    return {"mid": mid, "out_grad": out_grad, "expert_ids": expert_ids, "route_weights": route_weights, "gate_proj": gate_proj, "up_proj": up_proj, "down_proj": down_proj, "out_proj": out_proj, "branch_gate": branch_gate, "conv_out": conv_out, "prior_state": prior_state, "rate_gate_w": rate_gate_w, "input_gate_w": input_gate_w, "decay_param": decay_param, "decay_jump": decay_jump, "conv_taps": conv_taps}


RATE_SCALE = 8.0
CLAMP_LIMIT = 7.0
SHARPNESS = 1.702
NORM_EPSILON = 1e-06
STATE_FLOOR = 0.001
GELU_CUBIC = 0.044715
GELU_SCALE = 0.7978845608028654

def gelu_parts(values):
    inside = GELU_SCALE * (values + GELU_CUBIC * values * values * values)
    tangent = jnp.tanh(inside)
    result = 0.5 * values * (1.0 + tangent)
    slope_value = 0.5 * (1.0 + tangent) + 0.5 * values * (1.0 - tangent * tangent) * GELU_SCALE * (1.0 + 3.0 * GELU_CUBIC * values * values)
    return (result, slope_value)

def adjoint_chain(decay_factors, seeds, backward):

    def advance(incoming, step_pair):
        adjoint_now = step_pair[1] + incoming
        return (step_pair[0] * adjoint_now, adjoint_now)
    start_carry = jnp.zeros(seeds.shape[1:], jnp.float32)
    _, totals = lax.scan(advance, start_carry, (decay_factors, seeds), reverse=backward)
    return totals

def reference(mid, out_grad, expert_ids, route_weights, gate_proj, up_proj, down_proj, out_proj, branch_gate, conv_out, prior_state, rate_gate_w, input_gate_w, decay_param, decay_jump, conv_taps):
    mid_full = mid.astype(jnp.float32)
    inv_rms = lax.rsqrt(lax.optimization_barrier(jnp.mean(mid_full * mid_full, axis=1, keepdims=True)) + NORM_EPSILON)
    normed = mid_full * inv_rms
    normed_b = normed.astype(jnp.bfloat16)
    block_ids = expert_ids.reshape(N_SP, TOK_DEV * TOP)
    onehot = (block_ids[:, :, None] == jnp.arange(EXPERTS, dtype=jnp.int32)[None, None, :]).astype(jnp.int32)
    rank_ids = lax.optimization_barrier(jnp.sum((jnp.cumsum(onehot, axis=1) - onehot) * onehot, axis=2))
    positions = (jnp.arange(N_SP, dtype=jnp.int32)[:, None] * CAP + rank_ids).reshape(-1)
    flat_ids = expert_ids.reshape(-1)
    slot_table = jnp.full((EXPERTS, N_SP * CAP), -1, jnp.int32).at[flat_ids, positions].set(jnp.arange(STREAM_ITEMS * TOP, dtype=jnp.int32))
    route_flat = route_weights.reshape(-1)
    ff_group = FF // N_TP

    def expert_step(running, inputs):
        slot_rows, w_gate, w_up, down_weight = inputs
        filled = slot_rows >= 0
        assign = jnp.where(filled, slot_rows, 0)
        token_ids = assign // TOP
        rows_b = jnp.where(filled[:, None], normed_b[token_ids], jnp.zeros((), jnp.bfloat16))
        weights = jnp.where(filled, route_flat[assign], 0.0)
        grad_b = (out_grad[token_ids].astype(jnp.float32) * weights[:, None]).astype(jnp.bfloat16)
        gate_pre = jnp.dot(rows_b, w_gate, preferred_element_type=jnp.float32)
        up_pre = jnp.dot(rows_b, w_up, preferred_element_type=jnp.float32)
        gate_clamped = jnp.minimum(gate_pre, CLAMP_LIMIT)
        up_clamped = jnp.clip(up_pre, -CLAMP_LIMIT, CLAMP_LIMIT)
        gate_sigmoid = jax.nn.sigmoid(SHARPNESS * gate_clamped)
        swish_value = gate_clamped * gate_sigmoid
        act_b = ((up_clamped + 1.0) * swish_value).astype(jnp.bfloat16)
        act_grad = jnp.dot(grad_b, down_weight.T, preferred_element_type=jnp.float32)
        gate_delta = jnp.where(gate_pre < CLAMP_LIMIT, act_grad * (up_clamped + 1.0) * (gate_sigmoid + SHARPNESS * swish_value * (1.0 - gate_sigmoid)), 0.0).astype(jnp.bfloat16)
        up_delta = jnp.where(jnp.abs(up_pre) < CLAMP_LIMIT, act_grad * swish_value, 0.0).astype(jnp.bfloat16)
        down_grad = jnp.dot(act_b.T, grad_b, preferred_element_type=jnp.float32).astype(jnp.bfloat16)
        gate_grad = jnp.dot(rows_b.T, gate_delta, preferred_element_type=jnp.float32).astype(jnp.bfloat16)
        up_grad = jnp.dot(rows_b.T, up_delta, preferred_element_type=jnp.float32).astype(jnp.bfloat16)
        gate_parts = gate_delta.astype(jnp.float32).reshape(-1, N_TP, ff_group)
        up_parts = up_delta.astype(jnp.float32).reshape(-1, N_TP, ff_group)
        gate_cols = w_gate.astype(jnp.float32).reshape(D, N_TP, ff_group)
        up_cols = w_up.astype(jnp.float32).reshape(D, N_TP, ff_group)
        partials = jnp.einsum('rjf,djf->jrd', gate_parts, gate_cols) + jnp.einsum('rjf,djf->jrd', up_parts, up_cols)
        rounded = lax.optimization_barrier(partials.astype(jnp.bfloat16))
        slot_b = lax.optimization_barrier(jnp.sum(rounded.astype(jnp.float32), axis=0)).astype(jnp.bfloat16)
        running = running.at[token_ids].add(jnp.where(filled[:, None], slot_b.astype(jnp.float32), 0.0))
        return (running, (gate_grad, up_grad, down_grad))
    token_grad, (gate_grads, up_grads, down_grads) = lax.scan(expert_step, jnp.zeros((STREAM_ITEMS, D), jnp.float32), (slot_table, gate_proj, up_proj, down_proj))
    inner_mean = lax.optimization_barrier(jnp.mean(token_grad * normed, axis=1, keepdims=True))
    mid_grad_b = (out_grad.astype(jnp.float32) + inv_rms * (token_grad - normed * inner_mean)).astype(jnp.bfloat16)
    branch_grad = jnp.dot(mid_grad_b, out_proj.T, preferred_element_type=jnp.float32)
    conv_full = conv_out.astype(jnp.float32)
    conv_heads = conv_full.reshape(2, STREAM_ITEMS, HEADS, HEAD)
    rate_gate = jax.nn.sigmoid(jnp.einsum('sthc,shcd->sthd', conv_heads, rate_gate_w.astype(jnp.float32)).reshape(2, STREAM_ITEMS, W))
    input_gate = jax.nn.sigmoid(jnp.einsum('sthc,shcd->sthd', conv_heads, input_gate_w.astype(jnp.float32)).reshape(2, STREAM_ITEMS, W))
    decay_rate = jax.nn.softplus(-decay_param)[:, None, :]
    log_decay = -RATE_SCALE * rate_gate * decay_rate + decay_jump
    decay_factors = jnp.exp(log_decay)
    squared = jnp.exp(2.0 * log_decay)
    norm_factor = jnp.sqrt(STATE_FLOOR - jnp.expm1(2.0 * log_decay))
    drive_term = input_gate * conv_full
    states = decay_factors * prior_state + norm_factor * drive_term
    summed_states = states[0] + states[1]
    gelu_value, gelu_slope = gelu_parts(branch_gate.astype(jnp.float32))
    mixed_b = (summed_states * gelu_value).astype(jnp.bfloat16)
    branch_gate_grad = (branch_grad * summed_states * gelu_slope).astype(jnp.bfloat16)
    state_grad = branch_grad * gelu_value
    adjoint = jnp.stack([adjoint_chain(decay_factors[0], state_grad, True), adjoint_chain(decay_factors[1], state_grad, False)])
    decay_grad = adjoint * (decay_factors * prior_state - drive_term * squared / norm_factor)
    drive_grad = adjoint * norm_factor
    rate_pre = (decay_grad * (-RATE_SCALE * decay_rate) * rate_gate * (1.0 - rate_gate)).astype(jnp.bfloat16)
    input_pre = (drive_grad * conv_full * input_gate * (1.0 - input_gate)).astype(jnp.bfloat16)
    conv_grad = drive_grad * input_gate
    conv_grad = conv_grad + jnp.einsum('sthd,shcd->sthc', rate_pre.astype(jnp.float32).reshape(2, STREAM_ITEMS, HEADS, HEAD), rate_gate_w.astype(jnp.float32)).reshape(2, STREAM_ITEMS, W)
    conv_grad = conv_grad + jnp.einsum('sthd,shcd->sthc', input_pre.astype(jnp.float32).reshape(2, STREAM_ITEMS, HEADS, HEAD), input_gate_w.astype(jnp.float32)).reshape(2, STREAM_ITEMS, W)
    reach = TAPS - 1
    padded = jnp.pad(conv_grad, ((0, 0), (reach, reach), (0, 0)))
    taps_full = conv_taps.astype(jnp.float32)
    input_grad = jnp.zeros((STREAM_ITEMS, W), jnp.float32)
    for tap_index in range(TAPS):
        upper = 2 * reach - tap_index
        input_grad = input_grad + taps_full[0, tap_index] * padded[0, upper:upper + STREAM_ITEMS] + taps_full[1, tap_index] * padded[1, tap_index:tap_index + STREAM_ITEMS]
    proj_grad_t = jnp.dot(mid_grad_b.T, mixed_b, preferred_element_type=jnp.float32)
    return (gate_grads, up_grads, down_grads, proj_grad_t, input_grad.astype(jnp.bfloat16), branch_gate_grad)
```

```python
import functools
import math

import jax
import jax.numpy as jnp
from jax import lax
from jax.experimental import pallas as pl
from jax.experimental.pallas import tpu as pltpu
from jax.sharding import PartitionSpec as P

RATE_SCALE = 8.0
CLAMP_LIMIT = 7.0
SHARPNESS = 1.702
NORM_EPSILON = 1e-06
STATE_FLOOR = 0.001
GELU_CUBIC = 0.044715
GELU_SCALE = 0.7978845608028654

F32 = jnp.float32
BF16 = jnp.bfloat16
MESH = pl.DeviceIdType.MESH


def dot(a, b, ca=1, cb=0):
    return lax.dot_general(a, b, (((ca,), (cb,)), ((), ())), preferred_element_type=F32)


def gelu_parts(values):
    inside = GELU_SCALE * (values + GELU_CUBIC * values * values * values)
    tangent = jnp.tanh(inside)
    result = 0.5 * values * (1.0 + tangent)
    slope_value = 0.5 * (1.0 + tangent) + 0.5 * values * (1.0 - tangent * tangent) * GELU_SCALE * (
        1.0 + 3.0 * GELU_CUBIC * values * values
    )
    return (result, slope_value)


def less_one(x):
    series = jnp.ones_like(x)
    for n in range(8, 1, -1):
        series = 1.0 + x * (1.0 / n) * series
    return jnp.where(jnp.abs(x) < 0.35, x * series, jnp.exp(x) - 1.0)


class Sizes:
    def __init__(self, tok, d, ns, ny, room, ffl, ch):
        self.tok, self.d, self.ns, self.ny, self.room = tok, d, ns, ny, room
        self.ffl, self.ch = ffl, ch
        self.nj = math.isqrt(ns)
        self.nz = ns // self.nj
        self.bl = self.nj * room
        self.sl = ns * room
        self.hs = self.sl // 2
        self.ht = tok // 2
        self.nk = 2 * ny
        self.c = d // self.nk
        self.r = d // ns
        self.steps = [1 << i for i in range((tok - 1).bit_length())]


class Book:
    def __init__(self):
        self.n = 0

    def take(self, count):
        at, self.n = self.n, self.n + count
        return at


def layout(s):
    b = Book()
    return dict(
        s1=b.take(4 * s.nz), s2=b.take(4 * s.nj), y=b.take(16), rs=b.take(12),
        sa=b.take(2 * s.nj), sb=b.take(2 * s.nz), tg=b.take(8), cj=b.take(s.nj), cz=b.take(s.nz),
        halo=b.take(2), pj=b.take(s.nj), pz=b.take(s.nz),
    ), b.n


def kernel(s, *refs):
    (mid, og, idw, wg_hbm, wu_hbm, wd_hbm, outp, bgate, conv, prior, rgw, igw, dpar, djump, taps,
     gg_hbm, ug_hbm, dg_hbm, proj_out, ig_out, bgg_out,
     wgu, wd, inv_s, sel, gate, perm, s1, r1, s2, r2, xa, gu, ag, delta, act,
     p2, rt2, rb2, sp1, sm1, ft, fm, fo, rl, rr, s3, r3, s4, r4, tg, gg, ug, dg, mg,
     bd, gel, sslope, mixed, pst, prod, k1, k2, k3, dec, adj, cjs, cjr, czs, czr,
     cgr, hs_s, hr_s, pf, pr, ps2, pr2,
     ssem, rsem, lsem) = refs
    at, _ = layout(s)
    sp = lax.axis_index("sp")
    y = lax.axis_index("tp")
    z, j = sp // s.nj, sp % s.nj
    up, down = (y + 1) % s.ny, (y + s.ny - 1) % s.ny
    opp = (y + 2) % s.ny
    nxt, prv = (sp + 1) % s.ns, (sp + s.ns - 1) % s.ns

    def on_sp(i):
        return {"sp": i}

    def on_tp(i):
        return {"tp": i}

    def in_line(i):
        return {"sp": i * s.nj + j}

    def in_plane(i):
        return {"sp": z * s.nj + i}

    started = []

    def send(src, dst, si, ri, dev):
        cp = pltpu.make_async_remote_copy(
            src_ref=src, dst_ref=dst, send_sem=ssem.at[si], recv_sem=rsem.at[ri],
            device_id=dev, device_id_type=MESH)
        cp.start()
        started.append(cp)

    def recv(dst, ri):
        pltpu.make_async_remote_copy(
            src_ref=dst, dst_ref=dst, send_sem=ssem.at[0], recv_sem=rsem.at[ri],
            device_id=on_tp(up), device_id_type=MESH).wait_recv()

    def orders(n):
        half = n // 2
        out = [half]
        for d in range(half - 1, 0, -1):
            out += [d, n - d]
        return out if n > 2 else [1]

    loads = [
        pltpu.make_async_copy(wg_hbm, wgu.at[:, pl.ds(0, s.ffl)], lsem.at[0]),
        pltpu.make_async_copy(wu_hbm, wgu.at[:, pl.ds(s.ffl, s.ffl)], lsem.at[1]),
        pltpu.make_async_copy(wd_hbm, wd, lsem.at[2]),
    ]

    barrier = pltpu.get_barrier_semaphore()
    partners = [in_line((z + d) % s.nz) for d in range(1, s.nz)]
    partners += [in_plane((j + d) % s.nj) for d in range(1, s.nj)]
    partners += [on_tp(up), on_tp(down), on_sp(nxt), on_sp(prv)]
    for dev in partners:
        pl.semaphore_signal(barrier, inc=1, device_id=dev, device_id_type=MESH)
    for cp in loads:
        cp.start()

    squares = jnp.zeros((s.tok, s.c), F32)
    for k in range(s.nk):
        part = mid[:, k * s.c:(k + 1) * s.c].astype(F32)
        squares = squares + part * part
    inv = lax.rsqrt(jnp.sum(squares, axis=1, keepdims=True) * (1.0 / s.d) + NORM_EPSILON)
    inv_s[...] = jnp.broadcast_to(inv, inv_s.shape)
    ids0, ids1 = idw[0:1, :], idw[1:2, :]
    w0, w1 = idw[2:3, :], idw[3:4, :]
    names = lax.broadcasted_iota(jnp.int32, (s.ns, s.tok), 0).astype(F32)
    hit0, hit1 = names == ids0, names == ids1
    hits = jnp.where(hit0 | hit1, 1.0, 0.0)
    before = jnp.where(
        lax.broadcasted_iota(jnp.int32, (s.tok, s.tok), 0)
        < lax.broadcasted_iota(jnp.int32, (s.tok, s.tok), 1), 1.0, 0.0)
    counts = dot(hits.astype(BF16), before.astype(BF16))
    slot0 = ids0 * s.room + jnp.sum(jnp.where(hit0, counts, 0.0), axis=0, keepdims=True)
    slot1 = ids1 * s.room + jnp.sum(jnp.where(hit1, counts, 0.0), axis=0, keepdims=True)
    rows = lax.broadcasted_iota(jnp.int32, (s.sl, s.tok), 0).astype(F32)
    own0, own1 = rows == slot0, rows == slot1
    sel[...] = jnp.where(own0 | own1, 1.0, 0.0).astype(BF16)
    gate[...] = jnp.sum(jnp.where(own0, w0, 0.0) + jnp.where(own1, w1, 0.0), axis=1, keepdims=True)
    line = lax.broadcasted_iota(jnp.int32, (s.sl, 1), 0).astype(F32)
    outer = jnp.floor((line + 0.5) * (1.0 / s.bl))
    rest = line - outer * s.bl
    inner = jnp.floor((rest + 0.5) * (1.0 / s.room))
    source = inner * s.bl + outer * s.room + (rest - inner * s.room)
    perm[...] = jnp.where(
        lax.broadcasted_iota(jnp.int32, (s.sl, s.sl), 1).astype(F32) == source, 1.0, 0.0
    ).astype(BF16)

    def quarter(c):
        return pl.ds(pl.multiple_of((y * 2 + c) * s.c, s.c), s.c)

    def blocks(x):
        return x.reshape(-1, s.bl, s.c).astype(BF16)

    def flat(ref):
        return ref.astype(F32).reshape(s.sl, s.c).astype(BF16)

    for q in range(4):
        c, kind = q // 2, q % 2
        if kind == 0:
            piece = (mid[:, quarter(c)].astype(F32) * inv_s[:, 0:1]).astype(BF16)
            value = dot(sel[...], piece)
        else:
            value = dot(sel[...], og[:, quarter(c)]) * gate[...]
        s1[q] = blocks(value)
        if q == 0:
            pl.semaphore_wait(barrier, len(partners))
        for d in orders(s.nz):
            zd = (z + d) % s.nz
            send(s1.at[q, zd], r1.at[q, z], at["s1"] + q * s.nz + zd, at["s1"] + q * s.nz + z, in_line(zd))
        r1[q, z] = s1[q, z]

    for side in range(2):
        for n, w in enumerate((rgw, igw)):
            zero = jnp.zeros((w.shape[2], w.shape[3]), F32)
            top = jnp.concatenate([w[side, 0].astype(F32), zero], axis=1)
            low = jnp.concatenate([zero, w[side, 1].astype(F32)], axis=1)
            bd[2 * side + n] = jnp.concatenate([top, low], axis=0).astype(BF16)
    gelu_value, gelu_slope = gelu_parts(bgate[...].astype(F32))
    gel[...] = gelu_value
    both_states = jnp.zeros((s.tok, s.ch), F32)
    time = lax.broadcasted_iota(jnp.int32, (s.tok, s.ch), 0)
    for side in range(2):
        conv_b = conv[side]
        conv_f = conv_b.astype(F32)
        rate_gate = jax.nn.sigmoid(dot(conv_b, bd[2 * side]))
        input_gate = jax.nn.sigmoid(dot(conv_b, bd[2 * side + 1]))
        decay_rate = dpar[side:side + 1, :]
        log_decay = -RATE_SCALE * rate_gate * decay_rate + djump[side]
        factors = jnp.exp(log_decay)
        squared = jnp.exp(2.0 * log_decay)
        norm_factor = jnp.sqrt(STATE_FLOOR - less_one(2.0 * log_decay))
        drive = input_gate * conv_f
        carried = factors * prior[side]
        both_states = both_states + (carried + norm_factor * drive)
        k1[side] = (carried - drive * squared / norm_factor) * (
            -RATE_SCALE * decay_rate) * rate_gate * (1.0 - rate_gate)
        k2[side] = norm_factor * conv_f * input_gate * (1.0 - input_gate)
        k3[side] = norm_factor * input_gate
        if side == 0:
            link = jnp.where(time < s.tok - 1, pltpu.roll(factors, s.tok - 1, 0), 1.0)
            dec[0:1, :] = factors[0:1, :]
        else:
            link = jnp.where(time > 0, pltpu.roll(factors, 1, 0), 1.0)
            dec[1:2, :] = factors[s.tok - 1:s.tok, :]
        for n, d in enumerate(s.steps):
            inside = time < s.tok - d if side == 0 else time >= d
            pst[side, n] = jnp.where(inside, link, 0.0)
            shift = s.tok - d if side == 0 else d
            link = jnp.where(inside, link * pltpu.roll(link, shift, 0), link)
        prod[side] = link
    sslope[...] = both_states * gelu_slope
    mixed[...] = (both_states * gelu_value).astype(BF16)

    def turn(q):
        for d in range(1, s.nz):
            zs = (z + d) % s.nz
            recv(r1.at[q, zs], at["s1"] + q * s.nz + zs)
        s2[q] = blocks(dot(perm[...], flat(r1[q])))
        for d in orders(s.nj):
            jd = (j + d) % s.nj
            send(s2.at[q, jd], r2.at[q, j], at["s2"] + q * s.nj + jd, at["s2"] + q * s.nj + j, in_plane(jd))
        r2[q, j] = s2[q, j]

    top, low = pl.ds(0, s.hs), pl.ds(s.hs, s.hs)

    def spread(q):
        c, kind = q // 2, q % 2
        for d in range(1, s.nj):
            js = (j + d) % s.nj
            recv(r2.at[q, js], at["s2"] + q * s.nj + js)
        xa[kind, y * 2 + c] = flat(r2[q])
        ref = xa.at[kind, y * 2 + c]
        n = at["y"] + 4 * q
        send(ref, ref, n, n, on_tp(up))
        send(ref, ref, n + 1, n + 1, on_tp(down))

    def relay(q):
        c, kind = q // 2, q % 2
        n = at["y"] + 4 * q
        ref = xa.at[kind, down * 2 + c]
        recv(ref, n)
        send(ref.at[top], ref.at[top], n + 2, n + 2, on_tp(up))
        ref = xa.at[kind, up * 2 + c]
        recv(ref, n + 1)
        send(ref.at[low], ref.at[low], n + 3, n + 3, on_tp(down))

    def weights_of(k):
        return wgu[pl.ds(pl.multiple_of(k * s.c, s.c), s.c), :]

    def take(q):
        c, kind = q // 2, q % 2
        n = at["y"] + 4 * q
        far = xa.at[kind, opp * 2 + c]
        recv(far.at[top], n + 2)
        recv(far.at[low], n + 3)
        for i in range(s.ny):
            k = i * 2 + c
            if kind == 0:
                value = dot(xa[0, k], wgu[k * s.c:(k + 1) * s.c, :])
                total = gu
            else:
                value = dot(xa[1, k], wd[:, k * s.c:(k + 1) * s.c], 1, 1)
                total = ag
            if c == 0 and i == 0:
                total[...] = value
            else:
                total[...] += value

    turn(0)
    turn(1)
    spread(0)
    turn(2)
    spread(1)
    relay(0)
    turn(3)
    spread(2)
    relay(1)
    for cp in loads:
        cp.wait()
    take(0)
    spread(3)
    relay(2)
    take(1)
    relay(3)
    take(2)
    take(3)

    gate_pre, up_pre = gu[:, :s.ffl], gu[:, s.ffl:]
    act_grad = ag[...]
    gate_clamped = jnp.minimum(gate_pre, CLAMP_LIMIT)
    up_clamped = jnp.clip(up_pre, -CLAMP_LIMIT, CLAMP_LIMIT)
    gate_sigmoid = jax.nn.sigmoid(SHARPNESS * gate_clamped)
    swish_value = gate_clamped * gate_sigmoid
    act[...] = ((up_clamped + 1.0) * swish_value).astype(BF16)
    delta[:, :s.ffl] = jnp.where(
        gate_pre < CLAMP_LIMIT,
        act_grad * (up_clamped + 1.0)
        * (gate_sigmoid + SHARPNESS * swish_value * (1.0 - gate_sigmoid)), 0.0).astype(BF16)
    delta[:, s.ffl:] = jnp.where(
        jnp.abs(up_pre) < CLAMP_LIMIT, act_grad * swish_value, 0.0).astype(BF16)

    def partial(owner, c):
        return dot(delta[...], weights_of(owner * 2 + c), 1, 1)

    for c in range(2):
        n = at["rs"] + 6 * c
        p2[c] = partial(opp, c).astype(BF16)
        send(p2.at[c, top], rt2.at[c], n, n, on_tp(up))
        send(p2.at[c, low], rb2.at[c], n + 1, n + 1, on_tp(down))
    for c in range(2):
        n = at["rs"] + 6 * c
        value = partial(up, c)
        sp1[c, s.hs:, :] = value[s.hs:].astype(BF16)
        ft[c] = value[:s.hs]
        send(sp1.at[c, low], rl.at[c, low], n + 2, n + 2, on_tp(up))
        value = partial(down, c)
        sm1[c, :s.hs, :] = value[:s.hs].astype(BF16)
        fm[c] = value[s.hs:]
        send(sm1.at[c, top], rr.at[c, top], n + 3, n + 3, on_tp(down))

    def pass_on(c):
        n = at["rs"] + 6 * c
        recv(rt2.at[c], n)
        sp1[c, :s.hs, :] = (ft[c] + rt2[c].astype(F32)).astype(BF16)
        send(sp1.at[c, top], rl.at[c, top], n + 4, n + 4, on_tp(up))
        recv(rb2.at[c], n + 1)
        sm1[c, s.hs:, :] = (fm[c] + rb2[c].astype(F32)).astype(BF16)
        send(sm1.at[c, low], rr.at[c, low], n + 5, n + 5, on_tp(down))

    pass_on(0)
    for c in range(2):
        fo[c] = partial(y, c)
    pass_on(1)

    @pl.loop(0, s.nk)
    def _(k):
        value = dot(xa[0, k], delta[...], 0, 0)
        where = pl.ds(pl.multiple_of(k * s.c, s.c), s.c)
        gg[where, :] = value[:, :s.ffl].astype(BF16)
        ug[where, :] = value[:, s.ffl:].astype(BF16)

    stores = [
        pltpu.make_async_copy(gg, gg_hbm, lsem.at[3]),
        pltpu.make_async_copy(ug, ug_hbm, lsem.at[4]),
        pltpu.make_async_copy(dg, dg_hbm, lsem.at[5]),
    ]
    stores[0].start()
    stores[1].start()

    def give(c):
        n = at["rs"] + 6 * c
        recv(rl.at[c, low], n + 2)
        recv(rr.at[c, top], n + 3)
        recv(rl.at[c, top], n + 4)
        recv(rr.at[c, low], n + 5)
        s3[c] = blocks(fo[c] + rl[c].astype(F32) + rr[c].astype(F32))
        for d in orders(s.nj):
            jd = (j + d) % s.nj
            send(s3.at[c, jd], r3.at[c, j], at["sa"] + c * s.nj + jd, at["sa"] + c * s.nj + j, in_plane(jd))
        r3[c, j] = s3[c, j]

    def turn_back(c):
        for d in range(1, s.nj):
            js = (j + d) % s.nj
            recv(r3.at[c, js], at["sa"] + c * s.nj + js)
        s4[c] = blocks(dot(perm[...], flat(r3[c])))
        for d in orders(s.nz):
            zd = (z + d) % s.nz
            send(s4.at[c, zd], r4.at[c, z], at["sb"] + c * s.nz + zd, at["sb"] + c * s.nz + z, in_line(zd))
        r4[c, z] = s4[c, z]

    ttop, tlow = pl.ds(0, s.ht), pl.ds(s.ht, s.ht)

    def combine(c):
        for d in range(1, s.nz):
            zs = (z + d) % s.nz
            recv(r4.at[c, zs], at["sb"] + c * s.nz + zs)
        tg[y * 2 + c] = dot(sel[...], flat(r4[c]), 0, 0).astype(BF16)
        ref = tg.at[y * 2 + c]
        n = at["tg"] + 4 * c
        send(ref, ref, n, n, on_tp(up))
        send(ref, ref, n + 1, n + 1, on_tp(down))

    def tg_relay(c):
        n = at["tg"] + 4 * c
        ref = tg.at[down * 2 + c]
        recv(ref, n)
        send(ref.at[ttop], ref.at[ttop], n + 2, n + 2, on_tp(up))
        ref = tg.at[up * 2 + c]
        recv(ref, n + 1)
        send(ref.at[tlow], ref.at[tlow], n + 3, n + 3, on_tp(down))

    def tg_take(c):
        n = at["tg"] + 4 * c
        ref = tg.at[opp * 2 + c]
        recv(ref.at[ttop], n + 2)
        recv(ref.at[tlow], n + 3)

    give(0)
    give(1)
    turn_back(0)

    @pl.loop(0, s.nk)
    def _(k):
        value = dot(act[...], xa[1, k], 0, 0)
        dg[:, pl.ds(pl.multiple_of(k * s.c, s.c), s.c)] = value.astype(BF16)

    stores[2].start()
    turn_back(1)
    combine(0)
    tg_relay(0)
    combine(1)
    tg_take(0)
    tg_relay(1)
    tg_take(1)

    inv_col = inv_s[:, 0:1]
    prods = jnp.zeros((s.tok, s.c), F32)
    for k in range(s.nk):
        part = mid[:, k * s.c:(k + 1) * s.c].astype(F32) * inv_col
        prods = prods + tg[k].astype(F32) * part
    inner_mean = jnp.sum(prods, axis=1, keepdims=True) * (1.0 / s.d)
    branch_grad = jnp.zeros((s.tok, s.ch), F32)
    for k in range(s.nk):
        cols = slice(k * s.c, (k + 1) * s.c)
        part = mid[:, cols].astype(F32) * inv_col
        value = (og[:, cols].astype(F32) + inv_col * (tg[k].astype(F32) - part * inner_mean)).astype(BF16)
        mg[k] = value
        branch_grad = branch_grad + dot(value, outp[:, cols], 1, 1)
    bgg_out[...] = (branch_grad * sslope[...]).astype(BF16)
    state_grad = branch_grad * gel[...]

    for side in range(2):
        chain = state_grad
        for n, d in enumerate(s.steps):
            shift = s.tok - d if side == 0 else d
            chain = chain + pst[side, n] * pltpu.roll(chain, shift, 0)
        adj[side] = chain
        edge = slice(0, 1) if side == 0 else slice(s.tok - 1, s.tok)
        cjs[2 * side:2 * side + 1, :] = dec[side:side + 1, :] * prod[side, edge, :]
        cjs[2 * side + 1:2 * side + 2, :] = dec[side:side + 1, :] * chain[edge]
    cjr[j] = cjs[...]
    for d in orders(s.nj):
        jd = (j + d) % s.nj
        send(cjs, cjr.at[j], at["cj"] + jd, at["cj"] + j, in_plane(jd))

    def project(k):
        value = dot(mg[k], mixed[...], 0, 0).astype(BF16)
        if s.c == s.nj * s.r:
            pf[k] = value.reshape(s.nj, s.r, s.ch)
        else:
            a = k * s.c
            pf[a // (s.nj * s.r), (a // s.r) % s.nj, pl.ds(a % s.r, s.c), :] = value

    for k in range(s.nk):
        project(k)
    for d in orders(s.nj):
        jd = (j + d) % s.nj
        send(pf.at[:, jd], pr.at[j], at["pj"] + jd, at["pj"] + j, in_plane(jd))
    pr[j] = pf[:, j]

    for d in range(1, s.nj):
        js = (j + d) % s.nj
        recv(cjr.at[js], at["cj"] + js)

    def compose(got, count, place):
        one, nil = jnp.ones((1, s.ch), F32), jnp.zeros((1, s.ch), F32)
        later, earlier = (one, nil), (one, nil)
        whole_l, whole_e = (one, nil), (one, nil)
        for i in range(count - 1, -1, -1):
            a, b = got[i, 0:1, :], got[i, 1:2, :]
            whole_l = (whole_l[0] * a, a * whole_l[1] + b)
            keep = i > place
            later = (jnp.where(keep, whole_l[0], later[0]), jnp.where(keep, whole_l[1], later[1]))
        for i in range(count):
            a, b = got[i, 2:3, :], got[i, 3:4, :]
            whole_e = (whole_e[0] * a, a * whole_e[1] + b)
            keep = i < place
            earlier = (jnp.where(keep, whole_e[0], earlier[0]), jnp.where(keep, whole_e[1], earlier[1]))
        return later, earlier, whole_l, whole_e

    later_j, earlier_j, whole_l, whole_e = compose(cjr, s.nj, j)
    czs[0:1, :], czs[1:2, :] = whole_l
    czs[2:3, :], czs[3:4, :] = whole_e
    czr[z] = czs[...]
    for d in orders(s.nz):
        zd = (z + d) % s.nz
        send(czs, czr.at[z], at["cz"] + zd, at["cz"] + z, in_line(zd))

    for d in range(1, s.nj):
        js = (j + d) % s.nj
        recv(pr.at[js], at["pj"] + js)
    total = pr[0].astype(F32)
    for i in range(1, s.nj):
        total = total + pr[i].astype(F32)
    ps2[...] = total.astype(BF16)
    pr2[z] = ps2[z]

    for d in range(1, s.nz):
        zs = (z + d) % s.nz
        recv(czr.at[zs], at["cz"] + zs)
    for d in orders(s.nz):
        zd = (z + d) % s.nz
        send(ps2.at[zd], pr2.at[z], at["pz"] + zd, at["pz"] + z, in_line(zd))
    later_z, earlier_z, _, _ = compose(czr, s.nz, z)
    inflow = (later_j[0] * later_z[1] + later_j[1], earlier_j[0] * earlier_z[1] + earlier_j[1])

    for side in range(2):
        adjoint = adj[side] + prod[side] * inflow[side]
        rate_pre = (adjoint * k1[side]).astype(BF16)
        input_pre = (adjoint * k2[side]).astype(BF16)
        cgr[side] = (adjoint * k3[side] + dot(rate_pre, bd[2 * side], 1, 1)
                     + dot(input_pre, bd[2 * side + 1], 1, 1))
    hs_s[0] = cgr[0, 0:8, :]
    hs_s[1] = cgr[1, s.tok - 8:s.tok, :]
    send(hs_s.at[0], hr_s.at[0], at["halo"], at["halo"], on_sp(prv))
    send(hs_s.at[1], hr_s.at[1], at["halo"] + 1, at["halo"] + 1, on_sp(nxt))
    recv(hr_s.at[0], at["halo"])
    recv(hr_s.at[1], at["halo"] + 1)
    after = jnp.where(sp < s.ns - 1, hr_s[0], 0.0)
    ahead = jnp.where(sp > 0, hr_s[1], 0.0)
    ext0 = jnp.concatenate([cgr[0], after], axis=0)
    ext1 = jnp.concatenate([ahead, cgr[1]], axis=0)
    reach = taps.shape[1] - 1
    tap = taps[...].astype(F32)
    result = jnp.zeros((s.tok, s.ch), F32)
    for t in range(reach + 1):
        off = reach - t
        result = (result + tap[0, t:t + 1, :] * ext0[off:off + s.tok]
                  + tap[1, t:t + 1, :] * ext1[8 - off:8 - off + s.tok])
    ig_out[...] = result.astype(BF16)

    for d in range(1, s.nz):
        zs = (z + d) % s.nz
        recv(pr2.at[zs], at["pz"] + zs)
    total = pr2[0].astype(F32)
    for i in range(1, s.nz):
        total = total + pr2[i].astype(F32)
    proj_out[...] = total

    for cp in stores:
        cp.wait()
    for cp in started:
        cp.wait_send()


def on_device(mid, out_grad, expert_ids, route_weights, gate_proj, up_proj, down_proj, out_proj,
              branch_gate, conv_out, prior_state, rate_gate_w, input_gate_w, decay_param,
              decay_jump, conv_taps):
    tok, d = mid.shape
    ns, ny = lax.axis_size("sp"), lax.axis_size("tp")
    room = 3 * expert_ids.shape[1] * tok // (2 * ns)
    ffl, ch = gate_proj.shape[2], out_proj.shape[0]
    s = Sizes(tok, d, ns, ny, room, ffl, ch)
    idw = jnp.concatenate([expert_ids.astype(F32).T, route_weights.T], axis=0)
    decay_rate = jax.nn.softplus(-decay_param)
    _, count = layout(s)
    vm, hbm = pl.BlockSpec(memory_space=pltpu.VMEM), pl.BlockSpec(memory_space=pl.ANY)
    nst = len(s.steps)

    def b(*shape):
        return pltpu.VMEM(shape, BF16)

    def f(*shape):
        return pltpu.VMEM(shape, F32)

    scratch = [
        b(d, 2 * ffl), b(ffl, d), f(tok, 128), b(s.sl, tok), f(s.sl, 1), b(s.sl, s.sl),
        b(4, s.nz, s.bl, s.c), b(4, s.nz, s.bl, s.c), b(4, s.nj, s.bl, s.c), b(4, s.nj, s.bl, s.c),
        b(2, s.nk, s.sl, s.c), f(s.sl, 2 * ffl), f(s.sl, ffl), b(s.sl, 2 * ffl), b(s.sl, ffl),
        b(2, s.sl, s.c), b(2, s.hs, s.c), b(2, s.hs, s.c), b(2, s.sl, s.c), b(2, s.sl, s.c),
        f(2, s.hs, s.c), f(2, s.hs, s.c), f(2, s.sl, s.c), b(2, s.sl, s.c), b(2, s.sl, s.c),
        b(2, s.nj, s.bl, s.c), b(2, s.nj, s.bl, s.c), b(2, s.nz, s.bl, s.c), b(2, s.nz, s.bl, s.c),
        b(s.nk, tok, s.c), b(d, ffl), b(d, ffl), b(ffl, d), b(s.nk, tok, s.c),
        b(4, ch, ch), f(tok, ch), f(tok, ch), b(tok, ch), f(2, nst, tok, ch), f(2, tok, ch),
        f(2, tok, ch), f(2, tok, ch), f(2, tok, ch), f(2, ch), f(2, tok, ch),
        f(4, ch), f(s.nj, 4, ch), f(4, ch), f(s.nz, 4, ch),
        f(2, tok, ch), f(2, 8, ch), f(2, 8, ch),
        b(s.nz, s.nj, s.r, ch), b(s.nj, s.nz, s.r, ch), b(s.nz, s.r, ch), b(s.nz, s.r, ch),
        pltpu.SemaphoreType.DMA((count,)), pltpu.SemaphoreType.DMA((count,)),
        pltpu.SemaphoreType.DMA((6,)),
    ]
    shape = jax.ShapeDtypeStruct
    outs = pl.pallas_call(
        functools.partial(kernel, s),
        out_shape=(shape((d, ffl), BF16), shape((d, ffl), BF16), shape((ffl, d), BF16),
                   shape((s.r, ch), F32), shape((tok, ch), BF16), shape((tok, ch), BF16)),
        in_specs=[vm, vm, vm, hbm, hbm, hbm] + [vm] * 9,
        out_specs=(hbm, hbm, hbm, vm, vm, vm),
        scratch_shapes=scratch,
        compiler_params=pltpu.CompilerParams(
            collective_id=0, has_side_effects=True, vmem_limit_bytes=60 * 1024 * 1024),
        name="step",
    )(mid, out_grad, idw, gate_proj[0], up_proj[0], down_proj[0], out_proj, branch_gate, conv_out,
      prior_state, rate_gate_w, input_gate_w, decay_rate, decay_jump, conv_taps)
    gg, ug, dg, proj, ig, bgg = outs
    return gg[None], ug[None], dg[None], proj, ig, bgg


def solution(mesh):
    in_specs = (
        P("sp", None), P("sp", None), P("sp", None), P("sp", None),
        P("sp", None, "tp"), P("sp", None, "tp"), P("sp", "tp", None), P("tp", None),
        P("sp", "tp"), P(None, "sp", "tp"), P(None, "sp", "tp"), P(None, "tp", None, None),
        P(None, "tp", None, None), P(None, "tp"), P(None, "sp", "tp"), P(None, None, "tp"),
    )
    out_specs = (
        P("sp", None, "tp"), P("sp", None, "tp"), P("sp", "tp", None),
        P("sp", "tp"), P("sp", "tp"), P("sp", "tp"),
    )
    return jax.shard_map(
        on_device, mesh=mesh, in_specs=in_specs, out_specs=out_specs, check_vma=False
    )
```

```python
import functools
import math

import jax
import jax.numpy as jnp
from jax import lax
from jax.experimental import pallas as pl
from jax.experimental.pallas import tpu as pltpu
from jax.sharding import PartitionSpec as P

RATE_SCALE = 8.0
CLAMP_LIMIT = 7.0
SHARPNESS = 1.702
NORM_EPSILON = 1e-06
STATE_FLOOR = 0.001
GELU_CUBIC = 0.044715
GELU_SCALE = 0.7978845608028654

F32 = jnp.float32
BF16 = jnp.bfloat16
MESH = pl.DeviceIdType.MESH


def dot(a, b, ca=1, cb=0):
    return lax.dot_general(a, b, (((ca,), (cb,)), ((), ())), preferred_element_type=F32)


def gelu_parts(values):
    inside = GELU_SCALE * (values + GELU_CUBIC * values * values * values)
    tangent = jnp.tanh(inside)
    result = 0.5 * values * (1.0 + tangent)
    slope_value = 0.5 * (1.0 + tangent) + 0.5 * values * (1.0 - tangent * tangent) * GELU_SCALE * (
        1.0 + 3.0 * GELU_CUBIC * values * values
    )
    return (result, slope_value)


def less_one(x):
    series = jnp.ones_like(x)
    for n in range(8, 1, -1):
        series = 1.0 + x * (1.0 / n) * series
    return jnp.where(jnp.abs(x) < 0.35, x * series, jnp.exp(x) - 1.0)


def softplus_of_minus(x):
    return jnp.maximum(-x, 0.0) + jnp.log1p(jnp.exp(-jnp.abs(x)))


class Sizes:
    def __init__(self, tok, d, ns, ny, room, ffl, ch):
        self.tok, self.d, self.ns, self.ny, self.room = tok, d, ns, ny, room
        self.ffl, self.ch = ffl, ch
        self.nj = math.isqrt(ns)
        self.nz = ns // self.nj
        self.bl = self.nj * room
        self.sl = ns * room
        self.hs = self.sl // 2
        self.ht = tok // 2
        self.nk = 2 * ny
        self.c = d // self.nk
        self.w = self.c // 2
        self.via = 7
        self.nq = self.via + ny
        self.r = d // ns
        self.steps = [1 << i for i in range((tok - 1).bit_length())]


class Book:
    def __init__(self):
        self.n = 0

    def take(self, count):
        at, self.n = self.n, self.n + count
        return at


def layout(s):
    b, g = Book(), Book()
    arrivals = dict(
        s1=b.take(s.nq), s2=b.take(s.nq), y=b.take(3 * s.via), rs=b.take(16), sa=b.take(4),
        sb=b.take(4), tg=b.take(1), cm=b.take(1), ks=b.take(1), adj=b.take(1), pj=b.take(s.nz),
        pz=b.take(1),
    )
    groups = {name: g.take(1) for name in (
        "s1", "s2", "yu", "yd", "yr", "rs", "sa", "sb", "tg", "cm", "ks", "adj", "pj", "pz")}
    return arrivals, b.n, groups, g.n


def kernel(s, *refs):
    (mid_h, og_h, ids_h, rw_h, wg_hbm, wu_hbm, wd_hbm, outp_h, bgate_h, conv_h, prior_h, rgw_h,
     igw_h, dpar_h, djump_h, taps_h,
     gg_o, ug_o, dg_o, proj_o, ig_o, bgg_o,
     gg, ug, dg, proj_out, ig_out, bgg_out,
     mid, og, ids, rw, outp, bgate, conv, prior, rgw, igw, dpar, djump, taps,
     wgu, wd, inv_s, sel, gate, perm, s1, r1, s2, r2, xa, gu, ag, delta, act,
     p2, rt2, rb2, sp1, sm1, ft, fm, fo, rl, rr, s3, r3, s4, r4, tg,
     bd, gel, sslope, mixed, pst, ks, dec, adj, cms, cmr,
     cgr, pf, pr, ps2, pr2,
     ssem, rsem, lsem) = refs
    at, _, out, _ = layout(s)
    sp = lax.axis_index("sp")
    y = lax.axis_index("tp")
    z, j = sp // s.nj, sp % s.nj
    up, down = (y + 1) % s.ny, (y + s.ny - 1) % s.ny
    opp = (y + 2) % s.ny
    nxt, prv = (sp + 1) % s.ns, (sp + s.ns - 1) % s.ns

    def on_sp(i):
        return {"sp": i}

    def on_tp(i):
        return {"tp": i}

    def in_line(i):
        return {"sp": i * s.nj + j}

    def in_plane(i):
        return {"sp": z * s.nj + i}

    def send(src, dst, group, ri, dev):
        pltpu.make_async_remote_copy(
            src_ref=src, dst_ref=dst, send_sem=ssem.at[out[group]], recv_sem=rsem.at[ri],
            device_id=dev, device_id_type=MESH).start()

    def all_of(ref, group, ri):
        return pltpu.make_async_remote_copy(
            src_ref=ref, dst_ref=ref, send_sem=ssem.at[out[group]], recv_sem=rsem.at[ri],
            device_id=on_tp(up), device_id_type=MESH)

    def recv(ref, ri):
        all_of(ref, "s1", ri).wait_recv()

    def sent(ref, group):
        all_of(ref, group, 0).wait_send()

    def orders(n):
        half = n // 2
        out = [half]
        for d in range(half - 1, 0, -1):
            out += [d, n - d]
        return out if n > 2 else [1]

    def fetch(n, src, dst):
        cp = pltpu.make_async_copy(src, dst, lsem.at[n])
        cp.start()
        return cp

    barrier = pltpu.get_barrier_semaphore()
    partners = [in_line((z + d) % s.nz) for d in range(1, s.nz)]
    partners += [in_plane((j + d) % s.nj) for d in range(1, s.nj)]
    partners += [on_tp(up), on_tp(down), on_sp(nxt), on_sp(prv)]
    for dev in partners:
        pl.semaphore_signal(barrier, inc=1, device_id=dev, device_id_type=MESH)
    first = [fetch(0, ids_h, ids), fetch(1, rw_h, rw), fetch(2, mid_h, mid), fetch(3, og_h, og)]
    second = [fetch(n + 4, src, dst) for n, (src, dst) in enumerate((
        (bgate_h, bgate), (conv_h, conv), (prior_h, prior), (rgw_h, rgw), (igw_h, igw),
        (dpar_h, dpar), (djump_h, djump), (taps_h, taps), (outp_h, outp)))]
    loads = [
        fetch(13, wg_hbm, wgu.at[:, pl.ds(0, s.ffl)]),
        fetch(14, wu_hbm, wgu.at[:, pl.ds(s.ffl, s.ffl)]),
        fetch(15, wd_hbm, wd),
    ]
    first[0].wait()
    first[1].wait()

    ids0, ids1 = ids[0:1, :].astype(F32), ids[1:2, :].astype(F32)
    w0, w1 = rw[0:1, :], rw[1:2, :]
    names = lax.broadcasted_iota(jnp.int32, (s.ns, s.tok), 0).astype(F32)
    hit0, hit1 = names == ids0, names == ids1
    hits = jnp.where(hit0 | hit1, 1.0, 0.0)
    before = jnp.where(
        lax.broadcasted_iota(jnp.int32, (s.tok, s.tok), 0)
        < lax.broadcasted_iota(jnp.int32, (s.tok, s.tok), 1), 1.0, 0.0)
    counts = dot(hits.astype(BF16), before.astype(BF16))
    slot0 = ids0 * s.room + jnp.sum(jnp.where(hit0, counts, 0.0), axis=0, keepdims=True)
    slot1 = ids1 * s.room + jnp.sum(jnp.where(hit1, counts, 0.0), axis=0, keepdims=True)
    rows = lax.broadcasted_iota(jnp.int32, (s.sl, s.tok), 0).astype(F32)
    own0, own1 = rows == slot0, rows == slot1
    sel[...] = jnp.where(own0 | own1, 1.0, 0.0).astype(BF16)
    gate[...] = jnp.sum(jnp.where(own0, w0, 0.0) + jnp.where(own1, w1, 0.0), axis=1, keepdims=True)
    line = lax.broadcasted_iota(jnp.int32, (s.sl, 1), 0).astype(F32)
    outer = jnp.floor((line + 0.5) * (1.0 / s.bl))
    rest = line - outer * s.bl
    inner = jnp.floor((rest + 0.5) * (1.0 / s.room))
    source = inner * s.bl + outer * s.room + (rest - inner * s.room)
    perm[...] = jnp.where(
        lax.broadcasted_iota(jnp.int32, (s.sl, s.sl), 1).astype(F32) == source, 1.0, 0.0
    ).astype(BF16)

    first[2].wait()
    squares = jnp.zeros((s.tok, s.c), F32)
    for k in range(s.nk):
        part = mid[:, k * s.c:(k + 1) * s.c].astype(F32)
        squares = squares + part * part
    inv = lax.rsqrt(jnp.sum(squares, axis=1, keepdims=True) * (1.0 / s.d) + NORM_EPSILON)
    inv_s[...] = jnp.broadcast_to(inv, inv_s.shape)

    def quarter(c):
        return pl.ds(pl.multiple_of((y * 2 + c) * s.c, s.c), s.c)

    def source_of(i):
        return (y + i) % s.ny

    def blocks(x):
        return x.reshape(-1, s.bl, s.w).astype(BF16)

    def flat(ref):
        return ref.astype(F32).reshape(s.sl, s.w).astype(BF16)

    def half(i):
        return slice(i * s.w, (i + 1) * s.w)

    def toss(q, value):
        s1[q] = blocks(value)
        if q == 0:
            pl.semaphore_wait(barrier, len(partners))
        for d in orders(s.nz):
            zd = (z + d) % s.nz
            send(s1.at[q, zd], r1.at[q, z], "s1", at["s1"] + q, in_line(zd))
        r1[q, z] = s1[q, z]

    for pair in range(4):
        c, kind = pair // 2, pair % 2
        if kind == 0:
            piece = (mid[:, quarter(c)].astype(F32) * inv_s[:, 0:1]).astype(BF16)
            value = dot(sel[...], piece)
        else:
            if pair == 1:
                first[3].wait()
            value = dot(sel[...], og[:, quarter(c)]) * gate[...]
        for h in range(2):
            if 2 * pair + h < s.via:
                toss(2 * pair + h, value[:, half(h)])
            else:
                toss(s.via, value[:, half(h)])
    for i in range(1, s.ny):
        cols = pl.ds(pl.multiple_of((source_of(i) * 2 + 1) * s.c + s.w, s.w), s.w)
        toss(s.via + i, dot(sel[...], og[:, cols]) * gate[...])

    for cp in second:
        cp.wait()
    for side in range(2):
        for n, w in enumerate((rgw, igw)):
            zero = jnp.zeros((w.shape[2], w.shape[3]), F32)
            top = jnp.concatenate([w[side, 0].astype(F32), zero], axis=1)
            low = jnp.concatenate([zero, w[side, 1].astype(F32)], axis=1)
            bd[2 * side + n] = jnp.concatenate([top, low], axis=0).astype(BF16)
    gelu_value, gelu_slope = gelu_parts(bgate[...].astype(F32))
    gel[...] = gelu_value
    both_states = jnp.zeros((s.tok, s.ch), F32)
    mine = (slice(0, s.tok), slice(8, 8 + s.tok))
    front, back = pl.ds(0, 8), pl.ds(s.tok, 8)
    time = lax.broadcasted_iota(jnp.int32, (s.tok, s.ch), 0)
    for side in range(2):
        conv_b = conv[side]
        conv_f = conv_b.astype(F32)
        rate_gate = jax.nn.sigmoid(dot(conv_b, bd[2 * side]))
        input_gate = jax.nn.sigmoid(dot(conv_b, bd[2 * side + 1]))
        decay_rate = softplus_of_minus(dpar[side:side + 1, :])
        log_decay = -RATE_SCALE * rate_gate * decay_rate + djump[side]
        factors = jnp.exp(log_decay)
        squared = jnp.exp(2.0 * log_decay)
        norm_factor = jnp.sqrt(STATE_FLOOR - less_one(2.0 * log_decay))
        drive = input_gate * conv_f
        carried = factors * prior[side]
        both_states = both_states + (carried + norm_factor * drive)
        ks[side, 1, mine[side], :] = (carried - drive * squared / norm_factor) * (
            -RATE_SCALE * decay_rate) * rate_gate * (1.0 - rate_gate)
        ks[side, 2, mine[side], :] = norm_factor * conv_f * input_gate * (1.0 - input_gate)
        ks[side, 3, mine[side], :] = norm_factor * input_gate
        if side == 0:
            link = jnp.where(time < s.tok - 1, pltpu.roll(factors, s.tok - 1, 0), 1.0)
            dec[0:1, :] = factors[0:1, :]
        else:
            link = jnp.where(time > 0, pltpu.roll(factors, 1, 0), 1.0)
            dec[1:2, :] = factors[s.tok - 1:s.tok, :]
        for n, d in enumerate(s.steps):
            inside = time < s.tok - d if side == 0 else time >= d
            pst[side, n] = jnp.where(inside, link, 0.0)
            shift = s.tok - d if side == 0 else d
            link = jnp.where(inside, link * pltpu.roll(link, shift, 0), link)
        ks[side, 0, mine[side], :] = link
    sslope[...] = both_states * gelu_slope
    mixed[...] = (both_states * gelu_value).astype(BF16)
    send(ks.at[0, :, front], ks.at[0, :, back], "ks", at["ks"], on_sp(prv))
    send(ks.at[1, :, back], ks.at[1, :, front], "ks", at["ks"], on_sp(nxt))

    def turn(q):
        recv(r1.at[q, pl.ds(0, s.nz - 1)], at["s1"] + q)
        s2[q] = blocks(dot(perm[...], flat(r1[q])))
        for d in orders(s.nj):
            jd = (j + d) % s.nj
            send(s2.at[q, jd], r2.at[q, j], "s2", at["s2"] + q, in_plane(jd))
        r2[q, j] = s2[q, j]

    top, low = pl.ds(0, s.hs), pl.ds(s.hs, s.hs)

    def tile_of(q, y_of):
        pair, h = q // 2, q % 2
        return xa.at[pair % 2, y_of * 2 + pair // 2, :, half(h)]

    def rows_of(ref, part):
        return ref.at[part]

    def spread(q):
        recv(r2.at[q, pl.ds(0, s.nj - 1)], at["s2"] + q)
        if q >= s.via:
            xa[1, source_of(q - s.via) * 2 + 1, :, half(1)] = flat(r2[q])
            return
        pair, h = q // 2, q % 2
        xa[pair % 2, y * 2 + pair // 2, :, half(h)] = flat(r2[q])
        ref = tile_of(q, y)
        n = at["y"] + 3 * q
        send(ref, ref, "yu", n, on_tp(up))
        send(ref, ref, "yd", n + 1, on_tp(down))

    def relay(q):
        n = at["y"] + 3 * q
        ref = tile_of(q, down)
        recv(ref, n)
        send(ref.at[top], ref.at[top], "yr", n + 2, on_tp(up))
        ref = tile_of(q, up)
        recv(ref, n + 1)
        send(ref.at[low], ref.at[low], "yr", n + 2, on_tp(down))

    def arrive(q):
        recv(tile_of(q, opp), at["y"] + 3 * q + 2)

    def weights_of(k):
        return wgu[pl.ds(pl.multiple_of(k * s.c, s.c), s.c), :]

    def take(pair, places):
        c, kind = pair // 2, pair % 2
        for i, place in enumerate(places):
            k = place * 2 + c
            if kind == 0:
                value = dot(xa[0, k], weights_of(k))
                total = gu
            else:
                value = dot(xa[1, k], wd[:, pl.ds(pl.multiple_of(k * s.c, s.c), s.c)], 1, 1)
                total = ag
            if c == 0 and i == 0 and places[0] is y:
                total[...] = value
            else:
                total[...] += value

    def take_half(place, h):
        k = place * 2 + 1
        cols = pl.ds(pl.multiple_of(k * s.c + h * s.w, s.w), s.w)
        ag[...] += dot(xa[1, k, :, half(h)], wd[:, cols], 1, 1)

    turn(0)
    spread(0)
    turn(1)
    spread(1)
    turn(2)
    relay(0)
    spread(2)
    turn(3)
    relay(1)
    spread(3)
    turn(4)
    for cp in loads:
        cp.wait()
    relay(2)
    spread(4)
    turn(5)
    take(0, [y, up, down])
    relay(3)
    spread(5)
    turn(6)
    turn(7)
    spread(6)
    arrive(0)
    arrive(1)
    take(0, [opp])
    turn(8)
    relay(4)
    spread(7)
    turn(9)
    take(1, [y, up, down])
    relay(5)
    spread(8)
    turn(10)
    arrive(2)
    arrive(3)
    take(1, [opp])
    take(2, [y, up, down])
    spread(9)
    relay(6)
    take_half(source_of(0), 1)
    take_half(source_of(1), 1)
    arrive(4)
    arrive(5)
    take(2, [opp])
    for place in (y, up, down):
        take_half(place, 0)
    take_half(source_of(2), 1)
    spread(10)
    take_half(source_of(3), 1)
    arrive(6)
    take_half(opp, 0)

    gate_pre, up_pre = gu[:, :s.ffl], gu[:, s.ffl:]
    act_grad = ag[...]
    gate_clamped = jnp.minimum(gate_pre, CLAMP_LIMIT)
    up_clamped = jnp.clip(up_pre, -CLAMP_LIMIT, CLAMP_LIMIT)
    gate_sigmoid = jax.nn.sigmoid(SHARPNESS * gate_clamped)
    swish_value = gate_clamped * gate_sigmoid
    act[...] = ((up_clamped + 1.0) * swish_value).astype(BF16)
    delta[:, :s.ffl] = jnp.where(
        gate_pre < CLAMP_LIMIT,
        act_grad * (up_clamped + 1.0)
        * (gate_sigmoid + SHARPNESS * swish_value * (1.0 - gate_sigmoid)), 0.0).astype(BF16)
    delta[:, s.ffl:] = jnp.where(
        jnp.abs(up_pre) < CLAMP_LIMIT, act_grad * swish_value, 0.0).astype(BF16)

    def partial(owner, c):
        return dot(delta[...], weights_of(owner * 2 + c), 1, 1)

    def far_partial(c):
        p2[c] = partial(opp, c).astype(BF16)

    def near_partials(c):
        value = partial(up, c)
        sp1[c, s.hs:, :] = value[s.hs:].astype(BF16)
        ft[c] = value[:s.hs]
        value = partial(down, c)
        sm1[c, :s.hs, :] = value[:s.hs].astype(BF16)
        fm[c] = value[s.hs:]

    def send_far(i):
        c, h = i // 2, half(i % 2)
        n = at["rs"] + 4 * i
        send(p2.at[c, top, h], rt2.at[c, :, h], "rs", n, on_tp(up))
        send(p2.at[c, low, h], rb2.at[c, :, h], "rs", n + 1, on_tp(down))

    def send_near(i):
        c, h = i // 2, half(i % 2)
        n = at["rs"] + 4 * i
        send(sp1.at[c, low, h], rl.at[c, low, h], "rs", n + 2, on_tp(up))
        send(sm1.at[c, top, h], rr.at[c, top, h], "rs", n + 3, on_tp(down))

    def pass_on(i):
        c, h = i // 2, half(i % 2)
        n = at["rs"] + 4 * i
        recv(rt2.at[c, :, h], n)
        sp1[c, :s.hs, h] = (ft[c, :, h] + rt2[c, :, h].astype(F32)).astype(BF16)
        send(sp1.at[c, top, h], rl.at[c, top, h], "rs", n + 2, on_tp(up))
        recv(rb2.at[c, :, h], n + 1)
        sm1[c, s.hs:, h] = (fm[c, :, h] + rb2[c, :, h].astype(F32)).astype(BF16)
        send(sm1.at[c, low, h], rr.at[c, low, h], "rs", n + 3, on_tp(down))

    def own_partial(c):
        fo[c] = partial(y, c)

    def weight_grads(lo, hi):
        @pl.loop(lo, hi)
        def _(k):
            value = dot(xa[0, k], delta[...], 0, 0)
            where = pl.ds(pl.multiple_of(k * s.c, s.c), s.c)
            gg[where, :] = value[:, :s.ffl].astype(BF16)
            ug[where, :] = value[:, s.ffl:].astype(BF16)

    def down_grads(lo, hi):
        @pl.loop(lo, hi)
        def _(k):
            value = dot(act[...], xa[1, k], 0, 0)
            dg[:, pl.ds(pl.multiple_of(k * s.c, s.c), s.c)] = value.astype(BF16)

    stores = [
        pltpu.make_async_copy(src, dst, lsem.at[n]) for n, (src, dst) in enumerate((
            (gg, gg_o), (ug, ug_o), (dg, dg_o), (proj_out, proj_o), (ig_out, ig_o), (bgg_out, bgg_o)))]

    def put(n):
        stores[n].start()

    def give(i):
        c, h = i // 2, half(i % 2)
        n = at["rs"] + 4 * i
        recv(rl.at[c, :, h], n + 2)
        recv(rr.at[c, :, h], n + 3)
        s3[i] = blocks(fo[c, :, h] + rl[c, :, h].astype(F32) + rr[c, :, h].astype(F32))
        for d in orders(s.nj):
            jd = (j + d) % s.nj
            send(s3.at[i, jd], r3.at[i, j], "sa", at["sa"] + i, in_plane(jd))
        r3[i, j] = s3[i, j]

    def turn_back(i):
        recv(r3.at[i, pl.ds(0, s.nj - 1)], at["sa"] + i)
        s4[i] = blocks(dot(perm[...], flat(r3[i])))
        for d in orders(s.nz):
            zd = (z + d) % s.nz
            send(s4.at[i, zd], r4.at[i, z], "sb", at["sb"] + i, in_line(zd))
        r4[i, z] = s4[i, z]

    def tg_of(i, y_of):
        return tg.at[y_of * 2 + i // 2, :, half(i % 2)]

    def combine(i):
        recv(r4.at[i, pl.ds(0, s.nz - 1)], at["sb"] + i)
        tg[y * 2 + i // 2, :, half(i % 2)] = dot(sel[...], flat(r4[i]), 0, 0).astype(BF16)
        ref = tg_of(i, y)
        for to in (opp, up, down):
            send(ref, ref, "tg", at["tg"], on_tp(to))

    far_partial(0)
    send_far(0)
    near_partials(0)
    send_near(0)
    send_far(1)
    far_partial(1)
    own_partial(0)
    pass_on(0)
    send_near(1)
    send_far(2)
    near_partials(1)
    own_partial(1)
    weight_grads(0, s.nk // 4)
    pass_on(1)
    send_near(2)
    send_far(3)
    give(0)
    weight_grads(s.nk // 4, s.nk)
    put(0)
    put(1)
    pass_on(2)
    send_near(3)
    give(1)
    turn_back(0)
    down_grads(0, s.nk // 2)
    pass_on(3)
    give(2)
    turn_back(1)
    down_grads(s.nk // 2, s.nk)
    put(2)
    give(3)
    turn_back(2)
    combine(0)
    turn_back(3)
    combine(1)
    combine(2)
    combine(3)
    recv(tg.at[pl.ds(0, s.nk - 2)], at["tg"])

    inv_col = inv_s[:, 0:1]
    prods = jnp.zeros((s.tok, s.c), F32)
    for k in range(s.nk):
        part = mid[:, k * s.c:(k + 1) * s.c].astype(F32) * inv_col
        prods = prods + tg[k].astype(F32) * part
    inner_mean = jnp.sum(prods, axis=1, keepdims=True) * (1.0 / s.d)
    branch_grad = jnp.zeros((s.tok, s.ch), F32)
    per = s.nk // s.nz
    turns = orders(s.nz) + [0]
    step = max(1, s.nz // 2)
    for lot in (turns[:step], turns[step:]):
        for d in lot:
            zd = (z + d) % s.nz
            for i in range(per):
                k = zd * per + i
                cols = pl.ds(pl.multiple_of(k * s.c, s.c), s.c)
                part = mid[:, cols].astype(F32) * inv_col
                value = (og[:, cols].astype(F32)
                         + inv_col * (tg[k].astype(F32) - part * inner_mean)).astype(BF16)
                branch_grad = branch_grad + dot(value, outp[:, cols], 1, 1)
                value = dot(value, mixed[...], 0, 0).astype(BF16)
                if per == 1:
                    pf[zd] = value.reshape(s.nj, s.r, s.ch)
                else:
                    pf[zd, i * s.c // s.r, pl.ds(i * s.c % s.r, s.c), :] = value
        for d in lot:
            zd = (z + d) % s.nz
            for e in orders(s.nj):
                jd = (j + e) % s.nj
                send(pf.at[zd, jd], pr.at[j, zd], "pj", at["pj"] + zd, in_plane(jd))
            pr[j, zd] = pf[zd, j]
    bgg_out[...] = (branch_grad * sslope[...]).astype(BF16)
    put(5)
    state_grad = branch_grad * gel[...]

    for side in range(2):
        chain = state_grad
        for n, d in enumerate(s.steps):
            shift = s.tok - d if side == 0 else d
            chain = chain + pst[side, n] * pltpu.roll(chain, shift, 0)
        adj[side, mine[side], :] = chain
        edge = slice(0, 1) if side == 0 else slice(s.tok - 1, s.tok)
        edge_of = mine[side].start + edge.start
        cms[side, 0:1, :] = dec[side:side + 1, :] * ks[side, 0, edge_of:edge_of + 1, :]
        cms[side, 1:2, :] = dec[side:side + 1, :] * chain[edge]
    send(adj.at[0, front], adj.at[0, back], "adj", at["adj"], on_sp(prv))
    send(adj.at[1, back], adj.at[1, front], "adj", at["adj"], on_sp(nxt))
    for d in orders(s.nz) + [0]:
        for e in range(s.nj):
            if d or e:
                to = ((z + d) % s.nz) * s.nj + (j + e) % s.nj
                send(cms.at[jnp.where(to < sp, 0, 1)], cmr.at[sp], "cm", at["cm"], on_sp(to))

    for d in orders(s.nz) + [0]:
        zd = (z + d) % s.nz
        recv(pr.at[pl.ds(0, s.nj - 1), zd], at["pj"] + zd)
        total = pr[0, zd].astype(F32)
        for i in range(1, s.nj):
            total = total + pr[i, zd].astype(F32)
        ps2[zd] = total.astype(BF16)
        if d:
            send(ps2.at[zd], pr2.at[z], "pz", at["pz"], in_line(zd))
        else:
            pr2[z] = ps2[zd]

    recv(cmr.at[pl.ds(0, s.ns - 1)], at["cm"])
    recv(ks.at[:, :, front], at["ks"])
    recv(adj.at[:, front], at["adj"])

    nil = jnp.zeros((1, s.ch), F32)
    later, later_next = nil, nil
    for i in range(s.ns - 1, 0, -1):
        a = jnp.where(i > sp, cmr[i, 0:1, :], 1.0)
        b = jnp.where(i > sp, cmr[i, 1:2, :], 0.0)
        later = a * later + b
        later_next = jnp.where(i > sp + 1, later, later_next)
    earlier, earlier_next = nil, nil
    for i in range(s.ns - 1):
        a = jnp.where(i < sp, cmr[i, 0:1, :], 1.0)
        b = jnp.where(i < sp, cmr[i, 1:2, :], 0.0)
        earlier = a * earlier + b
        earlier_next = jnp.where(i < sp - 1, earlier, earlier_next)
    place = lax.broadcasted_iota(jnp.int32, (s.tok + 8, s.ch), 0)
    for side in range(2):
        if side == 0:
            own, inflow = place < s.tok, (later, later_next)
            live = own | (sp < s.ns - 1)
        else:
            own, inflow = place >= 8, (earlier, earlier_next)
            live = own | (sp > 0)
        adjoint = adj[side] + ks[side, 0] * jnp.where(own, inflow[0], inflow[1])
        rate_pre = (adjoint * ks[side, 1]).astype(BF16)
        input_pre = (adjoint * ks[side, 2]).astype(BF16)
        value = (adjoint * ks[side, 3] + dot(rate_pre, bd[2 * side], 1, 1)
                 + dot(input_pre, bd[2 * side + 1], 1, 1))
        cgr[side] = jnp.where(live, value, 0.0)
    reach = taps.shape[1] - 1
    tap = taps[...].astype(F32)
    result = jnp.zeros((s.tok, s.ch), F32)
    for t in range(reach + 1):
        off = reach - t
        result = (result + tap[0, t:t + 1, :] * cgr[0, off:off + s.tok, :]
                  + tap[1, t:t + 1, :] * cgr[1, 8 - off:8 - off + s.tok, :])
    ig_out[...] = result.astype(BF16)
    put(4)

    recv(pr2.at[pl.ds(0, s.nz - 1)], at["pz"])
    total = pr2[0].astype(F32)
    for i in range(1, s.nz):
        total = total + pr2[i].astype(F32)
    proj_out[...] = total
    put(3)

    for cp in stores:
        cp.wait()
    line, plane = pl.ds(0, s.nz - 1), pl.ds(0, s.nj - 1)
    sent(s1.at[:, line], "s1")
    sent(s2.at[:, plane], "s2")
    for group in ("yu", "yd", "yr"):
        sent(xa.at[0, pl.ds(0, s.via), :, half(0)], group)
    sent(xa.at[0, pl.ds(0, 6)], "rs")
    sent(s3.at[:, plane], "sa")
    sent(s4.at[:, line], "sb")
    sent(tg.at[pl.ds(0, 6)], "tg")
    sent(cmr.at[pl.ds(0, s.ns - 1)], "cm")
    sent(ks.at[:, :, front], "ks")
    sent(adj.at[:, front], "adj")
    sent(pf.at[:, plane], "pj")
    sent(ps2.at[line], "pz")


def on_device(mid, out_grad, expert_ids, route_weights, gate_proj, up_proj, down_proj, out_proj,
              branch_gate, conv_out, prior_state, rate_gate_w, input_gate_w, decay_param,
              decay_jump, conv_taps):
    tok, d = mid.shape
    ns, ny = lax.axis_size("sp"), lax.axis_size("tp")
    room = 3 * expert_ids.shape[1] * tok // (2 * ns)
    ffl, ch = gate_proj.shape[2], out_proj.shape[0]
    s = Sizes(tok, d, ns, ny, room, ffl, ch)
    _, count, _, groups = layout(s)
    vm, hbm = pl.BlockSpec(memory_space=pltpu.VMEM), pl.BlockSpec(memory_space=pl.ANY)
    nst = len(s.steps)

    def b(*shape):
        return pltpu.VMEM(shape, BF16)

    def f(*shape):
        return pltpu.VMEM(shape, F32)

    def like(x):
        return pltpu.VMEM(x.shape, x.dtype)

    inputs = (mid, out_grad, expert_ids.T, route_weights.T, gate_proj[0], up_proj[0], down_proj[0],
              out_proj, branch_gate, conv_out, prior_state, rate_gate_w, input_gate_w, decay_param,
              decay_jump, conv_taps)
    scratch = [like(x) for x in inputs[:4] + inputs[7:]] + [
        b(d, 2 * ffl), b(ffl, d), f(tok, 128), b(s.sl, tok), f(s.sl, 1), b(s.sl, s.sl),
        b(s.nq, s.nz, s.bl, s.w), b(s.nq, s.nz, s.bl, s.w), b(s.nq, s.nj, s.bl, s.w), b(s.nq, s.nj, s.bl, s.w),
        b(2, s.nk, s.sl, s.c), f(s.sl, 2 * ffl), f(s.sl, ffl), b(s.sl, 2 * ffl), b(s.sl, ffl),
        b(2, s.sl, s.c), b(2, s.hs, s.c), b(2, s.hs, s.c), b(2, s.sl, s.c), b(2, s.sl, s.c),
        f(2, s.hs, s.c), f(2, s.hs, s.c), f(2, s.sl, s.c), b(2, s.sl, s.c), b(2, s.sl, s.c),
        b(4, s.nj, s.bl, s.w), b(4, s.nj, s.bl, s.w), b(4, s.nz, s.bl, s.w), b(4, s.nz, s.bl, s.w),
        b(s.nk, tok, s.c),
        b(4, ch, ch), f(tok, ch), f(tok, ch), b(tok, ch), f(2, nst, tok, ch), f(2, 4, tok + 8, ch),
        f(2, ch), f(2, tok + 8, ch), f(2, 2, ch), f(ns, 2, ch),
        f(2, tok + 8, ch), b(s.nz, s.nj, s.r, ch), b(s.nj, s.nz, s.r, ch), b(s.nz, s.r, ch), b(s.nz, s.r, ch),
        pltpu.SemaphoreType.DMA((groups,)), pltpu.SemaphoreType.DMA((count,)),
        pltpu.SemaphoreType.DMA((16,)),
    ]
    shapes = (((d, ffl), BF16), ((d, ffl), BF16), ((ffl, d), BF16), ((s.r, ch), F32),
              ((tok, ch), BF16), ((tok, ch), BF16))
    scratch = [pltpu.VMEM(*x) for x in shapes] + scratch
    outs = pl.pallas_call(
        functools.partial(kernel, s),
        out_shape=tuple(pltpu.VMEM(*x) for x in shapes),
        in_specs=[hbm] * len(inputs),
        out_specs=(hbm,) * 6,
        scratch_shapes=scratch,
        compiler_params=pltpu.CompilerParams(
            collective_id=0, has_side_effects=True, vmem_limit_bytes=56 * 1024 * 1024),
        name="step",
    )(*inputs)
    outs = pl.pallas_call(
        write_out,
        out_shape=tuple(jax.ShapeDtypeStruct(*x) for x in shapes),
        in_specs=[hbm] * 6,
        out_specs=(hbm,) * 6,
        scratch_shapes=[pltpu.SemaphoreType.DMA((6,))],
        compiler_params=pltpu.CompilerParams(vmem_limit_bytes=1024 * 1024),
        name="write_out",
    )(*(pltpu.with_memory_space_constraint(x, pltpu.VMEM) for x in outs))
    gg, ug, dg, proj, ig, bgg = outs
    return gg[None], ug[None], dg[None], proj, ig, bgg


def write_out(*refs):
    copies = [pltpu.make_async_copy(refs[i], refs[6 + i], refs[12].at[i]) for i in range(6)]
    for cp in copies:
        cp.start()
    for cp in copies:
        cp.wait()


def solution(mesh):
    in_specs = (
        P("sp", None), P("sp", None), P("sp", None), P("sp", None),
        P("sp", None, "tp"), P("sp", None, "tp"), P("sp", "tp", None), P("tp", None),
        P("sp", "tp"), P(None, "sp", "tp"), P(None, "sp", "tp"), P(None, "tp", None, None),
        P(None, "tp", None, None), P(None, "tp"), P(None, "sp", "tp"), P(None, None, "tp"),
    )
    out_specs = (
        P("sp", None, "tp"), P("sp", None, "tp"), P("sp", "tp", None),
        P("sp", "tp"), P("sp", "tp"), P("sp", "tp"),
    )
    return jax.shard_map(
        on_device, mesh=mesh, in_specs=in_specs, out_specs=out_specs, check_vma=False
    )
```

```python
import functools
import math

import jax
import jax.numpy as jnp
from jax import lax
from jax.experimental import pallas as pl
from jax.experimental.pallas import tpu as pltpu
from jax.sharding import PartitionSpec as P

RATE_SCALE = 8.0
CLAMP_LIMIT = 7.0
SHARPNESS = 1.702
NORM_EPSILON = 1e-06
STATE_FLOOR = 0.001
GELU_CUBIC = 0.044715
GELU_SCALE = 0.7978845608028654

F32 = jnp.float32
BF16 = jnp.bfloat16
MESH = pl.DeviceIdType.MESH


def dot(a, b, ca=1, cb=0):
    return lax.dot_general(a, b, (((ca,), (cb,)), ((), ())), preferred_element_type=F32)


def gelu_parts(values):
    inside = GELU_SCALE * (values + GELU_CUBIC * values * values * values)
    tangent = jnp.tanh(inside)
    result = 0.5 * values * (1.0 + tangent)
    slope_value = 0.5 * (1.0 + tangent) + 0.5 * values * (1.0 - tangent * tangent) * GELU_SCALE * (
        1.0 + 3.0 * GELU_CUBIC * values * values
    )
    return (result, slope_value)


def less_one(x):
    series = jnp.ones_like(x)
    for n in range(8, 1, -1):
        series = 1.0 + x * (1.0 / n) * series
    return jnp.where(jnp.abs(x) < 0.35, x * series, jnp.exp(x) - 1.0)


def softplus_of_minus(x):
    return jnp.maximum(-x, 0.0) + jnp.log1p(jnp.exp(-jnp.abs(x)))


class Sizes:
    def __init__(self, tok, d, ns, ny, room, ffl, ch):
        self.tok, self.d, self.ns, self.ny, self.room = tok, d, ns, ny, room
        self.ffl, self.ch = ffl, ch
        self.nj = math.isqrt(ns)
        self.nz = ns // self.nj
        self.bl = self.nj * room
        self.sl = ns * room
        self.hs = self.sl // 2
        self.ht = tok // 2
        self.nk = 2 * ny
        self.c = d // self.nk
        self.w = self.c // 2
        self.via = 7
        self.nq = self.via + ny + 1
        self.early = 3
        self.across = self.nj // 2
        self.r = d // ns
        self.steps = [1 << i for i in range((tok - 1).bit_length())]


class Book:
    def __init__(self):
        self.n = 0

    def take(self, count):
        at, self.n = self.n, self.n + count
        return at


def layout(s):
    b, g = Book(), Book()
    arrivals = dict(
        s1=b.take(s.nq), s2=b.take(s.nq), s0=b.take(s.early * (s.nj // 2)), y=b.take(3 * s.via), rs=b.take(16), sa=b.take(6),
        sb=b.take(6), tf=b.take(1), tg=b.take(4), cm=b.take(1), ks=b.take(1), adj=b.take(1), pj=b.take(s.nz),
        pz=b.take(1), qz=b.take(1), qp=b.take(1),
    )
    groups = {name: g.take(1) for name in (
        "s1", "s2", "yu", "yd", "yr", "rs", "sa", "sb", "tf", "tg", "cm", "ks", "adj", "pj", "pz", "qz", "qp")}
    return arrivals, b.n, groups, g.n


def kernel(s, *refs):
    (mid_h, og_h, ids_h, rw_h, wg_hbm, wu_hbm, wd_hbm, outp_h, bgate_h, conv_h, prior_h, rgw_h,
     igw_h, dpar_h, djump_h, taps_h,
     gg_o, ug_o, dg_o, proj_o, ig_o, bgg_o,
     gg, ug, dg, proj_out, ig_out, bgg_out,
     mid, og, ids, rw, outp, bgate, conv, prior, rgw, igw, dpar, djump, taps,
     wgu, wd, inv_s, sel, gate, perm, s1, r1, s2, r2, xa, gu, ag, delta, act,
     p2, rt2, rb2, sp1, sm1, ft, fm, fo, rl, rr, s3, r3, s4, r4, tfs, tfr, tg,
     bd, gel, sslope, mixed, pst, ks, dec, adj, cms, cmr,
     cgr, pf, pr, ps2, pr2, qr, qs, qp,
     ssem, rsem, lsem) = refs
    at, _, out, _ = layout(s)
    sp = lax.axis_index("sp")
    y = lax.axis_index("tp")
    z, j = sp // s.nj, sp % s.nj
    up, down = (y + 1) % s.ny, (y + s.ny - 1) % s.ny
    opp = (y + 2) % s.ny
    nxt, prv = (sp + 1) % s.ns, (sp + s.ns - 1) % s.ns

    def orders(n):
        half = n // 2
        out = [half]
        for d in range(half - 1, 0, -1):
            out += [d, n - d]
        return out if n > 2 else [1]

    def on_sp(i):
        return {"sp": i}

    def on_tp(i):
        return {"tp": i}

    def in_line(i):
        return {"sp": i * s.nj + j}

    def in_plane(i):
        return {"sp": z * s.nj + i}

    def send(src, dst, group, ri, dev):
        pltpu.make_async_remote_copy(
            src_ref=src, dst_ref=dst, send_sem=ssem.at[out[group]], recv_sem=rsem.at[ri],
            device_id=dev, device_id_type=MESH).start()

    def all_of(ref, group, ri):
        return pltpu.make_async_remote_copy(
            src_ref=ref, dst_ref=ref, send_sem=ssem.at[out[group]], recv_sem=rsem.at[ri],
            device_id=on_tp(up), device_id_type=MESH)

    def recv(ref, ri):
        all_of(ref, "s1", ri).wait_recv()

    def sent(ref, group):
        all_of(ref, group, 0).wait_send()

    def fetch(n, src, dst):
        cp = pltpu.make_async_copy(src, dst, lsem.at[n])
        cp.start()
        return cp

    barrier = pltpu.get_barrier_semaphore()
    partners = [in_line((z + d) % s.nz) for d in orders(s.nz)]
    partners += [in_plane((j + d) % s.nj) for d in range(1, s.nj)]
    partners += [on_tp(up), on_tp(down), on_sp(nxt), on_sp(prv)]
    for dev in partners:
        pl.semaphore_signal(barrier, inc=1, device_id=dev, device_id_type=MESH)
    first = [fetch(0, ids_h, ids), fetch(1, rw_h, rw), fetch(2, mid_h, mid), fetch(3, og_h, og)]
    second = [fetch(n + 4, src, dst) for n, (src, dst) in enumerate((
        (bgate_h, bgate), (conv_h, conv), (prior_h, prior), (rgw_h, rgw), (igw_h, igw),
        (dpar_h, dpar), (djump_h, djump), (taps_h, taps), (outp_h, outp)))]
    loads = [
        fetch(13, wg_hbm, wgu.at[:, pl.ds(0, s.ffl)]),
        fetch(14, wu_hbm, wgu.at[:, pl.ds(s.ffl, s.ffl)]),
        fetch(15, wd_hbm, wd),
    ]
    first[0].wait()
    first[1].wait()

    ids0, ids1 = ids[0:1, :].astype(F32), ids[1:2, :].astype(F32)
    w0, w1 = rw[0:1, :], rw[1:2, :]
    names = lax.broadcasted_iota(jnp.int32, (s.ns, s.tok), 0).astype(F32)
    hit0, hit1 = names == ids0, names == ids1
    hits = jnp.where(hit0 | hit1, 1.0, 0.0)
    before = jnp.where(
        lax.broadcasted_iota(jnp.int32, (s.tok, s.tok), 0)
        < lax.broadcasted_iota(jnp.int32, (s.tok, s.tok), 1), 1.0, 0.0)
    counts = dot(hits.astype(BF16), before.astype(BF16))
    slot0 = ids0 * s.room + jnp.sum(jnp.where(hit0, counts, 0.0), axis=0, keepdims=True)
    slot1 = ids1 * s.room + jnp.sum(jnp.where(hit1, counts, 0.0), axis=0, keepdims=True)
    rows = lax.broadcasted_iota(jnp.int32, (s.sl, s.tok), 0).astype(F32)
    own0, own1 = rows == slot0, rows == slot1
    sel[...] = jnp.where(own0 | own1, 1.0, 0.0).astype(BF16)
    gate[...] = jnp.sum(jnp.where(own0, w0, 0.0) + jnp.where(own1, w1, 0.0), axis=1, keepdims=True)
    line = lax.broadcasted_iota(jnp.int32, (s.sl, 1), 0).astype(F32)
    outer = jnp.floor((line + 0.5) * (1.0 / s.bl))
    rest = line - outer * s.bl
    inner = jnp.floor((rest + 0.5) * (1.0 / s.room))
    source = inner * s.bl + outer * s.room + (rest - inner * s.room)
    perm[...] = jnp.where(
        lax.broadcasted_iota(jnp.int32, (s.sl, s.sl), 1).astype(F32) == source, 1.0, 0.0
    ).astype(BF16)

    first[2].wait()
    squares = jnp.zeros((s.tok, s.c), F32)
    for k in range(s.nk):
        part = mid[:, k * s.c:(k + 1) * s.c].astype(F32)
        squares = squares + part * part
    inv = lax.rsqrt(jnp.sum(squares, axis=1, keepdims=True) * (1.0 / s.d) + NORM_EPSILON)
    inv_s[...] = jnp.broadcast_to(inv, inv_s.shape)

    def quarter(c):
        return pl.ds(pl.multiple_of((y * 2 + c) * s.c, s.c), s.c)

    def source_of(i):
        return (y + i) % s.ny

    def straight(i):
        return (source_of(i), 1) if i < s.ny else (opp, 0)

    def blocks(x):
        return x.reshape(-1, s.bl, s.w).astype(BF16)

    def flat(ref):
        return ref.astype(F32).reshape(s.sl, s.w).astype(BF16)

    def half(i):
        return slice(i * s.w, (i + 1) * s.w)

    def toss(q, value):
        s1[q] = blocks(value)
        if q == 0:
            pl.semaphore_wait(barrier, len(partners))
        for d in orders(s.nz):
            zd = (z + d) % s.nz
            send(s1.at[q, zd], r1.at[q, z], "s1", at["s1"] + q, in_line(zd))
        r1[q, z] = s1[q, z]

    for pair in range(4):
        c, kind = pair // 2, pair % 2
        if kind == 0:
            piece = (mid[:, quarter(c)].astype(F32) * inv_s[:, 0:1]).astype(BF16)
            value = dot(sel[...], piece)
        else:
            if pair == 1:
                first[3].wait()
            value = dot(sel[...], og[:, quarter(c)]) * gate[...]
        for h in range(2):
            if 2 * pair + h < s.via:
                toss(2 * pair + h, value[:, half(h)])
            else:
                toss(s.via, value[:, half(h)])
    for i in range(1, s.ny + 1):
        owner, h = straight(i)
        cols = pl.ds(pl.multiple_of((owner * 2 + 1) * s.c + h * s.w, s.w), s.w)
        toss(s.via + i, dot(sel[...], og[:, cols]) * gate[...])

    for cp in second:
        cp.wait()
    for side in range(2):
        for n, w in enumerate((rgw, igw)):
            zero = jnp.zeros((w.shape[2], w.shape[3]), F32)
            top = jnp.concatenate([w[side, 0].astype(F32), zero], axis=1)
            low = jnp.concatenate([zero, w[side, 1].astype(F32)], axis=1)
            bd[2 * side + n] = jnp.concatenate([top, low], axis=0).astype(BF16)
    gelu_value, gelu_slope = gelu_parts(bgate[...].astype(F32))
    gel[...] = gelu_value
    both_states = jnp.zeros((s.tok, s.ch), F32)
    mine = (slice(0, s.tok), slice(8, 8 + s.tok))
    front, back = pl.ds(0, 8), pl.ds(s.tok, 8)
    time = lax.broadcasted_iota(jnp.int32, (s.tok, s.ch), 0)
    for side in range(2):
        conv_b = conv[side]
        conv_f = conv_b.astype(F32)
        rate_gate = jax.nn.sigmoid(dot(conv_b, bd[2 * side]))
        input_gate = jax.nn.sigmoid(dot(conv_b, bd[2 * side + 1]))
        decay_rate = softplus_of_minus(dpar[side:side + 1, :])
        log_decay = -RATE_SCALE * rate_gate * decay_rate + djump[side]
        factors = jnp.exp(log_decay)
        squared = jnp.exp(2.0 * log_decay)
        norm_factor = jnp.sqrt(STATE_FLOOR - less_one(2.0 * log_decay))
        drive = input_gate * conv_f
        carried = factors * prior[side]
        both_states = both_states + (carried + norm_factor * drive)
        ks[side, 1, mine[side], :] = (carried - drive * squared / norm_factor) * (
            -RATE_SCALE * decay_rate) * rate_gate * (1.0 - rate_gate)
        ks[side, 2, mine[side], :] = norm_factor * conv_f * input_gate * (1.0 - input_gate)
        ks[side, 3, mine[side], :] = norm_factor * input_gate
        if side == 0:
            link = jnp.where(time < s.tok - 1, pltpu.roll(factors, s.tok - 1, 0), 1.0)
            dec[0:1, :] = factors[0:1, :]
        else:
            link = jnp.where(time > 0, pltpu.roll(factors, 1, 0), 1.0)
            dec[1:2, :] = factors[s.tok - 1:s.tok, :]
        for n, d in enumerate(s.steps):
            inside = time < s.tok - d if side == 0 else time >= d
            pst[side, n] = jnp.where(inside, link, 0.0)
            shift = s.tok - d if side == 0 else d
            link = jnp.where(inside, link * pltpu.roll(link, shift, 0), link)
        ks[side, 0, mine[side], :] = link
    sslope[...] = both_states * gelu_slope
    mixed[...] = (both_states * gelu_value).astype(BF16)
    send(ks.at[0, :, front], ks.at[0, :, back], "ks", at["ks"], on_sp(prv))
    send(ks.at[1, :, back], ks.at[1, :, front], "ks", at["ks"], on_sp(nxt))

    def turn(q):
        recv(r1.at[q, pl.ds(0, s.nz - 1)], at["s1"] + q)
        s2[q] = blocks(dot(perm[...], flat(r1[q])))
        for d in [1] + [i for i in orders(s.nj) if i != 1]:
            jd = j ^ d
            number = at["s0"] + q * (s.nj // 2) + j // 2 if q < s.early else at["s2"] + q
            send(s2.at[q, jd], r2.at[q, j], "s2", number, in_plane(jd))
        r2[q, j] = s2[q, j]

    def spread_early(q, lo, hi):
        rows = 2 * s.bl
        pair, h = q // 2, q % 2
        for d in range(lo, hi):
            x = (j // 2) ^ d
            two = r2.at[q, pl.ds(2 * x, 2)]
            recv(r2.at[q, j ^ 1] if d == 0 else two, at["s0"] + q * (s.nj // 2) + x)
            part = pl.ds(pl.multiple_of(x * rows, rows), rows)
            xa[pair % 2, y * 2 + pair // 2, part, half(h)] = (
                two[...].astype(F32).reshape(rows, s.w).astype(BF16))
            ref = tile_of(q, y).at[part]
            send(ref, ref, "yu", at["y"] + 3 * q, on_tp(up))
            send(ref, ref, "yd", at["y"] + 3 * q + 1, on_tp(down))

    top, low = pl.ds(0, s.hs), pl.ds(s.hs, s.hs)

    def tile_of(q, y_of):
        pair, h = q // 2, q % 2
        return xa.at[pair % 2, y_of * 2 + pair // 2, :, half(h)]

    def rows_of(ref, part):
        return ref.at[part]

    def spread(q):
        recv(r2.at[q, pl.ds(0, s.nj - 1)], at["s2"] + q)
        if q >= s.via:
            owner, h = straight(q - s.via)
            xa[1, owner * 2 + 1, :, half(h)] = flat(r2[q])
            return
        pair, h = q // 2, q % 2
        xa[pair % 2, y * 2 + pair // 2, :, half(h)] = flat(r2[q])
        ref = tile_of(q, y)
        n = at["y"] + 3 * q
        send(ref, ref, "yu", n, on_tp(up))
        send(ref, ref, "yd", n + 1, on_tp(down))

    def relay(q):
        n = at["y"] + 3 * q
        ref = tile_of(q, down)
        recv(ref, n)
        if q < s.via - 1:
            send(ref.at[top], ref.at[top], "yr", n + 2, on_tp(up))
        ref = tile_of(q, up)
        recv(ref, n + 1)
        if q < s.via - 1:
            send(ref.at[low], ref.at[low], "yr", n + 2, on_tp(down))

    def arrive(q):
        recv(tile_of(q, opp), at["y"] + 3 * q + 2)

    def weights_of(k):
        return wgu[pl.ds(pl.multiple_of(k * s.c, s.c), s.c), :]

    def take(pair, places):
        c, kind = pair // 2, pair % 2
        for i, place in enumerate(places):
            k = place * 2 + c
            if kind == 0:
                value = dot(xa[0, k], weights_of(k))
                total = gu
            else:
                value = dot(xa[1, k], wd[:, pl.ds(pl.multiple_of(k * s.c, s.c), s.c)], 1, 1)
                total = ag
            if c == 0 and i == 0 and places[0] is y:
                total[...] = value
            else:
                total[...] += value

    def take_half(place, h):
        k = place * 2 + 1
        cols = pl.ds(pl.multiple_of(k * s.c + h * s.w, s.w), s.w)
        ag[...] += dot(xa[1, k, :, half(h)], wd[:, cols], 1, 1)

    chips = s.nj // 2
    turn(0)
    spread_early(0, 0, 1)
    turn(1)
    spread_early(0, 1, chips)
    spread_early(1, 0, 1)
    turn(2)
    spread_early(1, 1, chips)
    spread_early(2, 0, 1)
    turn(3)
    relay(0)
    spread_early(2, 1, chips)
    turn(4)
    spread(3)
    relay(1)
    turn(5)
    spread(4)
    turn(6)
    for cp in loads:
        cp.wait()
    relay(2)
    spread(5)
    turn(7)
    spread(6)
    relay(3)
    turn(8)
    take(0, [y, up, down])
    turn(9)
    relay(4)
    spread(7)
    arrive(0)
    arrive(1)
    take(0, [opp])
    turn(10)
    spread(8)
    relay(5)
    turn(11)
    take(1, [y, up, down])
    spread(9)
    take(2, [y, up, down])
    for i in range(3):
        take_half(source_of(i), 1)
    spread(10)
    take_half(source_of(3), 1)
    relay(6)
    for place in (y, up, down):
        take_half(place, 0)
    spread(11)
    take_half(opp, 0)
    arrive(2)
    arrive(3)
    take(1, [opp])
    arrive(4)
    arrive(5)
    take(2, [opp])

    gate_pre, up_pre = gu[:, :s.ffl], gu[:, s.ffl:]
    act_grad = ag[...]
    gate_clamped = jnp.minimum(gate_pre, CLAMP_LIMIT)
    up_clamped = jnp.clip(up_pre, -CLAMP_LIMIT, CLAMP_LIMIT)
    gate_sigmoid = jax.nn.sigmoid(SHARPNESS * gate_clamped)
    swish_value = gate_clamped * gate_sigmoid
    act[...] = ((up_clamped + 1.0) * swish_value).astype(BF16)
    delta[:, :s.ffl] = jnp.where(
        gate_pre < CLAMP_LIMIT,
        act_grad * (up_clamped + 1.0)
        * (gate_sigmoid + SHARPNESS * swish_value * (1.0 - gate_sigmoid)), 0.0).astype(BF16)
    delta[:, s.ffl:] = jnp.where(
        jnp.abs(up_pre) < CLAMP_LIMIT, act_grad * swish_value, 0.0).astype(BF16)

    def partial(owner, c):
        return dot(delta[...], weights_of(owner * 2 + c), 1, 1)

    def far_partial(c):
        p2[c] = partial(opp, c).astype(BF16)

    def near_partials(c):
        value = partial(up, c)
        sp1[c, s.hs:, :] = value[s.hs:].astype(BF16)
        ft[c] = value[:s.hs]
        value = partial(down, c)
        sm1[c, :s.hs, :] = value[:s.hs].astype(BF16)
        fm[c] = value[s.hs:]

    def near_full(c):
        sp1[c] = partial(up, c).astype(BF16)
        sm1[c] = partial(down, c).astype(BF16)

    def send_full(i):
        c, h = i // 2, half(i % 2)
        n = at["rs"] + 4 * i
        send(sp1.at[c, :, h], rl.at[c, :, h], "rs", n + 2, on_tp(up))
        send(sm1.at[c, :, h], rr.at[c, :, h], "rs", n + 3, on_tp(down))

    def far_direct(c):
        value = partial(opp, c)
        for h in range(2):
            into_plane(4 + h, value[:, half(h)])

    def send_far(i):
        c, h = i // 2, half(i % 2)
        n = at["rs"] + 4 * i
        send(p2.at[c, top, h], rt2.at[c, :, h], "rs", n, on_tp(up))
        send(p2.at[c, low, h], rb2.at[c, :, h], "rs", n + 1, on_tp(down))

    def send_near(i):
        c, h = i // 2, half(i % 2)
        n = at["rs"] + 4 * i
        send(sp1.at[c, low, h], rl.at[c, low, h], "rs", n + 2, on_tp(up))
        send(sm1.at[c, top, h], rr.at[c, top, h], "rs", n + 3, on_tp(down))

    def pass_on(i):
        c, h = i // 2, half(i % 2)
        n = at["rs"] + 4 * i
        recv(rt2.at[c, :, h], n)
        sp1[c, :s.hs, h] = (ft[c, :, h] + rt2[c, :, h].astype(F32)).astype(BF16)
        send(sp1.at[c, top, h], rl.at[c, top, h], "rs", n + 2, on_tp(up))
        recv(rb2.at[c, :, h], n + 1)
        sm1[c, s.hs:, h] = (fm[c, :, h] + rb2[c, :, h].astype(F32)).astype(BF16)
        send(sm1.at[c, low, h], rr.at[c, low, h], "rs", n + 3, on_tp(down))

    def own_partial(c):
        fo[c] = partial(y, c)

    def weight_grads(lo, hi):
        @pl.loop(lo, hi)
        def _(k):
            value = dot(xa[0, k], delta[...], 0, 0)
            where = pl.ds(pl.multiple_of(k * s.c, s.c), s.c)
            gg[where, :] = value[:, :s.ffl].astype(BF16)
            ug[where, :] = value[:, s.ffl:].astype(BF16)

    def down_grads(lo, hi):
        @pl.loop(lo, hi)
        def _(k):
            value = dot(act[...], xa[1, k], 0, 0)
            dg[:, pl.ds(pl.multiple_of(k * s.c, s.c), s.c)] = value.astype(BF16)

    stores = [
        pltpu.make_async_copy(src, dst, lsem.at[n]) for n, (src, dst) in enumerate((
            (gg, gg_o), (ug, ug_o), (dg, dg_o), (proj_out, proj_o), (ig_out, ig_o), (bgg_out, bgg_o)))]

    def put(n):
        stores[n].start()

    def give(i):
        c, h = i // 2, half(i % 2)
        n = at["rs"] + 4 * i
        recv(rl.at[c, :, h], n + 2)
        recv(rr.at[c, :, h], n + 3)
        into_plane(i, fo[c, :, h] + rl[c, :, h].astype(F32) + rr[c, :, h].astype(F32))

    def into_plane(i, value):
        s3[i] = blocks(value)
        for d in orders(s.nj):
            jd = (j + d) % s.nj
            send(s3.at[i, jd], r3.at[i, j], "sa", at["sa"] + i, in_plane(jd))
        r3[i, j] = s3[i, j]

    def turn_back(i):
        recv(r3.at[i, pl.ds(0, s.nj - 1)], at["sa"] + i)
        s4[i] = blocks(dot(perm[...], flat(r3[i])))
        for d in orders(s.nz):
            zd = (z + d) % s.nz
            send(s4.at[i, zd], r4.at[i, z], "sb", at["sb"] + i, in_line(zd))
        r4[i, z] = s4[i, z]

    def tg_of(i, y_of):
        return tg.at[y_of * 2 + i // 2, :, half(i % 2)]

    def token_sums(i):
        recv(r4.at[i, pl.ds(0, s.nz - 1)], at["sb"] + i)
        return dot(sel[...], flat(r4[i]), 0, 0)

    def combine_far(h):
        tfs[h] = token_sums(4 + h).astype(BF16)
        send(tfs.at[h], tfr.at[h], "tf", at["tf"], on_tp(opp))

    def combine(i):
        value = token_sums(i)
        if i >= 2:
            if i == 2:
                recv(tfr, at["tf"])
            value = value + tfr[i - 2].astype(F32)
        tg[y * 2 + i // 2, :, half(i % 2)] = value.astype(BF16)
        ref = tg_of(i, y)
        for to in (opp, up, down):
            send(ref, ref, "tg", at["tg"] + i, on_tp(to))

    far_partial(0)
    send_far(0)
    near_partials(0)
    send_near(0)
    send_far(1)
    far_direct(1)
    own_partial(0)
    near_full(1)
    pass_on(0)
    send_near(1)
    own_partial(1)
    weight_grads(0, s.nk // 4)
    pass_on(1)
    send_full(2)
    send_full(3)
    turn_back(4)
    turn_back(5)
    weight_grads(s.nk // 4, s.nk // 2)
    give(0)
    weight_grads(s.nk // 2, s.nk)
    put(0)
    put(1)
    give(1)
    turn_back(0)
    down_grads(0, s.nk // 2)
    give(2)
    combine_far(0)
    turn_back(1)
    combine_far(1)
    give(3)
    turn_back(2)
    combine(0)
    down_grads(s.nk // 2, s.nk)
    put(2)
    turn_back(3)
    combine(1)
    combine(2)
    combine(3)
    inv_col = inv_s[:, 0:1]
    prods = jnp.zeros((s.tok, s.w), F32)
    for i in range(4):
        recv(tg.at[pl.ds(0, s.ny - 1), :, half(0)], at["tg"] + i)
        for owner in range(s.ny):
            k, h = owner * 2 + i // 2, i % 2
            part = mid[:, k * s.c + h * s.w:k * s.c + (h + 1) * s.w].astype(F32) * inv_col
            prods = prods + tg[k, :, half(h)].astype(F32) * part
    inner_mean = jnp.sum(prods, axis=1, keepdims=True) * (1.0 / s.d)
    branch_grad = jnp.zeros((s.tok, s.ch), F32)
    per = s.nk // s.nz
    turns = orders(s.nz) + [0]
    over = (j + s.across) % s.nj
    beside = [e for e in orders(s.nj) if e != s.across]
    step = max(1, s.nz // 2)
    for lot in (turns[:step], turns[step:]):
        for d in lot:
            zd = (z + d) % s.nz
            for i in range(per):
                k = zd * per + i
                cols = pl.ds(pl.multiple_of(k * s.c, s.c), s.c)
                part = mid[:, cols].astype(F32) * inv_col
                value = (og[:, cols].astype(F32)
                         + inv_col * (tg[k].astype(F32) - part * inner_mean)).astype(BF16)
                branch_grad = branch_grad + dot(value, outp[:, cols], 1, 1)
                value = dot(value, mixed[...], 0, 0).astype(BF16)
                if per == 1:
                    pf[zd] = value.reshape(s.nj, s.r, s.ch)
                else:
                    pf[zd, i * s.c // s.r, pl.ds(i * s.c % s.r, s.c), :] = value
        for d in lot:
            zd = (z + d) % s.nz
            if d:
                send(pf.at[zd, over], qr.at[z], "qz", at["qz"], in_line(zd))
            else:
                qr[z] = pf[z, over]
            for e in beside:
                jd = (j + e) % s.nj
                send(pf.at[zd, jd], pr.at[j, zd], "pj", at["pj"] + zd, in_plane(jd))
            pr[j, zd] = pf[zd, j]
    bgg_out[...] = (branch_grad * sslope[...]).astype(BF16)
    put(5)
    state_grad = branch_grad * gel[...]

    for side in range(2):
        chain = state_grad
        for n, d in enumerate(s.steps):
            shift = s.tok - d if side == 0 else d
            chain = chain + pst[side, n] * pltpu.roll(chain, shift, 0)
        adj[side, mine[side], :] = chain
        edge = slice(0, 1) if side == 0 else slice(s.tok - 1, s.tok)
        edge_of = mine[side].start + edge.start
        cms[side, 0:1, :] = dec[side:side + 1, :] * ks[side, 0, edge_of:edge_of + 1, :]
        cms[side, 1:2, :] = dec[side:side + 1, :] * chain[edge]
    send(adj.at[0, front], adj.at[0, back], "adj", at["adj"], on_sp(prv))
    send(adj.at[1, back], adj.at[1, front], "adj", at["adj"], on_sp(nxt))
    for d in orders(s.nz) + [0]:
        for e in range(s.nj):
            if d or e:
                to = ((z + d) % s.nz) * s.nj + (j + e) % s.nj
                send(cms.at[jnp.where(to < sp, 0, 1)], cmr.at[sp], "cm", at["cm"], on_sp(to))

    for d in orders(s.nz) + [0]:
        zd = (z + d) % s.nz
        if beside:
            recv(pr.at[pl.ds(0, len(beside)), zd], at["pj"] + zd)
        total = pr[j, zd].astype(F32)
        for e in beside:
            total = total + pr[(j + e) % s.nj, zd].astype(F32)
        ps2[zd] = total.astype(BF16)
        if d:
            send(ps2.at[zd], pr2.at[z], "pz", at["pz"], in_line(zd))
        else:
            pr2[z] = ps2[zd]

    recv(qr.at[pl.ds(0, s.nz - 1)], at["qz"])
    total = qr[0].astype(F32)
    for i in range(1, s.nz):
        total = total + qr[i].astype(F32)
    qs[...] = total.astype(BF16)
    send(qs, qp, "qp", at["qp"], in_plane(over))

    recv(cmr.at[pl.ds(0, s.ns - 1)], at["cm"])
    recv(ks.at[:, :, front], at["ks"])
    recv(adj.at[:, front], at["adj"])

    nil = jnp.zeros((1, s.ch), F32)
    later, later_next = nil, nil
    for i in range(s.ns - 1, 0, -1):
        a = jnp.where(i > sp, cmr[i, 0:1, :], 1.0)
        b = jnp.where(i > sp, cmr[i, 1:2, :], 0.0)
        later = a * later + b
        later_next = jnp.where(i > sp + 1, later, later_next)
    earlier, earlier_next = nil, nil
    for i in range(s.ns - 1):
        a = jnp.where(i < sp, cmr[i, 0:1, :], 1.0)
        b = jnp.where(i < sp, cmr[i, 1:2, :], 0.0)
        earlier = a * earlier + b
        earlier_next = jnp.where(i < sp - 1, earlier, earlier_next)
    place = lax.broadcasted_iota(jnp.int32, (s.tok + 8, s.ch), 0)
    for side in range(2):
        if side == 0:
            own, inflow = place < s.tok, (later, later_next)
            live = own | (sp < s.ns - 1)
        else:
            own, inflow = place >= 8, (earlier, earlier_next)
            live = own | (sp > 0)
        adjoint = adj[side] + ks[side, 0] * jnp.where(own, inflow[0], inflow[1])
        rate_pre = (adjoint * ks[side, 1]).astype(BF16)
        input_pre = (adjoint * ks[side, 2]).astype(BF16)
        value = (adjoint * ks[side, 3] + dot(rate_pre, bd[2 * side], 1, 1)
                 + dot(input_pre, bd[2 * side + 1], 1, 1))
        cgr[side] = jnp.where(live, value, 0.0)
    reach = taps.shape[1] - 1
    tap = taps[...].astype(F32)
    result = jnp.zeros((s.tok, s.ch), F32)
    for t in range(reach + 1):
        off = reach - t
        result = (result + tap[0, t:t + 1, :] * cgr[0, off:off + s.tok, :]
                  + tap[1, t:t + 1, :] * cgr[1, 8 - off:8 - off + s.tok, :])
    ig_out[...] = result.astype(BF16)
    put(4)

    recv(pr2.at[pl.ds(0, s.nz - 1)], at["pz"])
    total = pr2[0].astype(F32)
    for i in range(1, s.nz):
        total = total + pr2[i].astype(F32)
    recv(qp, at["qp"])
    total = total + qp[...].astype(F32)
    proj_out[...] = total
    put(3)

    for cp in stores:
        cp.wait()
    line, plane = pl.ds(0, s.nz - 1), pl.ds(0, s.nj - 1)
    sent(s1.at[:, line], "s1")
    sent(s2.at[:, plane], "s2")
    for group in ("yu", "yd"):
        sent(xa.at[0, pl.ds(0, s.via), :, half(0)], group)
    sent(xa.at[0, pl.ds(0, s.via - 1), :, half(0)], "yr")
    sent(xa.at[0, pl.ds(0, 5)], "rs")
    sent(tfr, "tf")
    sent(s3.at[:, plane], "sa")
    sent(s4.at[:, line], "sb")
    sent(tg.at[pl.ds(0, 6)], "tg")
    sent(cmr.at[pl.ds(0, s.ns - 1)], "cm")
    sent(ks.at[:, :, front], "ks")
    sent(adj.at[:, front], "adj")
    if beside:
        sent(pf.at[:, pl.ds(0, len(beside))], "pj")
    sent(qr.at[line], "qz")
    sent(qs, "qp")
    sent(ps2.at[line], "pz")


def on_device(mid, out_grad, expert_ids, route_weights, gate_proj, up_proj, down_proj, out_proj,
              branch_gate, conv_out, prior_state, rate_gate_w, input_gate_w, decay_param,
              decay_jump, conv_taps):
    tok, d = mid.shape
    ns, ny = lax.axis_size("sp"), lax.axis_size("tp")
    room = 3 * expert_ids.shape[1] * tok // (2 * ns)
    ffl, ch = gate_proj.shape[2], out_proj.shape[0]
    s = Sizes(tok, d, ns, ny, room, ffl, ch)
    _, count, _, groups = layout(s)
    vm, hbm = pl.BlockSpec(memory_space=pltpu.VMEM), pl.BlockSpec(memory_space=pl.ANY)
    nst = len(s.steps)

    def b(*shape):
        return pltpu.VMEM(shape, BF16)

    def f(*shape):
        return pltpu.VMEM(shape, F32)

    def like(x):
        return pltpu.VMEM(x.shape, x.dtype)

    inputs = (mid, out_grad, expert_ids.T, route_weights.T, gate_proj[0], up_proj[0], down_proj[0],
              out_proj, branch_gate, conv_out, prior_state, rate_gate_w, input_gate_w, decay_param,
              decay_jump, conv_taps)
    scratch = [like(x) for x in inputs[:4] + inputs[7:]] + [
        b(d, 2 * ffl), b(ffl, d), f(tok, 128), b(s.sl, tok), f(s.sl, 1), b(s.sl, s.sl),
        b(s.nq, s.nz, s.bl, s.w), b(s.nq, s.nz, s.bl, s.w), b(s.nq, s.nj, s.bl, s.w), b(s.nq, s.nj, s.bl, s.w),
        b(2, s.nk, s.sl, s.c), f(s.sl, 2 * ffl), f(s.sl, ffl), b(s.sl, 2 * ffl), b(s.sl, ffl),
        b(2, s.sl, s.c), b(2, s.hs, s.c), b(2, s.hs, s.c), b(2, s.sl, s.c), b(2, s.sl, s.c),
        f(2, s.hs, s.c), f(2, s.hs, s.c), f(2, s.sl, s.c), b(2, s.sl, s.c), b(2, s.sl, s.c),
        b(6, s.nj, s.bl, s.w), b(6, s.nj, s.bl, s.w), b(6, s.nz, s.bl, s.w), b(6, s.nz, s.bl, s.w),
        b(2, tok, s.w), b(2, tok, s.w),
        b(s.nk, tok, s.c),
        b(4, ch, ch), f(tok, ch), f(tok, ch), b(tok, ch), f(2, nst, tok, ch), f(2, 4, tok + 8, ch),
        f(2, ch), f(2, tok + 8, ch), f(2, 2, ch), f(ns, 2, ch),
        f(2, tok + 8, ch), b(s.nz, s.nj, s.r, ch), b(s.nj, s.nz, s.r, ch), b(s.nz, s.r, ch), b(s.nz, s.r, ch),
        b(s.nz, s.r, ch), b(s.r, ch), b(s.r, ch),
        pltpu.SemaphoreType.DMA((groups,)), pltpu.SemaphoreType.DMA((count,)),
        pltpu.SemaphoreType.DMA((16,)),
    ]
    shapes = (((d, ffl), BF16), ((d, ffl), BF16), ((ffl, d), BF16), ((s.r, ch), F32),
              ((tok, ch), BF16), ((tok, ch), BF16))
    scratch = [pltpu.VMEM(*x) for x in shapes] + scratch
    outs = pl.pallas_call(
        functools.partial(kernel, s),
        out_shape=tuple(pltpu.VMEM(*x) for x in shapes),
        in_specs=[hbm] * len(inputs),
        out_specs=(hbm,) * 6,
        scratch_shapes=scratch,
        compiler_params=pltpu.CompilerParams(
            collective_id=0, has_side_effects=True, vmem_limit_bytes=56 * 1024 * 1024),
        name="step",
    )(*inputs)
    outs = pl.pallas_call(
        write_out,
        out_shape=tuple(jax.ShapeDtypeStruct(*x) for x in shapes),
        in_specs=[hbm] * 6,
        out_specs=(hbm,) * 6,
        scratch_shapes=[pltpu.SemaphoreType.DMA((6,))],
        compiler_params=pltpu.CompilerParams(vmem_limit_bytes=1024 * 1024),
        name="write_out",
    )(*(pltpu.with_memory_space_constraint(x, pltpu.VMEM) for x in outs))
    gg, ug, dg, proj, ig, bgg = outs
    return gg[None], ug[None], dg[None], proj, ig, bgg


def write_out(*refs):
    copies = [pltpu.make_async_copy(refs[i], refs[6 + i], refs[12].at[i]) for i in range(6)]
    for cp in copies:
        cp.start()
    for cp in copies:
        cp.wait()


def solution(mesh):
    in_specs = (
        P("sp", None), P("sp", None), P("sp", None), P("sp", None),
        P("sp", None, "tp"), P("sp", None, "tp"), P("sp", "tp", None), P("tp", None),
        P("sp", "tp"), P(None, "sp", "tp"), P(None, "sp", "tp"), P(None, "tp", None, None),
        P(None, "tp", None, None), P(None, "tp"), P(None, "sp", "tp"), P(None, None, "tp"),
    )
    out_specs = (
        P("sp", None, "tp"), P("sp", None, "tp"), P("sp", "tp", None),
        P("sp", "tp"), P("sp", "tp"), P("sp", "tp"),
    )
    return jax.shard_map(
        on_device, mesh=mesh, in_specs=in_specs, out_specs=out_specs, check_vma=False
    )
```

```python
import functools
import math

import jax
import jax.numpy as jnp
from jax import lax
from jax.experimental import pallas as pl
from jax.experimental.pallas import tpu as pltpu
from jax.sharding import PartitionSpec as P

RATE_SCALE = 8.0
CLAMP_LIMIT = 7.0
SHARPNESS = 1.702
NORM_EPSILON = 1e-06
STATE_FLOOR = 0.001
GELU_CUBIC = 0.044715
GELU_SCALE = 0.7978845608028654

F32 = jnp.float32
BF16 = jnp.bfloat16
MESH = pl.DeviceIdType.MESH


def dot(a, b, ca=1, cb=0):
    return lax.dot_general(a, b, (((ca,), (cb,)), ((), ())), preferred_element_type=F32)


def gelu_parts(values):
    inside = GELU_SCALE * (values + GELU_CUBIC * values * values * values)
    tangent = jnp.tanh(inside)
    result = 0.5 * values * (1.0 + tangent)
    slope_value = 0.5 * (1.0 + tangent) + 0.5 * values * (1.0 - tangent * tangent) * GELU_SCALE * (
        1.0 + 3.0 * GELU_CUBIC * values * values
    )
    return (result, slope_value)


def less_one(x):
    series = jnp.ones_like(x)
    for n in range(8, 1, -1):
        series = 1.0 + x * (1.0 / n) * series
    return jnp.where(jnp.abs(x) < 0.35, x * series, jnp.exp(x) - 1.0)


def softplus_of_minus(x):
    return jnp.maximum(-x, 0.0) + jnp.log1p(jnp.exp(-jnp.abs(x)))


class Sizes:
    def __init__(self, tok, d, ns, ny, room, ffl, ch):
        self.tok, self.d, self.ns, self.ny, self.room = tok, d, ns, ny, room
        self.ffl, self.ch = ffl, ch
        self.nj = math.isqrt(ns)
        self.nz = ns // self.nj
        self.bl = self.nj * room
        self.sl = ns * room
        self.hs = self.sl // 2
        self.ht = tok // 2
        self.nk = 2 * ny
        self.c = d // self.nk
        self.w = self.c // 2
        self.via = 7
        self.nq = self.via + ny + 1
        self.early = 3
        self.across = self.nj // 2
        self.r = d // ns
        self.steps = [1 << i for i in range((tok - 1).bit_length())]


class Book:
    def __init__(self):
        self.n = 0

    def take(self, count):
        at, self.n = self.n, self.n + count
        return at


def layout(s):
    b, g = Book(), Book()
    arrivals = dict(
        s1=b.take(s.nq), s2=b.take(s.nq), s0=b.take(s.early * (s.nj // 2)), y=b.take(3 * s.via), rs=b.take(16), sa=b.take(6),
        sb=b.take(6), tf=b.take(1), tg=b.take(4), cm=b.take(1), ks=b.take(1), adj=b.take(1), pj=b.take(s.nz),
        pz=b.take(1), qz=b.take(1), qp=b.take(1),
    )
    groups = {name: g.take(1) for name in (
        "s1", "s2", "yu", "yd", "yr", "rs", "sa", "sb", "tf", "tg", "cm", "ks", "adj", "pj", "pz", "qz", "qp")}
    return arrivals, b.n, groups, g.n


def kernel(s, *refs):
    (mid_h, og_h, ids_h, rw_h, wg_hbm, wu_hbm, wd_hbm, outp_h, bgate_h, conv_h, prior_h, rgw_h,
     igw_h, dpar_h, djump_h, taps_h,
     gg_o, ug_o, dg_o, proj_o, ig_o, bgg_o,
     gg, ug, dg, proj_out, ig_out, bgg_out,
     mid, og, ids, rw, outp, bgate, conv, prior, rgw, igw, dpar, djump, taps,
     wgu, wd, inv_s, sel, gate, perm, s1, r1, s2, r2, xa, gu, ag, delta, act,
     p2, rt2, rb2, sp1, sm1, ft, fm, fo, rl, rr, s3, r3, s4, r4, tfs, tfr, tg,
     bd, gel, sslope, mixed, pst, ks, dec, adj, cms, cmr,
     cgr, pf, pr, ps2, pr2, qr, qs, qp,
     ssem, rsem, lsem) = refs
    at, _, out, _ = layout(s)
    sp = lax.axis_index("sp")
    y = lax.axis_index("tp")
    z, j = sp // s.nj, sp % s.nj
    up, down = (y + 1) % s.ny, (y + s.ny - 1) % s.ny
    opp = (y + 2) % s.ny
    nxt, prv = (sp + 1) % s.ns, (sp + s.ns - 1) % s.ns

    def orders(n):
        half = n // 2
        out = [half]
        for d in range(half - 1, 0, -1):
            out += [d, n - d]
        return out if n > 2 else [1]

    def on_sp(i):
        return {"sp": i}

    def on_tp(i):
        return {"tp": i}

    def in_line(i):
        return {"sp": i * s.nj + j}

    def in_plane(i):
        return {"sp": z * s.nj + i}

    def send(src, dst, group, ri, dev):
        pltpu.make_async_remote_copy(
            src_ref=src, dst_ref=dst, send_sem=ssem.at[out[group]], recv_sem=rsem.at[ri],
            device_id=dev, device_id_type=MESH).start()

    def all_of(ref, group, ri):
        return pltpu.make_async_remote_copy(
            src_ref=ref, dst_ref=ref, send_sem=ssem.at[out[group]], recv_sem=rsem.at[ri],
            device_id=on_tp(up), device_id_type=MESH)

    def recv(ref, ri):
        all_of(ref, "s1", ri).wait_recv()

    def sent(ref, group):
        all_of(ref, group, 0).wait_send()

    def fetch(n, src, dst):
        cp = pltpu.make_async_copy(src, dst, lsem.at[n])
        cp.start()
        return cp

    barrier = pltpu.get_barrier_semaphore()
    partners = [in_line((z + d) % s.nz) for d in orders(s.nz)]
    partners += [in_plane((j + d) % s.nj) for d in range(1, s.nj)]
    partners += [on_tp(up), on_tp(down), on_sp(nxt), on_sp(prv)]
    for dev in partners:
        pl.semaphore_signal(barrier, inc=1, device_id=dev, device_id_type=MESH)
    first = [fetch(0, ids_h, ids), fetch(1, rw_h, rw), fetch(2, mid_h, mid), fetch(3, og_h, og)]
    second = [fetch(n + 4, src, dst) for n, (src, dst) in enumerate((
        (bgate_h, bgate), (conv_h, conv), (prior_h, prior), (rgw_h, rgw), (igw_h, igw),
        (dpar_h, dpar), (djump_h, djump), (taps_h, taps), (outp_h, outp)))]
    loads = [
        fetch(13, wg_hbm, wgu.at[:, pl.ds(0, s.ffl)]),
        fetch(14, wu_hbm, wgu.at[:, pl.ds(s.ffl, s.ffl)]),
        fetch(15, wd_hbm, wd),
    ]
    first[0].wait()
    first[1].wait()

    ids0, ids1 = ids[0:1, :].astype(F32), ids[1:2, :].astype(F32)
    w0, w1 = rw[0:1, :], rw[1:2, :]
    names = lax.broadcasted_iota(jnp.int32, (s.ns, s.tok), 0).astype(F32)
    hit0, hit1 = names == ids0, names == ids1
    hits = jnp.where(hit0 | hit1, 1.0, 0.0)
    before = jnp.where(
        lax.broadcasted_iota(jnp.int32, (s.tok, s.tok), 0)
        < lax.broadcasted_iota(jnp.int32, (s.tok, s.tok), 1), 1.0, 0.0)
    counts = dot(hits.astype(BF16), before.astype(BF16))
    slot0 = ids0 * s.room + jnp.sum(jnp.where(hit0, counts, 0.0), axis=0, keepdims=True)
    slot1 = ids1 * s.room + jnp.sum(jnp.where(hit1, counts, 0.0), axis=0, keepdims=True)
    rows = lax.broadcasted_iota(jnp.int32, (s.sl, s.tok), 0).astype(F32)
    own0, own1 = rows == slot0, rows == slot1
    sel[...] = jnp.where(own0 | own1, 1.0, 0.0).astype(BF16)
    gate[...] = jnp.sum(jnp.where(own0, w0, 0.0) + jnp.where(own1, w1, 0.0), axis=1, keepdims=True)
    line = lax.broadcasted_iota(jnp.int32, (s.sl, 1), 0).astype(F32)
    outer = jnp.floor((line + 0.5) * (1.0 / s.bl))
    rest = line - outer * s.bl
    inner = jnp.floor((rest + 0.5) * (1.0 / s.room))
    source = inner * s.bl + outer * s.room + (rest - inner * s.room)
    perm[...] = jnp.where(
        lax.broadcasted_iota(jnp.int32, (s.sl, s.sl), 1).astype(F32) == source, 1.0, 0.0
    ).astype(BF16)

    first[2].wait()
    squares = jnp.zeros((s.tok, s.c), F32)
    for k in range(s.nk):
        part = mid[:, k * s.c:(k + 1) * s.c].astype(F32)
        squares = squares + part * part
    inv = lax.rsqrt(jnp.sum(squares, axis=1, keepdims=True) * (1.0 / s.d) + NORM_EPSILON)
    inv_s[...] = jnp.broadcast_to(inv, inv_s.shape)

    def quarter(c):
        return pl.ds(pl.multiple_of((y * 2 + c) * s.c, s.c), s.c)

    def source_of(i):
        return (y + i) % s.ny

    def straight(i):
        return (source_of(i), 1) if i < s.ny else (opp, 0)

    def blocks(x):
        return x.reshape(-1, s.bl, s.w).astype(BF16)

    def flat(ref):
        return ref.astype(F32).reshape(s.sl, s.w).astype(BF16)

    def half(i):
        return slice(i * s.w, (i + 1) * s.w)

    def toss(q, value):
        s1[q] = blocks(value)
        if q == 0:
            pl.semaphore_wait(barrier, len(partners))
        for d in orders(s.nz):
            zd = (z + d) % s.nz
            send(s1.at[q, zd], r1.at[q, z], "s1", at["s1"] + q, in_line(zd))
        r1[q, z] = s1[q, z]

    for pair in range(4):
        c, kind = pair // 2, pair % 2
        if kind == 0:
            piece = (mid[:, quarter(c)].astype(F32) * inv_s[:, 0:1]).astype(BF16)
            value = dot(sel[...], piece)
        else:
            if pair == 1:
                first[3].wait()
            value = dot(sel[...], og[:, quarter(c)]) * gate[...]
        for h in range(2):
            if 2 * pair + h < s.via:
                toss(2 * pair + h, value[:, half(h)])
            else:
                toss(s.via, value[:, half(h)])
    for i in range(1, s.ny + 1):
        owner, h = straight(i)
        cols = pl.ds(pl.multiple_of((owner * 2 + 1) * s.c + h * s.w, s.w), s.w)
        toss(s.via + i, dot(sel[...], og[:, cols]) * gate[...])

    for cp in second:
        cp.wait()
    for side in range(2):
        for n, w in enumerate((rgw, igw)):
            zero = jnp.zeros((w.shape[2], w.shape[3]), F32)
            top = jnp.concatenate([w[side, 0].astype(F32), zero], axis=1)
            low = jnp.concatenate([zero, w[side, 1].astype(F32)], axis=1)
            bd[2 * side + n] = jnp.concatenate([top, low], axis=0).astype(BF16)
    gelu_value, gelu_slope = gelu_parts(bgate[...].astype(F32))
    gel[...] = gelu_value
    both_states = jnp.zeros((s.tok, s.ch), F32)
    mine = (slice(0, s.tok), slice(8, 8 + s.tok))
    front, back = pl.ds(0, 8), pl.ds(s.tok, 8)
    time = lax.broadcasted_iota(jnp.int32, (s.tok, s.ch), 0)
    for side in range(2):
        conv_b = conv[side]
        conv_f = conv_b.astype(F32)
        rate_gate = jax.nn.sigmoid(dot(conv_b, bd[2 * side]))
        input_gate = jax.nn.sigmoid(dot(conv_b, bd[2 * side + 1]))
        decay_rate = softplus_of_minus(dpar[side:side + 1, :])
        log_decay = -RATE_SCALE * rate_gate * decay_rate + djump[side]
        factors = jnp.exp(log_decay)
        squared = jnp.exp(2.0 * log_decay)
        norm_factor = jnp.sqrt(STATE_FLOOR - less_one(2.0 * log_decay))
        drive = input_gate * conv_f
        carried = factors * prior[side]
        both_states = both_states + (carried + norm_factor * drive)
        ks[side, 1, mine[side], :] = (carried - drive * squared / norm_factor) * (
            -RATE_SCALE * decay_rate) * rate_gate * (1.0 - rate_gate)
        ks[side, 2, mine[side], :] = norm_factor * conv_f * input_gate * (1.0 - input_gate)
        ks[side, 3, mine[side], :] = norm_factor * input_gate
        if side == 0:
            link = jnp.where(time < s.tok - 1, pltpu.roll(factors, s.tok - 1, 0), 1.0)
            dec[0:1, :] = factors[0:1, :]
        else:
            link = jnp.where(time > 0, pltpu.roll(factors, 1, 0), 1.0)
            dec[1:2, :] = factors[s.tok - 1:s.tok, :]
        for n, d in enumerate(s.steps):
            inside = time < s.tok - d if side == 0 else time >= d
            pst[side, n] = jnp.where(inside, link, 0.0)
            shift = s.tok - d if side == 0 else d
            link = jnp.where(inside, link * pltpu.roll(link, shift, 0), link)
        ks[side, 0, mine[side], :] = link
    sslope[...] = both_states * gelu_slope
    mixed[...] = (both_states * gelu_value).astype(BF16)
    send(ks.at[0, :, front], ks.at[0, :, back], "ks", at["ks"], on_sp(prv))
    send(ks.at[1, :, back], ks.at[1, :, front], "ks", at["ks"], on_sp(nxt))

    def turn(q):
        recv(r1.at[q, pl.ds(0, s.nz - 1)], at["s1"] + q)
        s2[q] = blocks(dot(perm[...], flat(r1[q])))
        for d in [1] + [i for i in orders(s.nj) if i != 1]:
            jd = j ^ d
            number = at["s0"] + q * (s.nj // 2) + j // 2 if q < s.early else at["s2"] + q
            send(s2.at[q, jd], r2.at[q, j], "s2", number, in_plane(jd))
        r2[q, j] = s2[q, j]

    def spread_early(q, lo, hi):
        rows = 2 * s.bl
        pair, h = q // 2, q % 2
        for d in range(lo, hi):
            x = (j // 2) ^ d
            two = r2.at[q, pl.ds(2 * x, 2)]
            recv(r2.at[q, j ^ 1] if d == 0 else two, at["s0"] + q * (s.nj // 2) + x)
            part = pl.ds(pl.multiple_of(x * rows, rows), rows)
            xa[pair % 2, y * 2 + pair // 2, part, half(h)] = (
                two[...].astype(F32).reshape(rows, s.w).astype(BF16))
            ref = tile_of(q, y).at[part]
            send(ref, ref, "yu", at["y"] + 3 * q, on_tp(up))
            send(ref, ref, "yd", at["y"] + 3 * q + 1, on_tp(down))

    top, low = pl.ds(0, s.hs), pl.ds(s.hs, s.hs)

    def tile_of(q, y_of):
        pair, h = q // 2, q % 2
        return xa.at[pair % 2, y_of * 2 + pair // 2, :, half(h)]

    def rows_of(ref, part):
        return ref.at[part]

    def spread(q):
        recv(r2.at[q, pl.ds(0, s.nj - 1)], at["s2"] + q)
        if q >= s.via:
            owner, h = straight(q - s.via)
            xa[1, owner * 2 + 1, :, half(h)] = flat(r2[q])
            return
        pair, h = q // 2, q % 2
        xa[pair % 2, y * 2 + pair // 2, :, half(h)] = flat(r2[q])
        ref = tile_of(q, y)
        n = at["y"] + 3 * q
        send(ref, ref, "yu", n, on_tp(up))
        send(ref, ref, "yd", n + 1, on_tp(down))

    def relay(q):
        n = at["y"] + 3 * q
        ref = tile_of(q, down)
        recv(ref, n)
        if q < s.via - 1:
            send(ref.at[top], ref.at[top], "yr", n + 2, on_tp(up))
        ref = tile_of(q, up)
        recv(ref, n + 1)
        if q < s.via - 1:
            send(ref.at[low], ref.at[low], "yr", n + 2, on_tp(down))

    def arrive(q):
        recv(tile_of(q, opp), at["y"] + 3 * q + 2)

    def weights_of(k):
        return wgu[pl.ds(pl.multiple_of(k * s.c, s.c), s.c), :]

    def take(pair, places):
        c, kind = pair // 2, pair % 2
        for i, place in enumerate(places):
            k = place * 2 + c
            if kind == 0:
                value = dot(xa[0, k], weights_of(k))
                total = gu
            else:
                value = dot(xa[1, k], wd[:, pl.ds(pl.multiple_of(k * s.c, s.c), s.c)], 1, 1)
                total = ag
            if c == 0 and i == 0 and places[0] is y:
                total[...] = value
            else:
                total[...] += value

    def take_half(place, h):
        k = place * 2 + 1
        cols = pl.ds(pl.multiple_of(k * s.c + h * s.w, s.w), s.w)
        ag[...] += dot(xa[1, k, :, half(h)], wd[:, cols], 1, 1)

    chips = s.nj // 2
    turn(0)
    spread_early(0, 0, 1)
    turn(1)
    spread_early(0, 1, chips)
    spread_early(1, 0, 1)
    turn(2)
    spread_early(1, 1, chips)
    spread_early(2, 0, 1)
    turn(3)
    relay(0)
    spread_early(2, 1, chips)
    turn(4)
    spread(3)
    relay(1)
    turn(5)
    spread(4)
    turn(6)
    for cp in loads:
        cp.wait()
    relay(2)
    spread(5)
    turn(7)
    spread(6)
    relay(3)
    turn(8)
    take(0, [y, up, down])
    turn(9)
    relay(4)
    spread(7)
    arrive(0)
    arrive(1)
    take(0, [opp])
    turn(10)
    spread(8)
    relay(5)
    turn(11)
    take(1, [y, up, down])
    spread(9)
    take(2, [y, up, down])
    for i in range(3):
        take_half(source_of(i), 1)
    spread(10)
    take_half(source_of(3), 1)
    relay(6)
    for place in (y, up, down):
        take_half(place, 0)
    arrive(2)
    arrive(3)
    take(1, [opp])
    arrive(4)
    arrive(5)
    take(2, [opp])
    spread(11)
    take_half(opp, 0)

    gate_pre, up_pre = gu[:, :s.ffl], gu[:, s.ffl:]
    act_grad = ag[...]
    gate_clamped = jnp.minimum(gate_pre, CLAMP_LIMIT)
    up_clamped = jnp.clip(up_pre, -CLAMP_LIMIT, CLAMP_LIMIT)
    gate_sigmoid = jax.nn.sigmoid(SHARPNESS * gate_clamped)
    swish_value = gate_clamped * gate_sigmoid
    act[...] = ((up_clamped + 1.0) * swish_value).astype(BF16)
    delta[:, :s.ffl] = jnp.where(
        gate_pre < CLAMP_LIMIT,
        act_grad * (up_clamped + 1.0)
        * (gate_sigmoid + SHARPNESS * swish_value * (1.0 - gate_sigmoid)), 0.0).astype(BF16)
    delta[:, s.ffl:] = jnp.where(
        jnp.abs(up_pre) < CLAMP_LIMIT, act_grad * swish_value, 0.0).astype(BF16)

    def partial(owner, c):
        return dot(delta[...], weights_of(owner * 2 + c), 1, 1)

    def far_partial(h):
        first_row = pl.multiple_of(opp * 2 * s.c + h * s.w, s.w)
        p2[0, :, half(h)] = dot(delta[...], wgu[pl.ds(first_row, s.w), :], 1, 1).astype(BF16)

    def near_partials(c):
        value = partial(up, c)
        sp1[c, s.hs:, :] = value[s.hs:].astype(BF16)
        ft[c] = value[:s.hs]
        value = partial(down, c)
        sm1[c, :s.hs, :] = value[:s.hs].astype(BF16)
        fm[c] = value[s.hs:]

    def near_full(c):
        sp1[c] = partial(up, c).astype(BF16)
        sm1[c] = partial(down, c).astype(BF16)

    def send_full(i):
        c, h = i // 2, half(i % 2)
        n = at["rs"] + 4 * i
        send(sp1.at[c, :, h], rl.at[c, :, h], "rs", n + 2, on_tp(up))
        send(sm1.at[c, :, h], rr.at[c, :, h], "rs", n + 3, on_tp(down))

    def far_direct(c):
        value = partial(opp, c)
        for h in range(2):
            into_plane(4 + h, value[:, half(h)])

    def send_far(i):
        c, h = i // 2, half(i % 2)
        n = at["rs"] + 4 * i
        send(p2.at[c, top, h], rt2.at[c, :, h], "rs", n, on_tp(up))
        send(p2.at[c, low, h], rb2.at[c, :, h], "rs", n + 1, on_tp(down))

    def send_near(i):
        c, h = i // 2, half(i % 2)
        n = at["rs"] + 4 * i
        send(sp1.at[c, low, h], rl.at[c, low, h], "rs", n + 2, on_tp(up))
        send(sm1.at[c, top, h], rr.at[c, top, h], "rs", n + 3, on_tp(down))

    def pass_on(i):
        c, h = i // 2, half(i % 2)
        n = at["rs"] + 4 * i
        recv(rt2.at[c, :, h], n)
        sp1[c, :s.hs, h] = (ft[c, :, h] + rt2[c, :, h].astype(F32)).astype(BF16)
        send(sp1.at[c, top, h], rl.at[c, top, h], "rs", n + 2, on_tp(up))
        recv(rb2.at[c, :, h], n + 1)
        sm1[c, s.hs:, h] = (fm[c, :, h] + rb2[c, :, h].astype(F32)).astype(BF16)
        send(sm1.at[c, low, h], rr.at[c, low, h], "rs", n + 3, on_tp(down))

    def own_partial(c):
        fo[c] = partial(y, c)

    def weight_grads(lo, hi):
        @pl.loop(lo, hi)
        def _(k):
            value = dot(xa[0, k], delta[...], 0, 0)
            where = pl.ds(pl.multiple_of(k * s.c, s.c), s.c)
            gg[where, :] = value[:, :s.ffl].astype(BF16)
            ug[where, :] = value[:, s.ffl:].astype(BF16)

    def down_grads(lo, hi):
        @pl.loop(lo, hi)
        def _(k):
            value = dot(act[...], xa[1, k], 0, 0)
            dg[:, pl.ds(pl.multiple_of(k * s.c, s.c), s.c)] = value.astype(BF16)

    stores = [
        pltpu.make_async_copy(src, dst, lsem.at[n]) for n, (src, dst) in enumerate((
            (gg, gg_o), (ug, ug_o), (dg, dg_o), (proj_out, proj_o), (ig_out, ig_o), (bgg_out, bgg_o)))]

    def put(n):
        stores[n].start()

    def give(i):
        c, h = i // 2, half(i % 2)
        n = at["rs"] + 4 * i
        recv(rl.at[c, :, h], n + 2)
        recv(rr.at[c, :, h], n + 3)
        into_plane(i, fo[c, :, h] + rl[c, :, h].astype(F32) + rr[c, :, h].astype(F32))

    def into_plane(i, value):
        s3[i] = blocks(value)
        for d in orders(s.nj):
            jd = (j + d) % s.nj
            send(s3.at[i, jd], r3.at[i, j], "sa", at["sa"] + i, in_plane(jd))
        r3[i, j] = s3[i, j]

    def turn_back(i):
        recv(r3.at[i, pl.ds(0, s.nj - 1)], at["sa"] + i)
        s4[i] = blocks(dot(perm[...], flat(r3[i])))
        for d in orders(s.nz):
            zd = (z + d) % s.nz
            send(s4.at[i, zd], r4.at[i, z], "sb", at["sb"] + i, in_line(zd))
        r4[i, z] = s4[i, z]

    def tg_of(i, y_of):
        return tg.at[y_of * 2 + i // 2, :, half(i % 2)]

    def token_sums(i):
        recv(r4.at[i, pl.ds(0, s.nz - 1)], at["sb"] + i)
        return dot(sel[...], flat(r4[i]), 0, 0)

    def combine_far(h):
        tfs[h] = token_sums(4 + h).astype(BF16)
        send(tfs.at[h], tfr.at[h], "tf", at["tf"], on_tp(opp))

    def combine(i):
        value = token_sums(i)
        if i >= 2:
            if i == 2:
                recv(tfr, at["tf"])
            value = value + tfr[i - 2].astype(F32)
        tg[y * 2 + i // 2, :, half(i % 2)] = value.astype(BF16)
        ref = tg_of(i, y)
        for to in (opp, up, down):
            send(ref, ref, "tg", at["tg"] + i, on_tp(to))

    far_partial(0)
    send_far(0)
    far_partial(1)
    send_far(1)
    far_direct(1)
    near_partials(0)
    send_near(0)
    send_near(1)
    near_full(1)
    own_partial(0)
    pass_on(0)
    own_partial(1)
    turn_back(4)
    turn_back(5)
    pass_on(1)
    send_full(2)
    send_full(3)
    weight_grads(0, s.nk // 4)
    give(0)
    weight_grads(s.nk // 4, s.nk)
    put(0)
    put(1)
    give(1)
    turn_back(0)
    down_grads(0, s.nk // 2)
    give(2)
    combine_far(0)
    turn_back(1)
    combine_far(1)
    give(3)
    turn_back(2)
    combine(0)
    turn_back(3)
    combine(1)
    down_grads(s.nk // 2, s.nk)
    put(2)
    combine(2)
    combine(3)
    inv_col = inv_s[:, 0:1]
    prods = jnp.zeros((s.tok, s.w), F32)
    for i in range(4):
        recv(tg.at[pl.ds(0, s.ny - 1), :, half(0)], at["tg"] + i)
        for owner in range(s.ny):
            k, h = owner * 2 + i // 2, i % 2
            part = mid[:, k * s.c + h * s.w:k * s.c + (h + 1) * s.w].astype(F32) * inv_col
            prods = prods + tg[k, :, half(h)].astype(F32) * part
    inner_mean = jnp.sum(prods, axis=1, keepdims=True) * (1.0 / s.d)
    branch_grad = jnp.zeros((s.tok, s.ch), F32)
    per = s.nk // s.nz
    turns = orders(s.nz) + [0]
    over = (j + s.across) % s.nj
    beside = [e for e in orders(s.nj) if e != s.across]
    step = max(1, s.nz // 4)
    for lot in [turns[i:i + step] for i in range(0, s.nz, step)]:
        for d in lot:
            zd = (z + d) % s.nz
            for i in range(per):
                k = zd * per + i
                cols = pl.ds(pl.multiple_of(k * s.c, s.c), s.c)
                part = mid[:, cols].astype(F32) * inv_col
                value = (og[:, cols].astype(F32)
                         + inv_col * (tg[k].astype(F32) - part * inner_mean)).astype(BF16)
                branch_grad = branch_grad + dot(value, outp[:, cols], 1, 1)
                value = dot(value, mixed[...], 0, 0).astype(BF16)
                if per == 1:
                    pf[zd] = value.reshape(s.nj, s.r, s.ch)
                else:
                    pf[zd, i * s.c // s.r, pl.ds(i * s.c % s.r, s.c), :] = value
        for d in lot:
            zd = (z + d) % s.nz
            if d:
                send(pf.at[zd, over], qr.at[z], "qz", at["qz"], in_line(zd))
            else:
                qr[z] = pf[z, over]
            for e in beside:
                jd = (j + e) % s.nj
                send(pf.at[zd, jd], pr.at[j, zd], "pj", at["pj"] + zd, in_plane(jd))
            pr[j, zd] = pf[zd, j]
    bgg_out[...] = (branch_grad * sslope[...]).astype(BF16)
    put(5)
    state_grad = branch_grad * gel[...]

    for side in range(2):
        chain = state_grad
        for n, d in enumerate(s.steps):
            shift = s.tok - d if side == 0 else d
            chain = chain + pst[side, n] * pltpu.roll(chain, shift, 0)
        adj[side, mine[side], :] = chain
        edge = slice(0, 1) if side == 0 else slice(s.tok - 1, s.tok)
        edge_of = mine[side].start + edge.start
        cms[side, 0:1, :] = dec[side:side + 1, :] * ks[side, 0, edge_of:edge_of + 1, :]
        cms[side, 1:2, :] = dec[side:side + 1, :] * chain[edge]
    send(adj.at[0, front], adj.at[0, back], "adj", at["adj"], on_sp(prv))
    send(adj.at[1, back], adj.at[1, front], "adj", at["adj"], on_sp(nxt))
    for d in orders(s.nz) + [0]:
        for e in range(s.nj):
            if d or e:
                to = ((z + d) % s.nz) * s.nj + (j + e) % s.nj
                send(cms.at[jnp.where(to < sp, 0, 1)], cmr.at[sp], "cm", at["cm"], on_sp(to))

    for d in orders(s.nz) + [0]:
        zd = (z + d) % s.nz
        if beside:
            recv(pr.at[pl.ds(0, len(beside)), zd], at["pj"] + zd)
        total = pr[j, zd].astype(F32)
        for e in beside:
            total = total + pr[(j + e) % s.nj, zd].astype(F32)
        ps2[zd] = total.astype(BF16)
        if d:
            send(ps2.at[zd], pr2.at[z], "pz", at["pz"], in_line(zd))
        else:
            pr2[z] = ps2[zd]

    recv(qr.at[pl.ds(0, s.nz - 1)], at["qz"])
    total = qr[0].astype(F32)
    for i in range(1, s.nz):
        total = total + qr[i].astype(F32)
    qs[...] = total.astype(BF16)
    send(qs, qp, "qp", at["qp"], in_plane(over))

    recv(cmr.at[pl.ds(0, s.ns - 1)], at["cm"])
    recv(ks.at[:, :, front], at["ks"])
    recv(adj.at[:, front], at["adj"])

    nil = jnp.zeros((1, s.ch), F32)
    later, later_next = nil, nil
    for i in range(s.ns - 1, 0, -1):
        a = jnp.where(i > sp, cmr[i, 0:1, :], 1.0)
        b = jnp.where(i > sp, cmr[i, 1:2, :], 0.0)
        later = a * later + b
        later_next = jnp.where(i > sp + 1, later, later_next)
    earlier, earlier_next = nil, nil
    for i in range(s.ns - 1):
        a = jnp.where(i < sp, cmr[i, 0:1, :], 1.0)
        b = jnp.where(i < sp, cmr[i, 1:2, :], 0.0)
        earlier = a * earlier + b
        earlier_next = jnp.where(i < sp - 1, earlier, earlier_next)
    place = lax.broadcasted_iota(jnp.int32, (s.tok + 8, s.ch), 0)
    for side in range(2):
        if side == 0:
            own, inflow = place < s.tok, (later, later_next)
            live = own | (sp < s.ns - 1)
        else:
            own, inflow = place >= 8, (earlier, earlier_next)
            live = own | (sp > 0)
        adjoint = adj[side] + ks[side, 0] * jnp.where(own, inflow[0], inflow[1])
        rate_pre = (adjoint * ks[side, 1]).astype(BF16)
        input_pre = (adjoint * ks[side, 2]).astype(BF16)
        value = (adjoint * ks[side, 3] + dot(rate_pre, bd[2 * side], 1, 1)
                 + dot(input_pre, bd[2 * side + 1], 1, 1))
        cgr[side] = jnp.where(live, value, 0.0)
    reach = taps.shape[1] - 1
    tap = taps[...].astype(F32)
    result = jnp.zeros((s.tok, s.ch), F32)
    for t in range(reach + 1):
        off = reach - t
        result = (result + tap[0, t:t + 1, :] * cgr[0, off:off + s.tok, :]
                  + tap[1, t:t + 1, :] * cgr[1, 8 - off:8 - off + s.tok, :])
    ig_out[...] = result.astype(BF16)
    put(4)

    recv(pr2.at[pl.ds(0, s.nz - 1)], at["pz"])
    total = pr2[0].astype(F32)
    for i in range(1, s.nz):
        total = total + pr2[i].astype(F32)
    recv(qp, at["qp"])
    total = total + qp[...].astype(F32)
    proj_out[...] = total
    put(3)

    for cp in stores:
        cp.wait()
    line, plane = pl.ds(0, s.nz - 1), pl.ds(0, s.nj - 1)
    sent(s1.at[:, line], "s1")
    sent(s2.at[:, plane], "s2")
    for group in ("yu", "yd"):
        sent(xa.at[0, pl.ds(0, s.via), :, half(0)], group)
    sent(xa.at[0, pl.ds(0, s.via - 1), :, half(0)], "yr")
    sent(xa.at[0, pl.ds(0, 5)], "rs")
    sent(tfr, "tf")
    sent(s3.at[:, plane], "sa")
    sent(s4.at[:, line], "sb")
    sent(tg.at[pl.ds(0, 6)], "tg")
    sent(cmr.at[pl.ds(0, s.ns - 1)], "cm")
    sent(ks.at[:, :, front], "ks")
    sent(adj.at[:, front], "adj")
    if beside:
        sent(pf.at[:, pl.ds(0, len(beside))], "pj")
    sent(qr.at[line], "qz")
    sent(qs, "qp")
    sent(ps2.at[line], "pz")


def on_device(mid, out_grad, expert_ids, route_weights, gate_proj, up_proj, down_proj, out_proj,
              branch_gate, conv_out, prior_state, rate_gate_w, input_gate_w, decay_param,
              decay_jump, conv_taps):
    tok, d = mid.shape
    ns, ny = lax.axis_size("sp"), lax.axis_size("tp")
    room = 3 * expert_ids.shape[1] * tok // (2 * ns)
    ffl, ch = gate_proj.shape[2], out_proj.shape[0]
    s = Sizes(tok, d, ns, ny, room, ffl, ch)
    _, count, _, groups = layout(s)
    vm, hbm = pl.BlockSpec(memory_space=pltpu.VMEM), pl.BlockSpec(memory_space=pl.ANY)
    nst = len(s.steps)

    def b(*shape):
        return pltpu.VMEM(shape, BF16)

    def f(*shape):
        return pltpu.VMEM(shape, F32)

    def like(x):
        return pltpu.VMEM(x.shape, x.dtype)

    inputs = (mid, out_grad, expert_ids.T, route_weights.T, gate_proj[0], up_proj[0], down_proj[0],
              out_proj, branch_gate, conv_out, prior_state, rate_gate_w, input_gate_w, decay_param,
              decay_jump, conv_taps)
    scratch = [like(x) for x in inputs[:4] + inputs[7:]] + [
        b(d, 2 * ffl), b(ffl, d), f(tok, 128), b(s.sl, tok), f(s.sl, 1), b(s.sl, s.sl),
        b(s.nq, s.nz, s.bl, s.w), b(s.nq, s.nz, s.bl, s.w), b(s.nq, s.nj, s.bl, s.w), b(s.nq, s.nj, s.bl, s.w),
        b(2, s.nk, s.sl, s.c), f(s.sl, 2 * ffl), f(s.sl, ffl), b(s.sl, 2 * ffl), b(s.sl, ffl),
        b(2, s.sl, s.c), b(2, s.hs, s.c), b(2, s.hs, s.c), b(2, s.sl, s.c), b(2, s.sl, s.c),
        f(2, s.hs, s.c), f(2, s.hs, s.c), f(2, s.sl, s.c), b(2, s.sl, s.c), b(2, s.sl, s.c),
        b(6, s.nj, s.bl, s.w), b(6, s.nj, s.bl, s.w), b(6, s.nz, s.bl, s.w), b(6, s.nz, s.bl, s.w),
        b(2, tok, s.w), b(2, tok, s.w),
        b(s.nk, tok, s.c),
        b(4, ch, ch), f(tok, ch), f(tok, ch), b(tok, ch), f(2, nst, tok, ch), f(2, 4, tok + 8, ch),
        f(2, ch), f(2, tok + 8, ch), f(2, 2, ch), f(ns, 2, ch),
        f(2, tok + 8, ch), b(s.nz, s.nj, s.r, ch), b(s.nj, s.nz, s.r, ch), b(s.nz, s.r, ch), b(s.nz, s.r, ch),
        b(s.nz, s.r, ch), b(s.r, ch), b(s.r, ch),
        pltpu.SemaphoreType.DMA((groups,)), pltpu.SemaphoreType.DMA((count,)),
        pltpu.SemaphoreType.DMA((16,)),
    ]
    shapes = (((d, ffl), BF16), ((d, ffl), BF16), ((ffl, d), BF16), ((s.r, ch), F32),
              ((tok, ch), BF16), ((tok, ch), BF16))
    scratch = [pltpu.VMEM(*x) for x in shapes] + scratch
    outs = pl.pallas_call(
        functools.partial(kernel, s),
        out_shape=tuple(pltpu.VMEM(*x) for x in shapes),
        in_specs=[hbm] * len(inputs),
        out_specs=(hbm,) * 6,
        scratch_shapes=scratch,
        compiler_params=pltpu.CompilerParams(
            collective_id=0, has_side_effects=True, vmem_limit_bytes=56 * 1024 * 1024),
        name="step",
    )(*inputs)
    outs = pl.pallas_call(
        write_out,
        out_shape=tuple(jax.ShapeDtypeStruct(*x) for x in shapes),
        in_specs=[hbm] * 6,
        out_specs=(hbm,) * 6,
        scratch_shapes=[pltpu.SemaphoreType.DMA((6,))],
        compiler_params=pltpu.CompilerParams(vmem_limit_bytes=1024 * 1024),
        name="write_out",
    )(*(pltpu.with_memory_space_constraint(x, pltpu.VMEM) for x in outs))
    gg, ug, dg, proj, ig, bgg = outs
    return gg[None], ug[None], dg[None], proj, ig, bgg


def write_out(*refs):
    copies = [pltpu.make_async_copy(refs[i], refs[6 + i], refs[12].at[i]) for i in range(6)]
    for cp in copies:
        cp.start()
    for cp in copies:
        cp.wait()


def solution(mesh):
    in_specs = (
        P("sp", None), P("sp", None), P("sp", None), P("sp", None),
        P("sp", None, "tp"), P("sp", None, "tp"), P("sp", "tp", None), P("tp", None),
        P("sp", "tp"), P(None, "sp", "tp"), P(None, "sp", "tp"), P(None, "tp", None, None),
        P(None, "tp", None, None), P(None, "tp"), P(None, "sp", "tp"), P(None, None, "tp"),
    )
    out_specs = (
        P("sp", None, "tp"), P("sp", None, "tp"), P("sp", "tp", None),
        P("sp", "tp"), P("sp", "tp"), P("sp", "tp"),
    )
    return jax.shard_map(
        on_device, mesh=mesh, in_specs=in_specs, out_specs=out_specs, check_vma=False
    )
```

```python
import functools
import math

import jax
import jax.numpy as jnp
from jax import lax
from jax.experimental import pallas as pl
from jax.experimental.pallas import tpu as pltpu
from jax.sharding import PartitionSpec as P

RATE_SCALE = 8.0
CLAMP_LIMIT = 7.0
SHARPNESS = 1.702
NORM_EPSILON = 1e-06
STATE_FLOOR = 0.001
GELU_CUBIC = 0.044715
GELU_SCALE = 0.7978845608028654

F32 = jnp.float32
BF16 = jnp.bfloat16
MESH = pl.DeviceIdType.MESH


def dot(a, b, ca=1, cb=0):
    return lax.dot_general(a, b, (((ca,), (cb,)), ((), ())), preferred_element_type=F32)


def gelu_parts(values):
    inside = GELU_SCALE * (values + GELU_CUBIC * values * values * values)
    tangent = jnp.tanh(inside)
    result = 0.5 * values * (1.0 + tangent)
    slope_value = 0.5 * (1.0 + tangent) + 0.5 * values * (1.0 - tangent * tangent) * GELU_SCALE * (
        1.0 + 3.0 * GELU_CUBIC * values * values
    )
    return (result, slope_value)


def less_one(x):
    series = jnp.ones_like(x)
    for n in range(8, 1, -1):
        series = 1.0 + x * (1.0 / n) * series
    return jnp.where(jnp.abs(x) < 0.35, x * series, jnp.exp(x) - 1.0)


def softplus_of_minus(x):
    return jnp.maximum(-x, 0.0) + jnp.log1p(jnp.exp(-jnp.abs(x)))


class Sizes:
    def __init__(self, tok, d, ns, ny, room, ffl, ch):
        self.tok, self.d, self.ns, self.ny, self.room = tok, d, ns, ny, room
        self.ffl, self.ch = ffl, ch
        self.nj = math.isqrt(ns)
        self.nz = ns // self.nj
        self.bl = self.nj * room
        self.sl = ns * room
        self.hs = self.sl // 2
        self.ht = tok // 2
        self.nk = 2 * ny
        self.c = d // self.nk
        self.w = self.c // 2
        self.via = 7
        self.nq = self.via + ny + 1
        self.early = 3
        self.across = self.nj // 2
        self.r = d // ns
        self.steps = [1 << i for i in range((tok - 1).bit_length())]


class Book:
    def __init__(self):
        self.n = 0

    def take(self, count):
        at, self.n = self.n, self.n + count
        return at


def layout(s):
    b, g = Book(), Book()
    arrivals = dict(
        s1=b.take(s.nq), s2=b.take(s.nq - s.early), s0=b.take(s.early * (s.nj // 2)), y=b.take(2 * s.via), rs=b.take(12), sa=b.take(6),
        sb=b.take(6), tf=b.take(1), tg=b.take(4), cm=b.take(1), ks=b.take(1), adj=b.take(1), pj=b.take(s.nz),
        pz=b.take(1), qz=b.take(1), qp=b.take(1),
    )
    groups = {name: g.take(1) for name in (
        "s1", "s2", "yu", "yd", "yr", "rs", "sa", "sb", "tf", "tg", "cm", "ks", "adj", "pj", "pz", "qz", "qp")}
    return arrivals, b.n, groups, g.n


def kernel(s, *refs):
    (mid_h, og_h, ids_h, rw_h, wg_hbm, wu_hbm, wd_hbm, outp_h, bgate_h, conv_h, prior_h, rgw_h,
     igw_h, dpar_h, djump_h, taps_h,
     gg_o, ug_o, dg_o, proj_o, ig_o, bgg_o,
     gg, ug, dg, proj_out, ig_out, bgg_out,
     mid, og, ids, rw, outp, bgate, conv, prior, rgw, igw, dpar, djump, taps,
     wgu, wd, inv_s, sel, gate, perm, s1, r1, s2, r2, xa, gu, ag, delta, act,
     p2, rt2, rb2, sp1, sm1, ft, fm, fo, rl, rr, s3, r3, s4, r4, tfs, tfr, tg,
     bd, gel, sslope, mixed, pst, ks, dec, adj, cms, cmr,
     cgr, pf, pr, ps2, pr2, qr, qs, qp,
     ssem, rsem, lsem) = refs
    at, _, out, _ = layout(s)
    sp = lax.axis_index("sp")
    y = lax.axis_index("tp")
    z, j = sp // s.nj, sp % s.nj
    up, down = (y + 1) % s.ny, (y + s.ny - 1) % s.ny
    opp = (y + 2) % s.ny
    nxt, prv = (sp + 1) % s.ns, (sp + s.ns - 1) % s.ns

    def orders(n):
        half = n // 2
        out = [half]
        for d in range(half - 1, 0, -1):
            out += [d, n - d]
        return out if n > 2 else [1]

    def on_sp(i):
        return {"sp": i}

    def on_tp(i):
        return {"tp": i}

    def in_line(i):
        return {"sp": i * s.nj + j}

    def in_plane(i):
        return {"sp": z * s.nj + i}

    def send(src, dst, group, ri, dev):
        pltpu.make_async_remote_copy(
            src_ref=src, dst_ref=dst, send_sem=ssem.at[out[group]], recv_sem=rsem.at[ri],
            device_id=dev, device_id_type=MESH).start()

    def all_of(ref, group, ri):
        return pltpu.make_async_remote_copy(
            src_ref=ref, dst_ref=ref, send_sem=ssem.at[out[group]], recv_sem=rsem.at[ri],
            device_id=on_tp(up), device_id_type=MESH)

    def recv(ref, ri):
        all_of(ref, "s1", ri).wait_recv()

    def sent(ref, group):
        all_of(ref, group, 0).wait_send()

    def fetch(n, src, dst):
        cp = pltpu.make_async_copy(src, dst, lsem.at[n])
        cp.start()
        return cp

    barrier = pltpu.get_barrier_semaphore()
    partners = [in_line((z + d) % s.nz) for d in orders(s.nz)]
    partners += [in_plane((j + d) % s.nj) for d in range(1, s.nj)]
    partners += [on_tp(up), on_tp(down), on_sp(nxt), on_sp(prv)]
    for dev in partners:
        pl.semaphore_signal(barrier, inc=1, device_id=dev, device_id_type=MESH)
    first = [fetch(0, ids_h, ids), fetch(1, rw_h, rw), fetch(2, mid_h, mid), fetch(3, og_h, og)]
    second = [fetch(n + 4, src, dst) for n, (src, dst) in enumerate((
        (bgate_h, bgate), (conv_h, conv), (prior_h, prior), (rgw_h, rgw), (igw_h, igw),
        (dpar_h, dpar), (djump_h, djump), (taps_h, taps), (outp_h, outp)))]
    loads = [
        fetch(13, wg_hbm, wgu.at[:, pl.ds(0, s.ffl)]),
        fetch(14, wu_hbm, wgu.at[:, pl.ds(s.ffl, s.ffl)]),
        fetch(15, wd_hbm, wd),
    ]
    first[0].wait()
    first[1].wait()

    ids0, ids1 = ids[0:1, :].astype(F32), ids[1:2, :].astype(F32)
    w0, w1 = rw[0:1, :], rw[1:2, :]
    names = lax.broadcasted_iota(jnp.int32, (s.ns, s.tok), 0).astype(F32)
    hit0, hit1 = names == ids0, names == ids1
    hits = jnp.where(hit0 | hit1, 1.0, 0.0)
    before = jnp.where(
        lax.broadcasted_iota(jnp.int32, (s.tok, s.tok), 0)
        < lax.broadcasted_iota(jnp.int32, (s.tok, s.tok), 1), 1.0, 0.0)
    counts = dot(hits.astype(BF16), before.astype(BF16))
    slot0 = ids0 * s.room + jnp.sum(jnp.where(hit0, counts, 0.0), axis=0, keepdims=True)
    slot1 = ids1 * s.room + jnp.sum(jnp.where(hit1, counts, 0.0), axis=0, keepdims=True)
    rows = lax.broadcasted_iota(jnp.int32, (s.sl, s.tok), 0).astype(F32)
    own0, own1 = rows == slot0, rows == slot1
    sel[...] = jnp.where(own0 | own1, 1.0, 0.0).astype(BF16)
    gate[...] = jnp.sum(jnp.where(own0, w0, 0.0) + jnp.where(own1, w1, 0.0), axis=1, keepdims=True)
    line = lax.broadcasted_iota(jnp.int32, (s.sl, 1), 0).astype(F32)
    outer = jnp.floor((line + 0.5) * (1.0 / s.bl))
    rest = line - outer * s.bl
    inner = jnp.floor((rest + 0.5) * (1.0 / s.room))
    source = inner * s.bl + outer * s.room + (rest - inner * s.room)
    perm[...] = jnp.where(
        lax.broadcasted_iota(jnp.int32, (s.sl, s.sl), 1).astype(F32) == source, 1.0, 0.0
    ).astype(BF16)

    first[2].wait()
    squares = jnp.zeros((s.tok, s.c), F32)
    for k in range(s.nk):
        part = mid[:, k * s.c:(k + 1) * s.c].astype(F32)
        squares = squares + part * part
    inv = lax.rsqrt(jnp.sum(squares, axis=1, keepdims=True) * (1.0 / s.d) + NORM_EPSILON)
    inv_s[...] = jnp.broadcast_to(inv, inv_s.shape)

    def quarter(c):
        return pl.ds(pl.multiple_of((y * 2 + c) * s.c, s.c), s.c)

    def source_of(i):
        return (y + i) % s.ny

    def straight(i):
        return (source_of(i), 1) if i < s.ny else (opp, 0)

    def blocks(x):
        return x.reshape(-1, s.bl, s.w).astype(BF16)

    def flat(ref):
        return ref.astype(F32).reshape(s.sl, s.w).astype(BF16)

    def half(i):
        return slice(i * s.w, (i + 1) * s.w)

    def toss(q, value):
        s1[q] = blocks(value)
        if q == 0:
            pl.semaphore_wait(barrier, len(partners))
        for d in orders(s.nz):
            zd = (z + d) % s.nz
            send(s1.at[q, zd], r1.at[q, z], "s1", at["s1"] + q, in_line(zd))
        r1[q, z] = s1[q, z]

    for pair in range(4):
        c, kind = pair // 2, pair % 2
        if kind == 0:
            piece = (mid[:, quarter(c)].astype(F32) * inv_s[:, 0:1]).astype(BF16)
            value = dot(sel[...], piece)
        else:
            if pair == 1:
                first[3].wait()
            value = dot(sel[...], og[:, quarter(c)]) * gate[...]
        for h in range(2):
            if 2 * pair + h < s.via:
                toss(2 * pair + h, value[:, half(h)])
            else:
                toss(s.via, value[:, half(h)])
    for i in range(1, s.ny + 1):
        owner, h = straight(i)
        cols = pl.ds(pl.multiple_of((owner * 2 + 1) * s.c + h * s.w, s.w), s.w)
        toss(s.via + i, dot(sel[...], og[:, cols]) * gate[...])

    for cp in second:
        cp.wait()
    for side in range(2):
        for n, w in enumerate((rgw, igw)):
            zero = jnp.zeros((w.shape[2], w.shape[3]), F32)
            top = jnp.concatenate([w[side, 0].astype(F32), zero], axis=1)
            low = jnp.concatenate([zero, w[side, 1].astype(F32)], axis=1)
            bd[2 * side + n] = jnp.concatenate([top, low], axis=0).astype(BF16)
    gelu_value, gelu_slope = gelu_parts(bgate[...].astype(F32))
    gel[...] = gelu_value
    both_states = jnp.zeros((s.tok, s.ch), F32)
    mine = (slice(0, s.tok), slice(8, 8 + s.tok))
    front, back = pl.ds(0, 8), pl.ds(s.tok, 8)
    time = lax.broadcasted_iota(jnp.int32, (s.tok, s.ch), 0)
    for side in range(2):
        conv_b = conv[side]
        conv_f = conv_b.astype(F32)
        rate_gate = jax.nn.sigmoid(dot(conv_b, bd[2 * side]))
        input_gate = jax.nn.sigmoid(dot(conv_b, bd[2 * side + 1]))
        decay_rate = softplus_of_minus(dpar[side:side + 1, :])
        log_decay = -RATE_SCALE * rate_gate * decay_rate + djump[side]
        factors = jnp.exp(log_decay)
        squared = jnp.exp(2.0 * log_decay)
        norm_factor = jnp.sqrt(STATE_FLOOR - less_one(2.0 * log_decay))
        drive = input_gate * conv_f
        carried = factors * prior[side]
        both_states = both_states + (carried + norm_factor * drive)
        ks[side, 1, mine[side], :] = (carried - drive * squared / norm_factor) * (
            -RATE_SCALE * decay_rate) * rate_gate * (1.0 - rate_gate)
        ks[side, 2, mine[side], :] = norm_factor * conv_f * input_gate * (1.0 - input_gate)
        ks[side, 3, mine[side], :] = norm_factor * input_gate
        if side == 0:
            link = jnp.where(time < s.tok - 1, pltpu.roll(factors, s.tok - 1, 0), 1.0)
            dec[0:1, :] = factors[0:1, :]
        else:
            link = jnp.where(time > 0, pltpu.roll(factors, 1, 0), 1.0)
            dec[1:2, :] = factors[s.tok - 1:s.tok, :]
        for n, d in enumerate(s.steps):
            inside = time < s.tok - d if side == 0 else time >= d
            pst[side, n] = jnp.where(inside, link, 0.0)
            shift = s.tok - d if side == 0 else d
            link = jnp.where(inside, link * pltpu.roll(link, shift, 0), link)
        ks[side, 0, mine[side], :] = link
    sslope[...] = both_states * gelu_slope
    mixed[...] = (both_states * gelu_value).astype(BF16)
    send(ks.at[0, :, front], ks.at[0, :, back], "ks", at["ks"], on_sp(prv))
    send(ks.at[1, :, back], ks.at[1, :, front], "ks", at["ks"], on_sp(nxt))

    def turn(q):
        recv(r1.at[q, pl.ds(0, s.nz - 1)], at["s1"] + q)
        s2[q] = blocks(dot(perm[...], flat(r1[q])))
        for d in [1] + [i for i in orders(s.nj) if i != 1]:
            jd = j ^ d
            number = at["s0"] + q * (s.nj // 2) + j // 2 if q < s.early else at["s2"] + q - s.early
            send(s2.at[q, jd], r2.at[q, j], "s2", number, in_plane(jd))
        r2[q, j] = s2[q, j]

    def spread_early(q, lo, hi):
        rows = 2 * s.bl
        pair, h = q // 2, q % 2
        for d in range(lo, hi):
            x = (j // 2) ^ d
            two = r2.at[q, pl.ds(2 * x, 2)]
            recv(r2.at[q, j ^ 1] if d == 0 else two, at["s0"] + q * (s.nj // 2) + x)
            part = pl.ds(pl.multiple_of(x * rows, rows), rows)
            xa[pair % 2, y * 2 + pair // 2, part, half(h)] = (
                two[...].astype(F32).reshape(rows, s.w).astype(BF16))
            ref = tile_of(q, y).at[part]
            send(ref, ref, "yu", at["y"] + 2 * q, on_tp(up))
            send(ref, ref, "yd", at["y"] + 2 * q, on_tp(down))

    top, low = pl.ds(0, s.hs), pl.ds(s.hs, s.hs)

    def tile_of(q, y_of):
        pair, h = q // 2, q % 2
        return xa.at[pair % 2, y_of * 2 + pair // 2, :, half(h)]

    def rows_of(ref, part):
        return ref.at[part]

    def spread(q):
        recv(r2.at[q, pl.ds(0, s.nj - 1)], at["s2"] + q - s.early)
        if q >= s.via:
            owner, h = straight(q - s.via)
            xa[1, owner * 2 + 1, :, half(h)] = flat(r2[q])
            return
        pair, h = q // 2, q % 2
        xa[pair % 2, y * 2 + pair // 2, :, half(h)] = flat(r2[q])
        ref = tile_of(q, y)
        n = at["y"] + 2 * q
        send(ref, ref, "yu", n, on_tp(up))
        send(ref, ref, "yd", n, on_tp(down))

    def relay(q):
        n = at["y"] + 2 * q
        pair, h = q // 2, q % 2
        recv(xa.at[pair % 2, pl.ds(0, 2), :, half(h)], n)
        if q < s.via - 1:
            ref = tile_of(q, down).at[top]
            send(ref, ref, "yr", n + 1, on_tp(up))
            ref = tile_of(q, up).at[low]
            send(ref, ref, "yr", n + 1, on_tp(down))

    def arrive(q):
        recv(tile_of(q, opp), at["y"] + 2 * q + 1)

    def weights_of(k):
        return wgu[pl.ds(pl.multiple_of(k * s.c, s.c), s.c), :]

    def take(pair, places):
        c, kind = pair // 2, pair % 2
        for i, place in enumerate(places):
            k = place * 2 + c
            if kind == 0:
                value = dot(xa[0, k], weights_of(k))
                total = gu
            else:
                value = dot(xa[1, k], wd[:, pl.ds(pl.multiple_of(k * s.c, s.c), s.c)], 1, 1)
                total = ag
            if c == 0 and i == 0 and places[0] is y:
                total[...] = value
            else:
                total[...] += value

    def slopes():
        gate_pre, up_pre = gu[:, :s.ffl], gu[:, s.ffl:]
        gate_clamped = jnp.minimum(gate_pre, CLAMP_LIMIT)
        up_clamped = jnp.clip(up_pre, -CLAMP_LIMIT, CLAMP_LIMIT)
        gate_sigmoid = jax.nn.sigmoid(SHARPNESS * gate_clamped)
        swish_value = gate_clamped * gate_sigmoid
        act[...] = ((up_clamped + 1.0) * swish_value).astype(BF16)
        gate_slope = (up_clamped + 1.0) * (
            gate_sigmoid + SHARPNESS * swish_value * (1.0 - gate_sigmoid))
        gu[:, :s.ffl] = jnp.where(gate_pre < CLAMP_LIMIT, gate_slope, 0.0)
        gu[:, s.ffl:] = jnp.where(jnp.abs(up_pre) < CLAMP_LIMIT, swish_value, 0.0)

    def take_half(place, h):
        k = place * 2 + 1
        cols = pl.ds(pl.multiple_of(k * s.c + h * s.w, s.w), s.w)
        ag[...] += dot(xa[1, k, :, half(h)], wd[:, cols], 1, 1)

    chips = s.nj // 2
    turn(0)
    spread_early(0, 0, 1)
    turn(1)
    spread_early(0, 1, chips)
    spread_early(1, 0, 1)
    turn(2)
    spread_early(1, 1, chips)
    spread_early(2, 0, 1)
    turn(3)
    relay(0)
    spread_early(2, 1, chips)
    turn(4)
    spread(3)
    relay(1)
    turn(5)
    spread(4)
    turn(6)
    for cp in loads:
        cp.wait()
    relay(2)
    spread(5)
    turn(7)
    spread(6)
    relay(3)
    turn(8)
    take(0, [y, up, down])
    turn(9)
    relay(4)
    spread(7)
    arrive(0)
    arrive(1)
    take(0, [opp])
    turn(10)
    spread(8)
    relay(5)
    turn(11)
    take(1, [y, up, down])
    spread(9)
    take(2, [y, up, down])
    for i in range(3):
        take_half(source_of(i), 1)
    spread(10)
    take_half(source_of(3), 1)
    relay(6)
    for place in (y, up, down):
        take_half(place, 0)
    arrive(2)
    arrive(3)
    take(1, [opp])
    arrive(4)
    arrive(5)
    take(2, [opp])
    slopes()
    spread(11)
    take_half(opp, 0)

    act_grad = ag[...]
    delta[:, :s.ffl] = (act_grad * gu[:, :s.ffl]).astype(BF16)
    delta[:, s.ffl:] = (act_grad * gu[:, s.ffl:]).astype(BF16)

    def partial(owner, c):
        return dot(delta[...], weights_of(owner * 2 + c), 1, 1)

    def far_partial(h):
        first_row = pl.multiple_of(opp * 2 * s.c + h * s.w, s.w)
        p2[0, :, half(h)] = dot(delta[...], wgu[pl.ds(first_row, s.w), :], 1, 1).astype(BF16)

    def near_partials(c):
        value = partial(up, c)
        sp1[c, s.hs:, :] = value[s.hs:].astype(BF16)
        ft[c] = value[:s.hs]
        value = partial(down, c)
        sm1[c, :s.hs, :] = value[:s.hs].astype(BF16)
        fm[c] = value[s.hs:]

    def rs_of(i):
        return at["rs"] + (4 * i if i < 2 else 2 * i + 2)

    def near_full(c):
        sp1[c] = partial(up, c).astype(BF16)
        sm1[c] = partial(down, c).astype(BF16)

    def send_full(i):
        c, h = i // 2, half(i % 2)
        n = rs_of(i)
        send(sp1.at[c, :, h], rl.at[c, :, h], "rs", n + 2, on_tp(up))
        send(sm1.at[c, :, h], rr.at[c, :, h], "rs", n + 3, on_tp(down))

    def far_direct(c):
        value = partial(opp, c)
        for h in range(2):
            into_plane(4 + h, value[:, half(h)])

    def send_far(i):
        c, h = i // 2, half(i % 2)
        n = rs_of(i)
        send(p2.at[c, top, h], rt2.at[c, :, h], "rs", n, on_tp(up))
        send(p2.at[c, low, h], rb2.at[c, :, h], "rs", n + 1, on_tp(down))

    def send_near(i):
        c, h = i // 2, half(i % 2)
        n = rs_of(i)
        send(sp1.at[c, low, h], rl.at[c, low, h], "rs", n + 2, on_tp(up))
        send(sm1.at[c, top, h], rr.at[c, top, h], "rs", n + 3, on_tp(down))

    def pass_on(i):
        c, h = i // 2, half(i % 2)
        n = rs_of(i)
        recv(rt2.at[c, :, h], n)
        sp1[c, :s.hs, h] = (ft[c, :, h] + rt2[c, :, h].astype(F32)).astype(BF16)
        send(sp1.at[c, top, h], rl.at[c, top, h], "rs", n + 2, on_tp(up))
        recv(rb2.at[c, :, h], n + 1)
        sm1[c, s.hs:, h] = (fm[c, :, h] + rb2[c, :, h].astype(F32)).astype(BF16)
        send(sm1.at[c, low, h], rr.at[c, low, h], "rs", n + 3, on_tp(down))

    def own_partial(c):
        fo[c] = partial(y, c)

    def weight_grads(lo, hi):
        @pl.loop(lo, hi)
        def _(k):
            value = dot(xa[0, k], delta[...], 0, 0)
            where = pl.ds(pl.multiple_of(k * s.c, s.c), s.c)
            gg[where, :] = value[:, :s.ffl].astype(BF16)
            ug[where, :] = value[:, s.ffl:].astype(BF16)

    def down_grads(lo, hi):
        @pl.loop(lo, hi)
        def _(k):
            value = dot(act[...], xa[1, k], 0, 0)
            dg[:, pl.ds(pl.multiple_of(k * s.c, s.c), s.c)] = value.astype(BF16)

    stores = [
        pltpu.make_async_copy(src, dst, lsem.at[n]) for n, (src, dst) in enumerate((
            (gg, gg_o), (ug, ug_o), (dg, dg_o), (proj_out, proj_o), (ig_out, ig_o), (bgg_out, bgg_o)))]

    def put(n):
        stores[n].start()

    def give(i):
        c, h = i // 2, half(i % 2)
        n = rs_of(i)
        recv(rl.at[c, :, h], n + 2)
        recv(rr.at[c, :, h], n + 3)
        into_plane(i, fo[c, :, h] + rl[c, :, h].astype(F32) + rr[c, :, h].astype(F32))

    def into_plane(i, value):
        s3[i] = blocks(value)
        for d in orders(s.nj):
            jd = (j + d) % s.nj
            send(s3.at[i, jd], r3.at[i, j], "sa", at["sa"] + i, in_plane(jd))
        r3[i, j] = s3[i, j]

    def turn_back(i):
        recv(r3.at[i, pl.ds(0, s.nj - 1)], at["sa"] + i)
        s4[i] = blocks(dot(perm[...], flat(r3[i])))
        for d in orders(s.nz):
            zd = (z + d) % s.nz
            send(s4.at[i, zd], r4.at[i, z], "sb", at["sb"] + i, in_line(zd))
        r4[i, z] = s4[i, z]

    def tg_of(i, y_of):
        return tg.at[y_of * 2 + i // 2, :, half(i % 2)]

    def token_sums(i):
        recv(r4.at[i, pl.ds(0, s.nz - 1)], at["sb"] + i)
        return dot(sel[...], flat(r4[i]), 0, 0)

    def combine_far(h):
        tfs[h] = token_sums(4 + h).astype(BF16)
        send(tfs.at[h], tfr.at[h], "tf", at["tf"], on_tp(opp))

    def combine(i):
        value = token_sums(i)
        if i >= 2:
            if i == 2:
                recv(tfr, at["tf"])
            value = value + tfr[i - 2].astype(F32)
        tg[y * 2 + i // 2, :, half(i % 2)] = value.astype(BF16)
        ref = tg_of(i, y)
        for to in (opp, up, down):
            send(ref, ref, "tg", at["tg"] + i, on_tp(to))

    far_partial(0)
    send_far(0)
    far_partial(1)
    send_far(1)
    far_direct(1)
    near_partials(0)
    send_near(0)
    send_near(1)
    near_full(1)
    own_partial(0)
    pass_on(0)
    own_partial(1)
    turn_back(4)
    turn_back(5)
    pass_on(1)
    send_full(2)
    send_full(3)
    weight_grads(0, s.nk // 4)
    give(0)
    weight_grads(s.nk // 4, s.nk)
    put(0)
    put(1)
    give(1)
    turn_back(0)
    down_grads(0, s.nk // 2)
    give(2)
    combine_far(0)
    turn_back(1)
    combine_far(1)
    give(3)
    turn_back(2)
    combine(0)
    turn_back(3)
    combine(1)
    down_grads(s.nk // 2, s.nk)
    put(2)
    combine(2)
    combine(3)
    inv_col = inv_s[:, 0:1]
    prods = jnp.zeros((s.tok, s.w), F32)
    for i in range(4):
        recv(tg.at[pl.ds(0, s.ny - 1), :, half(0)], at["tg"] + i)
        for owner in range(s.ny):
            k, h = owner * 2 + i // 2, i % 2
            part = mid[:, k * s.c + h * s.w:k * s.c + (h + 1) * s.w].astype(F32) * inv_col
            prods = prods + tg[k, :, half(h)].astype(F32) * part
    inner_mean = jnp.sum(prods, axis=1, keepdims=True) * (1.0 / s.d)
    branch_grad = jnp.zeros((s.tok, s.ch), F32)
    per = s.nk // s.nz
    kept = []
    turns = orders(s.nz) + [0]
    over = (j + s.across) % s.nj
    beside = [e for e in orders(s.nj) if e != s.across]
    step = max(1, s.nz // 4)
    for lot in [turns[i:i + step] for i in range(0, s.nz, step)]:
        for d in lot:
            zd = (z + d) % s.nz
            for i in range(per):
                k = zd * per + i
                cols = pl.ds(pl.multiple_of(k * s.c, s.c), s.c)
                part = mid[:, cols].astype(F32) * inv_col
                value = (og[:, cols].astype(F32)
                         + inv_col * (tg[k].astype(F32) - part * inner_mean)).astype(BF16)
                kept.append((value, cols))
                value = dot(value, mixed[...], 0, 0).astype(BF16)
                if per == 1:
                    pf[zd] = value.reshape(s.nj, s.r, s.ch)
                else:
                    pf[zd, i * s.c // s.r, pl.ds(i * s.c % s.r, s.c), :] = value
        for d in lot:
            zd = (z + d) % s.nz
            if d:
                send(pf.at[zd, over], qr.at[z], "qz", at["qz"], in_line(zd))
            else:
                qr[z] = pf[z, over]
            for e in beside:
                jd = (j + e) % s.nj
                send(pf.at[zd, jd], pr.at[j, zd], "pj", at["pj"] + zd, in_plane(jd))
            pr[j, zd] = pf[zd, j]
    for value, cols in kept:
        branch_grad = branch_grad + dot(value, outp[:, cols], 1, 1)
    bgg_out[...] = (branch_grad * sslope[...]).astype(BF16)
    put(5)
    state_grad = branch_grad * gel[...]

    for side in range(2):
        chain = state_grad
        for n, d in enumerate(s.steps):
            shift = s.tok - d if side == 0 else d
            chain = chain + pst[side, n] * pltpu.roll(chain, shift, 0)
        adj[side, mine[side], :] = chain
        edge = slice(0, 1) if side == 0 else slice(s.tok - 1, s.tok)
        edge_of = mine[side].start + edge.start
        cms[side, 0:1, :] = dec[side:side + 1, :] * ks[side, 0, edge_of:edge_of + 1, :]
        cms[side, 1:2, :] = dec[side:side + 1, :] * chain[edge]
    send(adj.at[0, front], adj.at[0, back], "adj", at["adj"], on_sp(prv))
    send(adj.at[1, back], adj.at[1, front], "adj", at["adj"], on_sp(nxt))
    for d in orders(s.nz) + [0]:
        for e in range(s.nj):
            if d or e:
                to = ((z + d) % s.nz) * s.nj + (j + e) % s.nj
                send(cms.at[jnp.where(to < sp, 0, 1)], cmr.at[sp], "cm", at["cm"], on_sp(to))

    for d in orders(s.nz) + [0]:
        zd = (z + d) % s.nz
        if beside:
            recv(pr.at[pl.ds(0, len(beside)), zd], at["pj"] + zd)
        total = pr[j, zd].astype(F32)
        for e in beside:
            total = total + pr[(j + e) % s.nj, zd].astype(F32)
        ps2[zd] = total.astype(BF16)
        if d:
            send(ps2.at[zd], pr2.at[z], "pz", at["pz"], in_line(zd))
        else:
            pr2[z] = ps2[zd]

    recv(qr.at[pl.ds(0, s.nz - 1)], at["qz"])
    total = qr[0].astype(F32)
    for i in range(1, s.nz):
        total = total + qr[i].astype(F32)
    qs[...] = total.astype(BF16)
    send(qs, qp, "qp", at["qp"], in_plane(over))

    recv(cmr.at[pl.ds(0, s.ns - 1)], at["cm"])
    recv(ks.at[:, :, front], at["ks"])
    recv(adj.at[:, front], at["adj"])

    nil = jnp.zeros((1, s.ch), F32)
    later, later_next = nil, nil
    for i in range(s.ns - 1, 0, -1):
        a = jnp.where(i > sp, cmr[i, 0:1, :], 1.0)
        b = jnp.where(i > sp, cmr[i, 1:2, :], 0.0)
        later = a * later + b
        later_next = jnp.where(i > sp + 1, later, later_next)
    earlier, earlier_next = nil, nil
    for i in range(s.ns - 1):
        a = jnp.where(i < sp, cmr[i, 0:1, :], 1.0)
        b = jnp.where(i < sp, cmr[i, 1:2, :], 0.0)
        earlier = a * earlier + b
        earlier_next = jnp.where(i < sp - 1, earlier, earlier_next)
    place = lax.broadcasted_iota(jnp.int32, (s.tok + 8, s.ch), 0)
    for side in range(2):
        if side == 0:
            own, inflow = place < s.tok, (later, later_next)
            live = own | (sp < s.ns - 1)
        else:
            own, inflow = place >= 8, (earlier, earlier_next)
            live = own | (sp > 0)
        adjoint = adj[side] + ks[side, 0] * jnp.where(own, inflow[0], inflow[1])
        rate_pre = (adjoint * ks[side, 1]).astype(BF16)
        input_pre = (adjoint * ks[side, 2]).astype(BF16)
        value = (adjoint * ks[side, 3] + dot(rate_pre, bd[2 * side], 1, 1)
                 + dot(input_pre, bd[2 * side + 1], 1, 1))
        cgr[side] = jnp.where(live, value, 0.0)
    reach = taps.shape[1] - 1
    tap = taps[...].astype(F32)
    result = jnp.zeros((s.tok, s.ch), F32)
    for t in range(reach + 1):
        off = reach - t
        result = (result + tap[0, t:t + 1, :] * cgr[0, off:off + s.tok, :]
                  + tap[1, t:t + 1, :] * cgr[1, 8 - off:8 - off + s.tok, :])
    ig_out[...] = result.astype(BF16)
    put(4)

    recv(pr2.at[pl.ds(0, s.nz - 1)], at["pz"])
    total = pr2[0].astype(F32)
    for i in range(1, s.nz):
        total = total + pr2[i].astype(F32)
    recv(qp, at["qp"])
    total = total + qp[...].astype(F32)
    proj_out[...] = total
    put(3)

    for cp in stores:
        cp.wait()
    line, plane = pl.ds(0, s.nz - 1), pl.ds(0, s.nj - 1)
    sent(s1.at[:, line], "s1")
    sent(s2.at[:, plane], "s2")
    for group in ("yu", "yd"):
        sent(xa.at[0, pl.ds(0, s.via), :, half(0)], group)
    sent(xa.at[0, pl.ds(0, s.via - 1), :, half(0)], "yr")
    sent(xa.at[0, pl.ds(0, 5)], "rs")
    sent(tfr, "tf")
    sent(s3.at[:, plane], "sa")
    sent(s4.at[:, line], "sb")
    sent(tg.at[pl.ds(0, 6)], "tg")
    sent(cmr.at[pl.ds(0, s.ns - 1)], "cm")
    sent(ks.at[:, :, front], "ks")
    sent(adj.at[:, front], "adj")
    if beside:
        sent(pf.at[:, pl.ds(0, len(beside))], "pj")
    sent(qr.at[line], "qz")
    sent(qs, "qp")
    sent(ps2.at[line], "pz")


def on_device(mid, out_grad, expert_ids, route_weights, gate_proj, up_proj, down_proj, out_proj,
              branch_gate, conv_out, prior_state, rate_gate_w, input_gate_w, decay_param,
              decay_jump, conv_taps):
    tok, d = mid.shape
    ns, ny = lax.axis_size("sp"), lax.axis_size("tp")
    room = 3 * expert_ids.shape[1] * tok // (2 * ns)
    ffl, ch = gate_proj.shape[2], out_proj.shape[0]
    s = Sizes(tok, d, ns, ny, room, ffl, ch)
    _, count, _, groups = layout(s)
    vm, hbm = pl.BlockSpec(memory_space=pltpu.VMEM), pl.BlockSpec(memory_space=pl.ANY)
    nst = len(s.steps)

    def b(*shape):
        return pltpu.VMEM(shape, BF16)

    def f(*shape):
        return pltpu.VMEM(shape, F32)

    def like(x):
        return pltpu.VMEM(x.shape, x.dtype)

    inputs = (mid, out_grad, expert_ids.T, route_weights.T, gate_proj[0], up_proj[0], down_proj[0],
              out_proj, branch_gate, conv_out, prior_state, rate_gate_w, input_gate_w, decay_param,
              decay_jump, conv_taps)
    scratch = [like(x) for x in inputs[:4] + inputs[7:]] + [
        b(d, 2 * ffl), b(ffl, d), f(tok, 128), b(s.sl, tok), f(s.sl, 1), b(s.sl, s.sl),
        b(s.nq, s.nz, s.bl, s.w), b(s.nq, s.nz, s.bl, s.w), b(s.nq, s.nj, s.bl, s.w), b(s.nq, s.nj, s.bl, s.w),
        b(2, s.nk, s.sl, s.c), f(s.sl, 2 * ffl), f(s.sl, ffl), b(s.sl, 2 * ffl), b(s.sl, ffl),
        b(2, s.sl, s.c), b(2, s.hs, s.c), b(2, s.hs, s.c), b(2, s.sl, s.c), b(2, s.sl, s.c),
        f(2, s.hs, s.c), f(2, s.hs, s.c), f(2, s.sl, s.c), b(2, s.sl, s.c), b(2, s.sl, s.c),
        b(6, s.nj, s.bl, s.w), b(6, s.nj, s.bl, s.w), b(6, s.nz, s.bl, s.w), b(6, s.nz, s.bl, s.w),
        b(2, tok, s.w), b(2, tok, s.w),
        b(s.nk, tok, s.c),
        b(4, ch, ch), f(tok, ch), f(tok, ch), b(tok, ch), f(2, nst, tok, ch), f(2, 4, tok + 8, ch),
        f(2, ch), f(2, tok + 8, ch), f(2, 2, ch), f(ns, 2, ch),
        f(2, tok + 8, ch), b(s.nz, s.nj, s.r, ch), b(s.nj, s.nz, s.r, ch), b(s.nz, s.r, ch), b(s.nz, s.r, ch),
        b(s.nz, s.r, ch), b(s.r, ch), b(s.r, ch),
        pltpu.SemaphoreType.DMA((groups,)), pltpu.SemaphoreType.DMA((count,)),
        pltpu.SemaphoreType.DMA((16,)),
    ]
    shapes = (((d, ffl), BF16), ((d, ffl), BF16), ((ffl, d), BF16), ((s.r, ch), F32),
              ((tok, ch), BF16), ((tok, ch), BF16))
    scratch = [pltpu.VMEM(*x) for x in shapes] + scratch
    outs = pl.pallas_call(
        functools.partial(kernel, s),
        out_shape=tuple(pltpu.VMEM(*x) for x in shapes),
        in_specs=[hbm] * len(inputs),
        out_specs=(hbm,) * 6,
        scratch_shapes=scratch,
        compiler_params=pltpu.CompilerParams(
            collective_id=0, has_side_effects=True, vmem_limit_bytes=56 * 1024 * 1024),
        name="step",
    )(*inputs)
    outs = pl.pallas_call(
        write_out,
        out_shape=tuple(jax.ShapeDtypeStruct(*x) for x in shapes),
        in_specs=[hbm] * 6,
        out_specs=(hbm,) * 6,
        scratch_shapes=[pltpu.SemaphoreType.DMA((15,))],
        compiler_params=pltpu.CompilerParams(vmem_limit_bytes=1024 * 1024),
        name="write_out",
    )(*(pltpu.with_memory_space_constraint(x, pltpu.VMEM) for x in outs))
    gg, ug, dg, proj, ig, bgg = outs
    return gg[None], ug[None], dg[None], proj, ig, bgg


def write_out(*refs):
    copies = []
    for i in range(6):
        parts = 4 if i < 3 else 1
        rows = refs[i].shape[0] // parts
        for n in range(parts):
            part = pl.ds(n * rows, rows)
            copies.append(pltpu.make_async_copy(
                refs[i].at[part], refs[6 + i].at[part], refs[12].at[len(copies)]))
    for cp in copies:
        cp.start()
    for cp in copies:
        cp.wait()


def solution(mesh):
    in_specs = (
        P("sp", None), P("sp", None), P("sp", None), P("sp", None),
        P("sp", None, "tp"), P("sp", None, "tp"), P("sp", "tp", None), P("tp", None),
        P("sp", "tp"), P(None, "sp", "tp"), P(None, "sp", "tp"), P(None, "tp", None, None),
        P(None, "tp", None, None), P(None, "tp"), P(None, "sp", "tp"), P(None, None, "tp"),
    )
    out_specs = (
        P("sp", None, "tp"), P("sp", None, "tp"), P("sp", "tp", None),
        P("sp", "tp"), P("sp", "tp"), P("sp", "tp"),
    )
    return jax.shard_map(
        on_device, mesh=mesh, in_specs=in_specs, out_specs=out_specs, check_vma=False
    )
```
